256 devices in a mesh: fs: 32 (over z, y), rep: 4 (over x), tp: 2 (over core).
Axes of the slice: x: 4, y: 4, z: 8, core: 2. Of those that a mesh axis runs over, the one named last changes fastest.
Arguments:
- first_mix: bfloat16 [98304, 2048], P(('fs', 'rep'), 'tp'), may hold values from -6 to 6
- second_mix: bfloat16 [98304, 2048], P(('fs', 'rep'), 'tp'), may hold values from -6 to 6
- lambda_head: float32 [8], P('tp'), may hold values from 0.3 to 0.8
- head_gain: float32 [256], replicated, may hold values from 0.1 to 1.9
- out_cotangent: bfloat16 [98304, 2048], P(('fs', 'rep')), may hold values from -0.078125 to 0.078125
- basis: bfloat16 [2048, 256], P('tp'), may hold values from -0.125 to 0.125
- weight: float32 [2048, 2048], P('tp', 'fs'), may hold values from -3 to 3
- first_moment: float32 [2048, 256], P('fs', 'tp'), may hold values from -4.5 to 4.5
- second_moment: float32 [2048, 256], P('fs', 'tp'), may hold values from 0.05 to 0.5
Outputs:
- weight_new: float32 [2048, 2048], P('tp', 'fs')
- weight_copy: bfloat16 [2048, 2048], P('tp')
- step_out: float32 [2048, 2048], P('tp', 'fs')
- first_new: float32 [2048, 256], P('fs', 'tp')
- second_new: float32 [2048, 256], P('fs', 'tp')
The draws below stay inside these ranges and needn't reach their ends.
All inputs are finite; a program needn't handle non-finite values.
Results may differ from the reference program's by a relative error of at most 0.0075.
Values may be sent and summed in bfloat16 or wider, within the bound.
No kernel may reach another device: no remote copies, remote signals or barrier semaphores. Data moves between devices by JAX's collectives and lax.ppermute only.
A program may use at most 64 MiB of HBM per device.

```python
import math
import jax
import jax.numpy as jnp
from jax import lax

D = 2048
HEADS = 8
HEAD_V = 256
RANK = 256
TOK_DEV = 768
HV = 2048
TOKENS = 98304


def draw_first_moment(key, part):
    draw_base = jnp.clip(jax.random.normal(key, (D, RANK), jnp.float32), -3.0, 3.0)
    roughness = jax.random.uniform(jax.random.fold_in(key, 7), (D, RANK), jnp.float32, 0.5, 1.5)
    rising = 10.0 ** (jnp.arange(D, dtype=jnp.float32) / D)
    return draw_base * 0.1 * rising[:, None] * roughness


def raised(entries, own_key, source, target, parts, factor):
    def block_of(axis_at):
        return (jnp.arange(entries.shape[axis_at]) // (entries.shape[axis_at] // parts)).reshape((-1,) + (1,) * (entries.ndim - 1 - axis_at))

    near = jax.random.permutation(own_key, parts)[block_of(target)]
    second = (block_of(target) + parts // 2) % parts
    return jnp.where((block_of(source) == near) | (block_of(source) == second), factor * entries, entries)


def shard_levels(stream_key, extent, cuts, low, largest):
    def one(axis_at, blocks):
        steps = jax.random.uniform(jax.random.fold_in(jax.random.fold_in(stream_key, 6), axis_at), (blocks,), jnp.float32, low / len(cuts), largest / len(cuts))
        return jnp.repeat(jnp.exp(steps), extent[axis_at] // blocks).reshape((-1,) + (1,) * (len(extent) - axis_at - 1))

    gain = one(*cuts[0])
    for cut in cuts[1:]:
        gain = gain * one(*cut)
    return gain


def bell_draw(stream_key, shape, deviation, limit, cuts=(), kind=jnp.bfloat16):
    loudness = shard_levels(stream_key, shape, cuts, -0.22, 0.18) if cuts else 1.0
    array = jax.random.normal(stream_key, shape, jnp.float32) * deviation * loudness
    return jnp.minimum(jnp.maximum(array, -limit), limit).astype(kind)


def gaussian_with(key, extent, width, most, cuts, heavy, held_as=jnp.bfloat16):
    values = width * jax.random.normal(key, extent, jnp.float32)
    if cuts:
        values = values * shard_levels(key, extent, cuts, -0.22, 0.18)
    return jnp.clip(raised(values, jax.random.fold_in(key, 3), *heavy), -most, most).astype(held_as)


def setup_inputs(seed: int = 0) -> dict:
    splits = jax.random.split(jax.random.key(seed), 10)
    return {
        "first_mix": bell_draw(splits[0], (TOKENS, HV), 1.0, 6.0, ((0, 128), (1, 2))),
        "second_mix": bell_draw(splits[1], (TOKENS, HV), 1.0, 6.0, ((0, 128), (1, 2))),
        "lambda_head": jnp.clip(0.3 + 0.5 * jax.random.uniform(splits[2], (HEADS,), jnp.float32) ** shard_levels(splits[2], (HEADS,), ((0, 2),), -0.2, 0.2), 0.3, 0.8),
        "head_gain": jnp.clip(1.0 + 0.18 * jax.random.normal(splits[3], (HEAD_V,), jnp.float32), 0.1, 1.9),
        "out_cotangent": gaussian_with(splits[4], (TOKENS, D), (TOKENS ** -0.5), 0.078125, ((0, 128),), (0, 1, 128, 5.5)),
        "basis": bell_draw(splits[5], (HV, RANK), HV ** -0.5, 0.125, ((0, 2),)),
        "weight": bell_draw(splits[6], (HV, D), 0.5, 3.0, ((0, 2), (1, 32)), jnp.float32),
        "first_moment": draw_first_moment(jax.random.fold_in(splits[9], 71), 0),
        "second_moment": jnp.clip(jnp.exp(math.log(0.5) - 2.3025851 * jax.random.uniform(splits[8], (D, RANK), jnp.float32) ** shard_levels(splits[8], (D, RANK), ((0, 32), (1, 2)), -0.2, 0.2)), 0.05, 0.5),
    }


out_scale = 0.8
beta_first = 0.9
beta_second = 0.95

def head_output(first_piece, second_piece, lambdas, head_gain):
    token_count = first_piece.shape[0]
    head_width = head_gain.shape[0]
    head_count = lambdas.shape[0] // head_width
    mixture = first_piece.astype(jnp.float32) - lambdas[None, :] * second_piece.astype(jnp.float32)
    grouped = mixture.reshape(token_count, head_count, head_width)
    inverse = lax.rsqrt(lax.optimization_barrier(jnp.mean(grouped * grouped, axis=-1, keepdims=True)) + 1e-06)
    normed = grouped * inverse * head_gain[None, None, :] * out_scale
    return normed.reshape(token_count, head_count * head_width).astype(jnp.bfloat16)

def reference(first_mix, second_mix, lambda_head, head_gain, out_cotangent, basis, weight, first_moment, second_moment):
    block_count = first_mix.shape[0] // TOK_DEV
    lambdas = jnp.repeat(lambda_head, HEAD_V)

    def accumulate(running, pieces):
        first_piece, second_piece, cot_piece = pieces
        head_out = head_output(first_piece, second_piece, lambdas, head_gain)
        term = lax.dot_general(cot_piece, head_out, (((0,), (0,)), ((), ())), preferred_element_type=jnp.float32)
        return (running + term, None)
    grad_t, _ = lax.scan(accumulate, jnp.zeros((D, HV), jnp.float32), (first_mix.reshape(block_count, TOK_DEV, HV), second_mix.reshape(block_count, TOK_DEV, HV), out_cotangent.reshape(block_count, TOK_DEV, D)))
    basis_wide = basis.astype(jnp.float32)
    projected = jnp.dot(grad_t, basis_wide, precision=lax.Precision.HIGHEST)
    first_new = beta_first * first_moment + (1.0 - beta_first) * projected
    second_new = beta_second * second_moment + (1.0 - beta_second) * projected * projected
    direction = first_new / (jnp.sqrt(second_new) + 1e-08)
    spread = jnp.sqrt(jnp.mean(direction * direction))
    step_out = jnp.dot(basis_wide, direction.T, precision=lax.Precision.HIGHEST) * (-1.0 / (spread + 1e-06))
    weight_new = weight + step_out
    weight_copy = weight_new.astype(jnp.bfloat16)
    return (weight_new, weight_copy, step_out, first_new, second_new)
```

```python
import functools

import jax
import jax.numpy as jnp
from jax import lax
from jax.experimental import pallas as pl
from jax.experimental.pallas import tpu as pltpu
from jax.sharding import Mesh
from jax.sharding import PartitionSpec as P

OUT_SCALE = 0.8
BETA_FIRST = 0.9
BETA_SECOND = 0.95
FS = ("z", "y")
FS_REP = ("z", "y", "x")


def shift(array, axis, hops):
    count = lax.axis_size(axis)
    return lax.ppermute(array, axis, [(i, (i + hops) % count) for i in range(count)])


def swap_cores(array):
    return lax.ppermute(array, "tp", [(0, 1), (1, 0)])


def reduced_kernel(half_ref, lam_ref, first_ref, second_ref, gain_ref, basis_ref, own_ref, sent_ref):
    width = gain_ref.shape[1]
    gain = gain_ref[...] * OUT_SCALE
    total = None
    for head in range(first_ref.shape[1] // width):
        cols = slice(head * width, (head + 1) * width)
        mixture = first_ref[:, cols].astype(jnp.float32) - lam_ref[head] * second_ref[:, cols].astype(jnp.float32)
        inverse = lax.rsqrt(jnp.mean(mixture * mixture, axis=-1, keepdims=True) + 1e-06)
        normed = (mixture * inverse * gain).astype(jnp.bfloat16)
        term = jnp.dot(normed, basis_ref[cols, :], preferred_element_type=jnp.float32)
        total = term if total is None else total + term
    half = total.shape[1] // 2
    low, high = total[:, :half], total[:, half:]
    is_low = half_ref[0] == 0
    own_ref[...] = jnp.where(is_low, low, high)
    sent_ref[...] = jnp.where(is_low, high, low).astype(jnp.bfloat16)


def reduced_parts(half_index, lambda_head, first_mix, second_mix, head_gain, basis):
    tokens, values = first_mix.shape
    rank = basis.shape[1]
    tile = 128
    smem = pl.BlockSpec(memory_space=pltpu.SMEM)
    return pl.pallas_call(
        reduced_kernel,
        grid=(tokens // tile,),
        in_specs=[
            smem,
            smem,
            pl.BlockSpec((tile, values), lambda i: (i, 0)),
            pl.BlockSpec((tile, values), lambda i: (i, 0)),
            pl.BlockSpec((1, head_gain.shape[0]), lambda i: (0, 0)),
            pl.BlockSpec((values, rank), lambda i: (0, 0)),
        ],
        out_specs=[pl.BlockSpec((tile, rank // 2), lambda i: (i, 0))] * 2,
        out_shape=[
            jax.ShapeDtypeStruct((tokens, rank // 2), jnp.float32),
            jax.ShapeDtypeStruct((tokens, rank // 2), jnp.bfloat16),
        ],
        name="reduced_parts",
    )(half_index, lambda_head, first_mix, second_mix, head_gain[None, :], basis)


def widen_kernel(y_ref, own_ref, one_ref, three_ref, two_ref, out_ref, slots):
    y = y_ref[0]
    slots[y] = own_ref[...]
    slots[(y + 3) % 4] = one_ref[...]
    slots[(y + 1) % 4] = three_ref[...]
    slots[(y + 2) % 4] = two_ref[...]
    rows, lanes = own_ref.shape
    side = lanes // 2
    for pair in range(2):
        cols = slice(pair * lanes, (pair + 1) * lanes)
        left, right = slots[2 * pair], slots[2 * pair + 1]
        out_ref[:rows, cols] = jnp.concatenate([left[:, :side], right[:, :side]], axis=1)
        out_ref[rows:, cols] = jnp.concatenate([left[:, side:], right[:, side:]], axis=1)


def widen(y_index, own, one, three, two):
    rows, lanes = own.shape
    vmem = pl.BlockSpec(memory_space=pltpu.VMEM)
    return pl.pallas_call(
        widen_kernel,
        in_specs=[pl.BlockSpec(memory_space=pltpu.SMEM)] + [vmem] * 4,
        out_specs=vmem,
        out_shape=jax.ShapeDtypeStruct((2 * rows, 2 * lanes), own.dtype),
        scratch_shapes=[pltpu.VMEM((4, rows, lanes), own.dtype)],
        name="widen",
    )(y_index, own, one, three, two)


def product(left, right):
    return lax.dot_general(left, right, (((1,), (1,)), ((), ())), preferred_element_type=jnp.float32)


def finish_kernel(
    place_ref, basis_ref, near_ref, far_ref, weight_ref, w0, f1, f2, f3, b1, b2, b3, h1, h2,
    new_ref, step_ref, copy_ref, tiles, sems,
):
    z, fs, half = place_ref[0], place_ref[1], place_ref[2]
    near = near_ref[...].astype(jnp.float32)
    far = far_ref[...].astype(jnp.float32)
    energy = jnp.sum(near * near + far * far)
    spread = jnp.sqrt(jnp.full((1, 128), energy / (2 * near.shape[0] * near.shape[1]), jnp.float32))
    scale = (-1.0 / (spread + 1e-06))[:, :1]
    rank = near.shape[1]
    low, high = basis_ref[:, :rank], basis_ref[:, rank:]
    is_low = half == 0
    mine = jnp.where(is_low, low, high)
    other = jnp.where(is_low, high, low)

    def step_of(start, count):
        rows = pl.ds(pl.multiple_of(start, count), count)
        return (product(mine, near_ref[rows, :]) + product(other, far_ref[rows, :])) * scale

    step = step_of(fs * 64, 64)
    step_ref[...] = step
    new_ref[...] = weight_ref[...] + step
    copies = []
    for k, block in enumerate((w0, f1, f2, f3, None, b3, b2, b1)):
        at = (z + 8 - k) % 8
        wide = step_of(at * 256, 256)
        slot = k
        if block is None:
            part = wide.shape[0] // 2
            tiles[slot, :part] = (h1[...].astype(jnp.float32) + wide[:part]).astype(jnp.bfloat16)
            tiles[slot, part:] = (h2[...].astype(jnp.float32) + wide[part:]).astype(jnp.bfloat16)
        else:
            tiles[slot] = (block[...].astype(jnp.float32) + wide).astype(jnp.bfloat16)
        copy = pltpu.make_async_copy(
            tiles.at[slot], copy_ref.at[:, pl.ds(pl.multiple_of(at * 256, 256), 256)], sems.at[slot]
        )
        copy.start()
        copies.append(copy)
    for copy in copies:
        copy.wait()


def finish(place, basis, near, far, weight, blocks):
    vmem = pl.BlockSpec(memory_space=pltpu.VMEM)
    rows = basis.shape[0]
    model = near.shape[0]
    return pl.pallas_call(
        finish_kernel,
        in_specs=[pl.BlockSpec(memory_space=pltpu.SMEM)] + [vmem] * (4 + len(blocks)),
        out_specs=[vmem, vmem, pl.BlockSpec(memory_space=pl.ANY)],
        out_shape=[
            jax.ShapeDtypeStruct(weight.shape, jnp.float32),
            jax.ShapeDtypeStruct(weight.shape, jnp.float32),
            jax.ShapeDtypeStruct((rows, model), jnp.bfloat16),
        ],
        scratch_shapes=[pltpu.VMEM((8, rows, model // 8), jnp.bfloat16), pltpu.SemaphoreType.DMA((8,))],
        name="finish",
    )(place, basis, near, far, weight, *blocks)


def body(first_mix, second_mix, lambda_head, head_gain, out_cotangent, basis, weight, first_moment, second_moment):
    z, y, x, tp = (lax.axis_index(name).astype(jnp.int32) for name in ("z", "y", "x", "tp"))
    lead = weight.shape[0] // 2

    packed = jnp.concatenate([weight[:lead], weight[lead:]], axis=1).astype(jnp.bfloat16)
    around = [shift(packed, "y", hops) for hops in (1, 3, 2)]
    w0 = widen(y[None], packed, *around)
    f1, b1 = shift(w0, "z", 1), shift(w0, "z", -1)
    f2, b2 = shift(f1, "z", 1), shift(b1, "z", -1)
    f3, b3 = shift(f2, "z", 1), shift(b2, "z", -1)
    h1, h2 = shift(f3[:lead], "z", 1), shift(b3[lead:], "z", -1)

    own, sent = reduced_parts(tp[None], lambda_head, first_mix, second_mix, head_gain, basis)
    reduced = (own + swap_cores(sent).astype(jnp.float32)).astype(jnp.bfloat16)
    partial = lax.dot_general(
        out_cotangent, reduced, (((0,), (0,)), ((), ())), preferred_element_type=jnp.float32
    ).astype(jnp.bfloat16)
    rank = partial.shape[1]
    pieces = lax.all_to_all(partial.reshape(128, 16, rank), FS_REP, 0, 0, tiled=True)
    piece = jnp.sum(pieces.astype(jnp.float32), axis=0)

    def moments(projected, first, second):
        first_new = BETA_FIRST * first + (1.0 - BETA_FIRST) * projected
        second_new = BETA_SECOND * second + (1.0 - BETA_SECOND) * projected * projected
        return first_new, second_new

    first_16 = lax.dynamic_slice_in_dim(first_moment, x * 16, 16, 0)
    second_16 = lax.dynamic_slice_in_dim(second_moment, x * 16, 16, 0)
    first_piece, second_piece = moments(piece, first_16, second_16)
    direction = (first_piece / (jnp.sqrt(second_piece) + 1e-08)).astype(jnp.bfloat16)
    near = lax.all_to_all(
        jnp.broadcast_to(direction[None], (128, 16, rank)), FS_REP, 0, 0, tiled=True
    ).reshape(2048, rank)
    far = swap_cores(near)
    projected = lax.all_to_all(
        jnp.broadcast_to(piece[None], (4, 16, rank)), "x", 0, 0, tiled=True
    ).reshape(64, rank)
    first_new, second_new = moments(projected, first_moment, second_moment)
    place = jnp.stack([z, z * 4 + y, tp])
    weight_new, step_out, weight_copy = finish(
        place, basis, near, far, weight, (w0, f1, f2, f3, b1, b2, b3, h1, h2)
    )
    return (weight_new, weight_copy, step_out, first_new, second_new)


def solution(mesh):
    finer = Mesh(
        mesh.devices.reshape(8, 4, mesh.shape["rep"], mesh.shape["tp"]),
        ("z", "y", "x", "tp"),
    )
    return jax.shard_map(
        body,
        mesh=finer,
        in_specs=(
            P(FS_REP, "tp"),
            P(FS_REP, "tp"),
            P("tp"),
            P(),
            P(FS_REP, None),
            P("tp", None),
            P("tp", FS),
            P(FS, "tp"),
            P(FS, "tp"),
        ),
        out_specs=(P("tp", FS), P("tp", None), P("tp", FS), P(FS, "tp"), P(FS, "tp")),
        check_vma=False,
    )
```

```python
import jax
import jax.numpy as jnp
from jax import lax
from jax.experimental import pallas as pl
from jax.experimental.pallas import tpu as pltpu
from jax.sharding import Mesh
from jax.sharding import PartitionSpec as P

OUT_SCALE = 0.8
BETA_FIRST = 0.9
BETA_SECOND = 0.95
FS = ("z", "y")
FS_REP = ("z", "y", "x")
SMEM = pl.BlockSpec(memory_space=pltpu.SMEM)
VMEM = pl.BlockSpec(memory_space=pltpu.VMEM)
MIB = 1024 * 1024


def shift(array, axis, hops):
    count = lax.axis_size(axis)
    return lax.ppermute(array, axis, [(i, (i + hops) % count) for i in range(count)])


def swap_cores(array):
    return lax.ppermute(array, "tp", [(0, 1), (1, 0)])


def dot(left, right, left_dim, right_dim):
    return lax.dot_general(
        left, right, (((left_dim,), (right_dim,)), ((), ())), preferred_element_type=jnp.float32
    )


def limit(mib):
    return pltpu.CompilerParams(vmem_limit_bytes=mib * MIB)


def heads_kernel(place_ref, lam_ref, first_ref, second_ref, gain_ref, basis_ref, own_ref, sent_ref):
    width = gain_ref.shape[1]
    gain = gain_ref[...] * OUT_SCALE
    total = None
    for head in range(first_ref.shape[1] // width):
        cols = slice(head * width, (head + 1) * width)
        mixture = first_ref[:, cols].astype(jnp.float32) - lam_ref[head] * second_ref[:, cols].astype(jnp.float32)
        inverse = lax.rsqrt(jnp.mean(mixture * mixture, axis=-1, keepdims=True) + 1e-06)
        normed = (mixture * inverse * gain).astype(jnp.bfloat16)
        term = jnp.dot(normed, basis_ref[cols, :], preferred_element_type=jnp.float32)
        total = term if total is None else total + term
    half = total.shape[1] // 2
    low, high = total[:, :half], total[:, half:]
    is_low = place_ref[3] == 0
    own_ref[...] = jnp.where(is_low, low, high)
    sent_ref[...] = jnp.where(is_low, high, low).astype(jnp.bfloat16)


def heads(place, lambda_head, first_mix, second_mix, head_gain, basis):
    tokens, values = first_mix.shape
    rank = basis.shape[1]
    tile = 256
    return pl.pallas_call(
        heads_kernel,
        grid=(tokens // tile,),
        in_specs=[
            SMEM,
            SMEM,
            pl.BlockSpec((tile, values), lambda i: (i, 0)),
            pl.BlockSpec((tile, values), lambda i: (i, 0)),
            pl.BlockSpec((1, head_gain.shape[0]), lambda i: (0, 0)),
            pl.BlockSpec((values, rank), lambda i: (0, 0)),
        ],
        out_specs=[pl.BlockSpec((tile, rank // 2), lambda i: (i, 0))] * 2,
        out_shape=[
            jax.ShapeDtypeStruct((tokens, rank // 2), jnp.float32),
            jax.ShapeDtypeStruct((tokens, rank // 2), jnp.bfloat16),
        ],
        compiler_params=limit(16),
        name="heads",
    )(place, lambda_head, first_mix, second_mix, head_gain[None, :], basis)


def widen_kernel(place_ref, own_ref, one_ref, two_ref, three_ref, out_ref, slots):
    y = place_ref[1]
    slots[y] = own_ref[...].astype(jnp.float32)
    slots[(y + 3) % 4] = one_ref[...].astype(jnp.float32)
    slots[(y + 2) % 4] = two_ref[...].astype(jnp.float32)
    slots[(y + 1) % 4] = three_ref[...].astype(jnp.float32)
    rows = slots.shape[0] * slots.shape[1]
    out_ref[...] = slots[...].reshape(rows, slots.shape[2]).T.astype(jnp.bfloat16)


def widen(place, blocks):
    rows, cols = blocks[0].shape
    return pl.pallas_call(
        widen_kernel,
        in_specs=[SMEM] + [VMEM] * 4,
        out_specs=VMEM,
        out_shape=jax.ShapeDtypeStruct((cols, 4 * rows), jnp.bfloat16),
        scratch_shapes=[pltpu.VMEM((4, rows, cols), jnp.float32)],
        compiler_params=limit(8),
        name="widen",
    )(place, *blocks)


def gradient_kernel(place_ref, own_ref, far_ref, cot_ref, out0, out1, out2, out3, parts):
    x = place_ref[2]
    reduced = (own_ref[...] + far_ref[...].astype(jnp.float32)).T.astype(jnp.bfloat16)
    wide = 512
    for at in range(cot_ref.shape[1] // wide):
        block = dot(reduced, cot_ref[:, at * wide : (at + 1) * wide], 1, 0).T.astype(jnp.bfloat16)
        parts[at * 8 : (at + 1) * 8] = block.reshape(8, 4, 16, block.shape[1])
    for hops, out in enumerate((out0, out1, out2, out3)):
        out[...] = parts[:, (x + hops) % 4]


def gradient(place, own, far, cot):
    rank = own.shape[1]
    return pl.pallas_call(
        gradient_kernel,
        in_specs=[SMEM] + [VMEM] * 3,
        out_specs=[VMEM] * 4,
        out_shape=[jax.ShapeDtypeStruct((32, 16, rank), jnp.bfloat16)] * 4,
        scratch_shapes=[pltpu.VMEM((32, 4, 16, rank), jnp.bfloat16)],
        compiler_params=limit(16),
        name="gradient",
    )(place, own, far, cot)


def moments(projected, first, second):
    first_new = BETA_FIRST * first + (1.0 - BETA_FIRST) * projected
    second_new = BETA_SECOND * second + (1.0 - BETA_SECOND) * projected * projected
    return first_new, second_new


def update_kernel(place_ref, pieces_ref, first_ref, second_ref, piece_ref, copies_ref):
    rows = pl.ds(pl.multiple_of(place_ref[2] * 16, 16), 16)
    piece = jnp.sum(pieces_ref[...].astype(jnp.float32), axis=0)
    piece_ref[...] = piece
    first_new, second_new = moments(piece, first_ref[rows, :], second_ref[rows, :])
    direction = (first_new / (jnp.sqrt(second_new) + 1e-08)).astype(jnp.bfloat16)
    copies_ref[...] = jnp.broadcast_to(direction[None], copies_ref.shape)


def update(place, pieces, first, second):
    return pl.pallas_call(
        update_kernel,
        in_specs=[SMEM] + [VMEM] * 3,
        out_specs=[VMEM] * 2,
        out_shape=[
            jax.ShapeDtypeStruct(pieces.shape[1:], jnp.float32),
            jax.ShapeDtypeStruct(pieces.shape, jnp.bfloat16),
        ],
        compiler_params=limit(4),
        name="update",
    )(place, pieces, first, second)


def finish_kernel(
    place_ref, basis_ref, weight_ref, first_ref, second_ref,
    p0, p1, p2, p3, n0, n1, n2, n3, m0, m1, m2, m3,
    w0, f1, f2, f3, b1, b2, b3, h1, h2,
    new_ref, step_ref, copy_ref, first_out, second_out,
    rows_ref, tiles, sems,
):
    z, y, x = place_ref[0], place_ref[1], place_ref[2]
    is_low = place_ref[3] == 0
    energy = jnp.float32(0.0)
    for hops, (piece, near_ref, far_ref) in enumerate(
        ((p0, n0, m0), (p1, n1, m1), (p2, n2, m2), (p3, n3, m3))
    ):
        source = (x + 4 - hops) % 4
        rows = pl.ds(pl.multiple_of(source * 16, 16), 16)
        first_new, second_new = moments(piece[...], first_ref[rows, :], second_ref[rows, :])
        first_out[rows, :] = first_new
        second_out[rows, :] = second_new
        near, far = near_ref[...], far_ref[...]
        rank = near.shape[2]
        rows_ref[:, source, :, :rank] = jnp.where(is_low, near, far)
        rows_ref[:, source, :, rank:] = jnp.where(is_low, far, near)
        wide_near, wide_far = near.astype(jnp.float32), far.astype(jnp.float32)
        energy += jnp.sum(wide_near * wide_near + wide_far * wide_far)
    count = rows_ref.shape[0] * rows_ref.shape[1] * rows_ref.shape[2] * rows_ref.shape[3]
    spread = jnp.sqrt(jnp.full((1, 128), energy / count, jnp.float32))
    scale = (-1.0 / (spread + 1e-06))[:, :1]
    basis = basis_ref[...]

    step = dot(rows_ref[z * 4 + y].reshape(64, basis.shape[1]), basis, 1, 1) * scale
    step_ref[...] = step
    new_ref[...] = weight_ref[...] + step
    copies = []
    for k, block in enumerate((w0, f1, f2, f3, b3, b2, b1, None)):
        at = (z + 8 - (k if k < 4 else k + 1 if block is not None else 4)) % 8
        part = rows_ref[pl.ds(at * 4, 4)].reshape(256, basis.shape[1])
        wide = dot(basis, part, 1, 1) * scale
        if block is None:
            lead = wide.shape[0] // 2
            tiles[k, :lead] = (h1[...].astype(jnp.float32) + wide[:lead]).astype(jnp.bfloat16)
            tiles[k, lead:] = (h2[...].astype(jnp.float32) + wide[lead:]).astype(jnp.bfloat16)
        else:
            tiles[k] = (block[...].astype(jnp.float32) + wide).astype(jnp.bfloat16)
        copy = pltpu.make_async_copy(
            tiles.at[k], copy_ref.at[:, pl.ds(pl.multiple_of(at * 256, 256), 256)], sems.at[k]
        )
        copy.start()
        copies.append(copy)
    for copy in copies:
        copy.wait()


def finish(place, basis, weight, first, second, pieces, near, far, blocks):
    values, rank = basis.shape
    like = lambda array: jax.ShapeDtypeStruct(array.shape, jnp.float32)
    return pl.pallas_call(
        finish_kernel,
        in_specs=[SMEM] + [VMEM] * (4 + 12 + len(blocks)),
        out_specs=[VMEM, VMEM, pl.BlockSpec(memory_space=pl.ANY), VMEM, VMEM],
        out_shape=[
            like(weight),
            like(weight),
            jax.ShapeDtypeStruct((values, 2048), jnp.bfloat16),
            like(first),
            like(second),
        ],
        scratch_shapes=[
            pltpu.VMEM((32, 4, 16, rank), jnp.bfloat16),
            pltpu.VMEM((8, values, 256), jnp.bfloat16),
            pltpu.SemaphoreType.DMA((8,)),
        ],
        compiler_params=limit(24),
        name="finish",
    )(place, basis, weight, first, second, *pieces, *near, *far, *blocks)


def to_all(array):
    return lax.all_to_all(array, FS, 0, 0, tiled=True)


def chain(first_mix, second_mix, lambda_head, head_gain, out_cotangent, basis, weight, first_moment, second_moment):
    place = jnp.stack([lax.axis_index(name).astype(jnp.int32) for name in ("z", "y", "x", "tp")])
    turned = weight.T
    lead = turned.shape[1] // 2

    narrow = turned.astype(jnp.bfloat16)
    w0 = widen(place, [narrow] + [shift(narrow, "y", hops) for hops in (1, 2, 3)])
    f1, b1 = shift(w0, "z", 1), shift(w0, "z", -1)
    f2, b2 = shift(f1, "z", 1), shift(b1, "z", -1)
    f3, b3 = shift(f2, "z", 1), shift(b2, "z", -1)
    h1, h2 = shift(f3[:lead], "z", 1), shift(b3[lead:], "z", -1)

    own, sent = heads(place, lambda_head, first_mix, second_mix, head_gain, basis)
    parts = gradient(place, own, swap_cores(sent), out_cotangent)
    arrived = [shift(parts[hops], "x", hops) for hops in (1, 2, 3)]
    summed = parts[0].astype(jnp.float32)
    for part in arrived:
        summed = summed + part.astype(jnp.float32)
    summed = summed.astype(jnp.bfloat16)
    piece, copies = update(place, to_all(summed), first_moment, second_moment)
    pieces = [piece] + [shift(piece, "x", hops) for hops in (1, 2, 3)]
    quarter = to_all(copies)
    near = [quarter] + [shift(quarter, "x", hops) for hops in (1, 2, 3)]
    far = [swap_cores(array) for array in near]
    weight_new, step_out, weight_copy, first_new, second_new = finish(
        place, basis, turned, first_moment, second_moment, pieces, near, far, (w0, f1, f2, f3, b1, b2, b3, h1, h2)
    )
    return (weight_new.T, weight_copy, step_out.T, first_new, second_new)


def solution(mesh):
    finer = Mesh(
        mesh.devices.reshape(8, 4, mesh.shape["rep"], mesh.shape["tp"]),
        ("z", "y", "x", "tp"),
    )
    return jax.shard_map(
        chain,
        mesh=finer,
        in_specs=(
            P(FS_REP, "tp"),
            P(FS_REP, "tp"),
            P("tp"),
            P(),
            P(FS_REP, None),
            P("tp", None),
            P("tp", FS),
            P(FS, "tp"),
            P(FS, "tp"),
        ),
        out_specs=(P("tp", FS), P("tp", None), P("tp", FS), P(FS, "tp"), P(FS, "tp")),
        check_vma=False,
    )
```

```python
import jax
import jax.numpy as jnp
from jax import lax
from jax.experimental import pallas as pl
from jax.experimental.pallas import tpu as pltpu
from jax.sharding import Mesh
from jax.sharding import PartitionSpec as P

OUT_SCALE = 0.8
BETA_FIRST = 0.9
BETA_SECOND = 0.95
FS = ("z", "y")
FS_REP = ("z", "y", "x")
SMEM = pl.BlockSpec(memory_space=pltpu.SMEM)
VMEM = pl.BlockSpec(memory_space=pltpu.VMEM)
HBM = pl.BlockSpec(memory_space=pltpu.HBM)
MIB = 1024 * 1024


def in_hbm(*arrays):
    return [pltpu.with_memory_space_constraint(array, pltpu.HBM) for array in arrays]


def in_vmem(*arrays):
    return [pltpu.with_memory_space_constraint(array, pltpu.VMEM) for array in arrays]


def shift(array, axis, hops):
    count = lax.axis_size(axis)
    return lax.ppermute(array, axis, [(i, (i + hops) % count) for i in range(count)])


def swap_cores(array):
    return lax.ppermute(array, "tp", [(0, 1), (1, 0)])


def dot(left, right, left_dim, right_dim):
    return lax.dot_general(
        left, right, (((left_dim,), (right_dim,)), ((), ())), preferred_element_type=jnp.float32
    )


def limit(mib):
    return pltpu.CompilerParams(vmem_limit_bytes=mib * MIB)


def heads_kernel(
    place_ref, lam_hbm, first_hbm, second_hbm, gain_hbm, basis_hbm, weight_hbm,
    own_ref, sent_ref, narrow_ref, first_ref, second_ref, basis_ref, lam_ref, gain_ref, weight_ref, sems,
):
    tokens, values = first_ref.shape
    width = gain_ref.shape[1]
    tile = tokens // 3

    def fetch(source, target, slot):
        copy = pltpu.make_async_copy(source, target, sems.at[slot])
        copy.start()
        return copy

    fixed = [fetch(lam_hbm, lam_ref, 0), fetch(gain_hbm, gain_ref, 1)]
    moving = []
    for step in range(3):
        rows = pl.ds(step * tile, tile)
        moving.append(
            [
                fetch(first_hbm.at[rows], first_ref.at[rows], 4 + 2 * step),
                fetch(second_hbm.at[rows], second_ref.at[rows], 5 + 2 * step),
            ]
        )
        if step == 0:
            fixed.append(fetch(basis_hbm, basis_ref, 2))
    last = fetch(weight_hbm, weight_ref, 3)
    for copy in fixed[:2]:
        copy.wait()
    gain = gain_ref[...] * OUT_SCALE
    is_low = place_ref[3] == 0
    for step in range(3):
        rows = pl.ds(step * tile, tile)
        for copy in moving[step]:
            copy.wait()
        if step == 0:
            fixed[2].wait()
        total = None
        for head in range(values // width):
            cols = slice(head * width, (head + 1) * width)
            first = first_ref[rows, cols].astype(jnp.float32)
            second = second_ref[rows, cols].astype(jnp.float32)
            mixture = first - lam_ref[:, head : head + 1] * second
            inverse = lax.rsqrt(jnp.mean(mixture * mixture, axis=-1, keepdims=True) + 1e-06)
            normed = (mixture * inverse * gain).astype(jnp.bfloat16)
            term = jnp.dot(normed, basis_ref[cols, :], preferred_element_type=jnp.float32)
            total = term if total is None else total + term
        half = total.shape[1] // 2
        low, high = total[:, :half], total[:, half:]
        own_ref[rows, :] = jnp.where(is_low, low, high)
        sent_ref[rows, :] = jnp.where(is_low, high, low).astype(jnp.bfloat16)
    last.wait()
    narrow_ref[...] = weight_ref[...].astype(jnp.bfloat16)


def heads(place, lambda_head, first_mix, second_mix, head_gain, basis, weight):
    tokens, values = first_mix.shape
    half = basis.shape[1] // 2
    lam, gain = lambda_head[None, :], head_gain[None, :]
    return pl.pallas_call(
        heads_kernel,
        in_specs=[SMEM] + [HBM] * 6,
        out_specs=[VMEM] * 3,
        out_shape=[
            jax.ShapeDtypeStruct((tokens, half), jnp.float32),
            jax.ShapeDtypeStruct((tokens, half), jnp.bfloat16),
            jax.ShapeDtypeStruct(weight.shape, jnp.bfloat16),
        ],
        scratch_shapes=[
            pltpu.VMEM((tokens, values), jnp.bfloat16),
            pltpu.VMEM((tokens, values), jnp.bfloat16),
            pltpu.VMEM(basis.shape, jnp.bfloat16),
            pltpu.VMEM(lam.shape, jnp.float32),
            pltpu.VMEM(gain.shape, jnp.float32),
            pltpu.VMEM(weight.shape, jnp.float32),
            pltpu.SemaphoreType.DMA((10,)),
        ],
        compiler_params=limit(12),
        name="heads",
    )(place, *in_hbm(lam, first_mix, second_mix, gain, basis, weight))


def widen_kernel(place_ref, own_ref, one_ref, two_ref, three_ref, out_ref, slots):
    y = place_ref[1]
    slots[y] = own_ref[...].astype(jnp.float32)
    slots[(y + 3) % 4] = one_ref[...].astype(jnp.float32)
    slots[(y + 2) % 4] = two_ref[...].astype(jnp.float32)
    slots[(y + 1) % 4] = three_ref[...].astype(jnp.float32)
    rows = slots.shape[0] * slots.shape[1]
    out_ref[...] = slots[...].reshape(rows, slots.shape[2]).T.astype(jnp.bfloat16)


def widen(place, blocks):
    rows, cols = blocks[0].shape
    return pl.pallas_call(
        widen_kernel,
        in_specs=[SMEM] + [VMEM] * 4,
        out_specs=VMEM,
        out_shape=jax.ShapeDtypeStruct((cols, 4 * rows), jnp.bfloat16),
        scratch_shapes=[pltpu.VMEM((4, rows, cols), jnp.float32)],
        compiler_params=limit(8),
        name="widen",
    )(place, *blocks)


def gradient_kernel(own_ref, far_ref, cot_ref, out_hbm, parts, sems):
    reduced = (own_ref[...] + far_ref[...].astype(jnp.float32)).T.astype(jnp.bfloat16)
    wide = 512
    copies = []
    for at in range(cot_ref.shape[1] // wide):
        block = dot(reduced, cot_ref[:, at * wide : (at + 1) * wide], 1, 0).T.astype(jnp.bfloat16)
        for z in range(2):
            rows = block[z * 256 : (z + 1) * 256]
            parts[:, at * 2 + z] = rows.reshape(16, 16, rows.shape[1])
        pair = pl.ds(at * 2, 2)
        copy = pltpu.make_async_copy(parts.at[:, pair], out_hbm.at[:, pair], sems.at[at])
        copy.start()
        copies.append(copy)
    for copy in copies:
        copy.wait()


def gradient(own, far, cot):
    shape = (16, 8, 16, own.shape[1])
    return pl.pallas_call(
        gradient_kernel,
        in_specs=[VMEM] * 3,
        out_specs=HBM,
        out_shape=pltpu.HBM(shape, jnp.bfloat16),
        scratch_shapes=[pltpu.VMEM(shape, jnp.bfloat16), pltpu.SemaphoreType.DMA((4,))],
        compiler_params=limit(8),
        name="gradient",
    )(own, far, cot)


def fold_kernel(parts_ref, out_hbm, sums, sem):
    sums[...] = jnp.sum(parts_ref[...].astype(jnp.float32), axis=0).astype(jnp.bfloat16)
    copy = pltpu.make_async_copy(sums, out_hbm, sem)
    copy.start()
    copy.wait()


def fold(parts):
    shape = parts.shape[1:]
    return pl.pallas_call(
        fold_kernel,
        in_specs=[VMEM],
        out_specs=HBM,
        out_shape=pltpu.HBM(shape, jnp.bfloat16),
        scratch_shapes=[pltpu.VMEM(shape, jnp.bfloat16), pltpu.SemaphoreType.DMA],
        compiler_params=limit(4),
        name="fold",
    )(parts)


def copy_to_all(source, target, sems):
    copies = []
    for slot in range(target.shape[0]):
        copy = pltpu.make_async_copy(source, target.at[slot], sems.at[slot])
        copy.start()
        copies.append(copy)
    for copy in copies:
        copy.wait()


def copies_of(array, count):
    return pl.pallas_call(
        copy_to_all,
        in_specs=[VMEM],
        out_specs=HBM,
        out_shape=pltpu.HBM((count, *array.shape), array.dtype),
        scratch_shapes=[pltpu.SemaphoreType.DMA((count,))],
        compiler_params=limit(4),
        name="copies",
    )(array)


def moments(projected, first, second):
    first_new = BETA_FIRST * first + (1.0 - BETA_FIRST) * projected
    second_new = BETA_SECOND * second + (1.0 - BETA_SECOND) * projected * projected
    return first_new, second_new


def update_kernel(place_ref, pieces_ref, first_ref, second_ref, piece_ref, copies_hbm, direction_ref, sems):
    rows = pl.ds(pl.multiple_of(place_ref[2] * 16, 16), 16)
    piece = jnp.sum(pieces_ref[...].astype(jnp.float32), axis=0)
    piece_ref[...] = piece
    first_new, second_new = moments(piece, first_ref[rows, :], second_ref[rows, :])
    direction_ref[...] = (first_new / (jnp.sqrt(second_new) + 1e-08)).astype(jnp.bfloat16)
    copy_to_all(direction_ref, copies_hbm, sems)


def update(place, pieces, first, second):
    count, rows, rank = pieces.shape
    return pl.pallas_call(
        update_kernel,
        in_specs=[SMEM] + [VMEM] * 3,
        out_specs=[VMEM, HBM],
        out_shape=[
            jax.ShapeDtypeStruct((rows, rank), jnp.float32),
            pltpu.HBM(pieces.shape, jnp.bfloat16),
        ],
        scratch_shapes=[pltpu.VMEM((rows, rank), jnp.bfloat16), pltpu.SemaphoreType.DMA((count,))],
        compiler_params=limit(4),
        name="update",
    )(place, pieces, first, second)


def finish_kernel(
    place_ref, basis_hbm, weight_hbm, first_hbm, second_hbm, p0, p1, p2, p3, near_ref, far_ref,
    w0, f1, f2, f3, b1, b2, b3, h1, h2,
    new_ref, step_ref, copy_ref, first_out, second_out,
    basis_ref, weight_ref, first_ref, second_ref, tiles, sems,
):
    fetched = []
    for slot, (source, target) in enumerate(
        ((basis_hbm, basis_ref), (weight_hbm, weight_ref), (first_hbm, first_ref), (second_hbm, second_ref))
    ):
        copy = pltpu.make_async_copy(source, target, sems.at[8 + slot])
        copy.start()
        fetched.append(copy)
    z, y, x = place_ref[0], place_ref[1], place_ref[2]
    is_low = place_ref[3] == 0
    near, far = near_ref[...].astype(jnp.float32), far_ref[...].astype(jnp.float32)
    energy = jnp.sum(near * near + far * far)
    count = 2 * near.shape[0] * near.shape[1] * near.shape[2] * near.shape[3]
    spread = jnp.sqrt(jnp.full((1, 128), energy / count, jnp.float32))
    scale = (-1.0 / (spread + 1e-06))[:, :1]
    for copy in fetched:
        copy.wait()
    basis = basis_ref[...]

    def rows_of(close, distant):
        close, distant = (array.reshape(-1, array.shape[-1]) for array in (close, distant))
        return jnp.concatenate(
            [jnp.where(is_low, close, distant), jnp.where(is_low, distant, close)], axis=1
        )

    copies = []
    for k, block in enumerate((w0, f1, f2, f3, b3, b2, b1, None)):
        at = (z + 8 - (k if k < 4 else k + 1 if block is not None else 4)) % 8
        wide = dot(basis, rows_of(near_ref[:, at], far_ref[:, at]), 1, 1) * scale
        if block is None:
            lead = wide.shape[0] // 2
            tiles[k, :lead] = (h1[...].astype(jnp.float32) + wide[:lead]).astype(jnp.bfloat16)
            tiles[k, lead:] = (h2[...].astype(jnp.float32) + wide[lead:]).astype(jnp.bfloat16)
        else:
            tiles[k] = (block[...].astype(jnp.float32) + wide).astype(jnp.bfloat16)
        copy = pltpu.make_async_copy(
            tiles.at[k], copy_ref.at[:, pl.ds(pl.multiple_of(at * 256, 256), 256)], sems.at[k]
        )
        copy.start()
        copies.append(copy)

    mine = pl.ds(y * 4, 4)
    step = dot(rows_of(near_ref[mine, z], far_ref[mine, z]), basis, 1, 1) * scale
    step_ref[...] = step
    new_ref[...] = weight_ref[...] + step
    for hops, piece in enumerate((p0, p1, p2, p3)):
        rows = pl.ds(pl.multiple_of((x + 4 - hops) % 4 * 16, 16), 16)
        first_new, second_new = moments(piece[...], first_ref[rows, :], second_ref[rows, :])
        first_out[rows, :] = first_new
        second_out[rows, :] = second_new
    for copy in copies:
        copy.wait()


def finish(place, basis, weight, first, second, pieces, near, far, blocks):
    values = basis.shape[0]
    like = lambda array: jax.ShapeDtypeStruct(array.shape, jnp.float32)
    return pl.pallas_call(
        finish_kernel,
        in_specs=[SMEM] + [HBM] * 4 + [VMEM] * (6 + len(blocks)),
        out_specs=[VMEM, VMEM, HBM, VMEM, VMEM],
        out_shape=[
            like(weight),
            like(weight),
            pltpu.HBM((values, 2048), jnp.bfloat16),
            like(first),
            like(second),
        ],
        scratch_shapes=[
            pltpu.VMEM(basis.shape, basis.dtype),
            pltpu.VMEM(weight.shape, weight.dtype),
            pltpu.VMEM(first.shape, first.dtype),
            pltpu.VMEM(second.shape, second.dtype),
            pltpu.VMEM((8, values, 256), jnp.bfloat16),
            pltpu.SemaphoreType.DMA((12,)),
        ],
        compiler_params=limit(16),
        name="finish",
    )(place, *in_hbm(basis, weight, first, second), *pieces, near, far, *in_vmem(*blocks))


def exchange(array, axes):
    return lax.all_to_all(array, axes, 0, 0, tiled=True)


def chain(first_mix, second_mix, lambda_head, head_gain, out_cotangent, basis, weight, first_moment, second_moment):
    place = jnp.stack([lax.axis_index(name).astype(jnp.int32) for name in ("z", "y", "x", "tp")])
    turned = weight.T
    own, sent, narrow = heads(place, lambda_head, first_mix, second_mix, head_gain, basis, turned)

    lead = turned.shape[1] // 2
    w0 = widen(place, [narrow] + [shift(narrow, "y", hops) for hops in (1, 2, 3)])
    f1, b1 = shift(w0, "z", 1), shift(w0, "z", -1)
    f2, b2 = shift(f1, "z", 1), shift(b1, "z", -1)
    f3, b3 = shift(f2, "z", 1), shift(b2, "z", -1)
    h1, h2 = shift(f3[:lead], "z", 1), shift(b3[lead:], "z", -1)

    parts = gradient(own, swap_cores(sent), out_cotangent)
    folded = fold(exchange(parts, ("y", "x")))
    piece, copies = update(place, exchange(folded, "z"), first_moment, second_moment)
    pieces = [piece] + [shift(piece, "x", hops) for hops in (1, 2, 3)]
    column = exchange(copies, "z")
    near = exchange(copies_of(column, 16), ("y", "x"))
    far = swap_cores(near)
    weight_new, step_out, weight_copy, first_new, second_new = finish(
        place, basis, turned, first_moment, second_moment, pieces, near, far, (w0, f1, f2, f3, b1, b2, b3, h1, h2)
    )
    return (weight_new.T, weight_copy, step_out.T, first_new, second_new)


def solution(mesh):
    finer = Mesh(
        mesh.devices.reshape(8, 4, mesh.shape["rep"], mesh.shape["tp"]),
        ("z", "y", "x", "tp"),
    )
    return jax.shard_map(
        chain,
        mesh=finer,
        in_specs=(
            P(FS_REP, "tp"),
            P(FS_REP, "tp"),
            P("tp"),
            P(),
            P(FS_REP, None),
            P("tp", None),
            P("tp", FS),
            P(FS, "tp"),
            P(FS, "tp"),
        ),
        out_specs=(P("tp", FS), P("tp", None), P("tp", FS), P(FS, "tp"), P(FS, "tp")),
        check_vma=False,
    )
```

```python
import jax
import jax.numpy as jnp
from jax import lax
from jax.experimental import pallas as pl
from jax.experimental.pallas import tpu as pltpu
from jax.sharding import Mesh
from jax.sharding import PartitionSpec as P

OUT_SCALE = 0.8
BETA_FIRST = 0.9
BETA_SECOND = 0.95
FS = ("z", "y")
FS_REP = ("z", "y", "x")
SMEM = pl.BlockSpec(memory_space=pltpu.SMEM)
VMEM = pl.BlockSpec(memory_space=pltpu.VMEM)
HBM = pl.BlockSpec(memory_space=pltpu.HBM)
MIB = 1024 * 1024


def in_hbm(*arrays):
    return [pltpu.with_memory_space_constraint(array, pltpu.HBM) for array in arrays]


def in_vmem(*arrays):
    return [pltpu.with_memory_space_constraint(array, pltpu.VMEM) for array in arrays]


def shift(array, axis, hops):
    count = lax.axis_size(axis)
    return lax.ppermute(array, axis, [(i, (i + hops) % count) for i in range(count)])


def swap_cores(array):
    return lax.ppermute(array, "tp", [(0, 1), (1, 0)])


def dot(left, right, left_dim, right_dim):
    return lax.dot_general(
        left, right, (((left_dim,), (right_dim,)), ((), ())), preferred_element_type=jnp.float32
    )


def limit(mib):
    return pltpu.CompilerParams(vmem_limit_bytes=mib * MIB)


def heads_kernel(
    place_ref, lam_hbm, first_hbm, second_hbm, gain_hbm, basis_hbm,
    own_ref, sent_ref, first_ref, second_ref, basis_ref, lam_ref, gain_ref, sems,
):
    tokens, values = first_ref.shape
    width = gain_ref.shape[1]
    tile = tokens // 3

    def fetch(source, target, slot):
        copy = pltpu.make_async_copy(source, target, sems.at[slot])
        copy.start()
        return copy

    fixed = [fetch(lam_hbm, lam_ref, 0), fetch(gain_hbm, gain_ref, 1)]
    moving = []
    for step in range(3):
        rows = pl.ds(step * tile, tile)
        moving.append(
            [
                fetch(first_hbm.at[rows], first_ref.at[rows], 3 + 2 * step),
                fetch(second_hbm.at[rows], second_ref.at[rows], 4 + 2 * step),
            ]
        )
        if step == 0:
            fixed.append(fetch(basis_hbm, basis_ref, 2))
    for copy in fixed[:2]:
        copy.wait()
    gain = gain_ref[...] * OUT_SCALE
    is_low = place_ref[3] == 0
    for step in range(3):
        rows = pl.ds(step * tile, tile)
        for copy in moving[step]:
            copy.wait()
        if step == 0:
            fixed[2].wait()
        total = None
        for head in range(values // width):
            cols = slice(head * width, (head + 1) * width)
            first = first_ref[rows, cols].astype(jnp.float32)
            second = second_ref[rows, cols].astype(jnp.float32)
            mixture = first - lam_ref[:, head : head + 1] * second
            inverse = lax.rsqrt(jnp.mean(mixture * mixture, axis=-1, keepdims=True) + 1e-06)
            normed = (mixture * inverse * gain).astype(jnp.bfloat16)
            term = jnp.dot(normed, basis_ref[cols, :], preferred_element_type=jnp.float32)
            total = term if total is None else total + term
        half = total.shape[1] // 2
        low, high = total[:, :half], total[:, half:]
        own_ref[rows, :] = jnp.where(is_low, low, high)
        sent_ref[rows, :] = jnp.where(is_low, high, low).astype(jnp.bfloat16)


def heads(place, lambda_head, first_mix, second_mix, head_gain, basis):
    tokens, values = first_mix.shape
    half = basis.shape[1] // 2
    lam, gain = lambda_head[None, :], head_gain[None, :]
    return pl.pallas_call(
        heads_kernel,
        in_specs=[SMEM] + [HBM] * 5,
        out_specs=[VMEM] * 2,
        out_shape=[
            jax.ShapeDtypeStruct((tokens, half), jnp.float32),
            jax.ShapeDtypeStruct((tokens, half), jnp.bfloat16),
        ],
        scratch_shapes=[
            pltpu.VMEM((tokens, values), jnp.bfloat16),
            pltpu.VMEM((tokens, values), jnp.bfloat16),
            pltpu.VMEM(basis.shape, jnp.bfloat16),
            pltpu.VMEM(lam.shape, jnp.float32),
            pltpu.VMEM(gain.shape, jnp.float32),
            pltpu.SemaphoreType.DMA((9,)),
        ],
        compiler_params=limit(12),
        name="heads",
    )(place, *in_hbm(lam, first_mix, second_mix, gain, basis))


def widen_kernel(place_ref, own_ref, one_ref, two_ref, three_ref, out_ref, slots):
    y = place_ref[1]
    slots[y] = own_ref[...].astype(jnp.float32)
    slots[(y + 3) % 4] = one_ref[...].astype(jnp.float32)
    slots[(y + 2) % 4] = two_ref[...].astype(jnp.float32)
    slots[(y + 1) % 4] = three_ref[...].astype(jnp.float32)
    rows = slots.shape[0] * slots.shape[1]
    out_ref[...] = slots[...].reshape(rows, slots.shape[2]).T.astype(jnp.bfloat16)


def widen(place, blocks):
    rows, cols = blocks[0].shape
    return pl.pallas_call(
        widen_kernel,
        in_specs=[SMEM] + [VMEM] * 4,
        out_specs=VMEM,
        out_shape=jax.ShapeDtypeStruct((cols, 4 * rows), jnp.bfloat16),
        scratch_shapes=[pltpu.VMEM((4, rows, cols), jnp.float32)],
        compiler_params=limit(8),
        name="widen",
    )(place, *blocks)


def gradient_kernel(own_ref, far_ref, cot_ref, out_hbm, parts, sems):
    reduced = (own_ref[...] + far_ref[...].astype(jnp.float32)).T.astype(jnp.bfloat16)
    wide = 512
    copies = []
    for at in range(cot_ref.shape[1] // wide):
        block = dot(reduced, cot_ref[:, at * wide : (at + 1) * wide], 1, 0).T.astype(jnp.bfloat16)
        for z in range(2):
            rows = block[z * 256 : (z + 1) * 256]
            parts[:, at * 2 + z] = rows.reshape(16, 16, rows.shape[1])
        pair = pl.ds(at * 2, 2)
        copy = pltpu.make_async_copy(parts.at[:, pair], out_hbm.at[:, pair], sems.at[at])
        copy.start()
        copies.append(copy)
    for copy in copies:
        copy.wait()


def gradient(own, far, cot):
    shape = (16, 8, 16, own.shape[1])
    return pl.pallas_call(
        gradient_kernel,
        in_specs=[VMEM] * 3,
        out_specs=HBM,
        out_shape=pltpu.HBM(shape, jnp.bfloat16),
        scratch_shapes=[pltpu.VMEM(shape, jnp.bfloat16), pltpu.SemaphoreType.DMA((4,))],
        compiler_params=limit(8),
        name="gradient",
    )(own, far, cot)


def fold_kernel(parts_ref, out_hbm, sums, sem):
    sums[...] = jnp.sum(parts_ref[...].astype(jnp.float32), axis=0).astype(jnp.bfloat16)
    copy = pltpu.make_async_copy(sums, out_hbm, sem)
    copy.start()
    copy.wait()


def fold(parts):
    shape = parts.shape[1:]
    return pl.pallas_call(
        fold_kernel,
        in_specs=[VMEM],
        out_specs=HBM,
        out_shape=pltpu.HBM(shape, jnp.bfloat16),
        scratch_shapes=[pltpu.VMEM(shape, jnp.bfloat16), pltpu.SemaphoreType.DMA],
        compiler_params=limit(4),
        name="fold",
    )(parts)


def copy_to_all(source, target, sems):
    copies = []
    for slot in range(target.shape[0]):
        copy = pltpu.make_async_copy(source, target.at[slot], sems.at[slot])
        copy.start()
        copies.append(copy)
    for copy in copies:
        copy.wait()


def letters_kernel(column_ref, extra_ref, out_hbm, sems):
    rows = column_ref.shape[0]
    copies = []
    for slot in range(out_hbm.shape[0]):
        for part, (source, target) in enumerate(((column_ref, pl.ds(0, rows)), (extra_ref, pl.ds(rows, 2)))):
            copy = pltpu.make_async_copy(source, out_hbm.at[slot, target], sems.at[slot, part])
            copy.start()
            copies.append(copy)
    for copy in copies:
        copy.wait()


def letters(column, extra, count):
    blocks, rows, rank = column.shape
    return pl.pallas_call(
        letters_kernel,
        in_specs=[VMEM] * 2,
        out_specs=HBM,
        out_shape=pltpu.HBM((count, blocks + 2, rows, rank), column.dtype),
        scratch_shapes=[pltpu.SemaphoreType.DMA((count, 2))],
        compiler_params=limit(4),
        name="letters",
    )(column, extra)


def moments(projected, first, second):
    first_new = BETA_FIRST * first + (1.0 - BETA_FIRST) * projected
    second_new = BETA_SECOND * second + (1.0 - BETA_SECOND) * projected * projected
    return first_new, second_new


def update_kernel(place_ref, pieces_ref, first_ref, second_ref, piece_ref, copies_hbm, direction_ref, sems):
    rows = pl.ds(pl.multiple_of(place_ref[2] * 16, 16), 16)
    piece = jnp.sum(pieces_ref[...].astype(jnp.float32), axis=0)
    high = piece.astype(jnp.bfloat16)
    piece_ref[0] = high
    piece_ref[1] = (piece - high.astype(jnp.float32)).astype(jnp.bfloat16)
    first_new, second_new = moments(piece, first_ref[rows, :], second_ref[rows, :])
    direction_ref[...] = (first_new / (jnp.sqrt(second_new) + 1e-08)).astype(jnp.bfloat16)
    copy_to_all(direction_ref, copies_hbm, sems)


def update(place, pieces, first, second):
    count, rows, rank = pieces.shape
    return pl.pallas_call(
        update_kernel,
        in_specs=[SMEM] + [VMEM] * 3,
        out_specs=[VMEM, HBM],
        out_shape=[
            jax.ShapeDtypeStruct((2, rows, rank), jnp.bfloat16),
            pltpu.HBM(pieces.shape, jnp.bfloat16),
        ],
        scratch_shapes=[pltpu.VMEM((rows, rank), jnp.bfloat16), pltpu.SemaphoreType.DMA((count,))],
        compiler_params=limit(4),
        name="update",
    )(place, pieces, first, second)


def finish_kernel(
    place_ref, basis_hbm, weight_hbm, first_hbm, second_hbm, near_ref, far_ref,
    w0, f1, f2, f3, b1, b2, b3, h1, h2,
    new_ref, step_ref, copy_ref, first_out, second_out,
    basis_ref, weight_ref, first_ref, second_ref, tiles, sems,
):
    fetched = []
    for slot, (source, target) in enumerate(
        ((basis_hbm, basis_ref), (weight_hbm, weight_ref), (first_hbm, first_ref), (second_hbm, second_ref))
    ):
        copy = pltpu.make_async_copy(source, target, sems.at[8 + slot])
        copy.start()
        fetched.append(copy)
    z, y = place_ref[0], place_ref[1]
    is_low = place_ref[3] == 0
    near, far = near_ref[:, :8].astype(jnp.float32), far_ref[:, :8].astype(jnp.float32)
    energy = jnp.sum(near * near + far * far)
    count = 2 * near.shape[0] * near.shape[1] * near.shape[2] * near.shape[3]
    spread = jnp.sqrt(jnp.full((1, 128), energy / count, jnp.float32))
    scale = (-1.0 / (spread + 1e-06))[:, :1]
    for copy in fetched:
        copy.wait()
    basis = basis_ref[...]

    def rows_of(close, distant):
        close, distant = (array.reshape(-1, array.shape[-1]) for array in (close, distant))
        return jnp.concatenate(
            [jnp.where(is_low, close, distant), jnp.where(is_low, distant, close)], axis=1
        )

    copies = []
    for k, block in enumerate((w0, f1, f2, f3, b3, b2, b1, None)):
        at = (z + 8 - (k if k < 4 else k + 1 if block is not None else 4)) % 8
        wide = dot(basis, rows_of(near_ref[:, at], far_ref[:, at]), 1, 1) * scale
        if block is None:
            lead = wide.shape[0] // 2
            tiles[k, :lead] = (h1[...].astype(jnp.float32) + wide[:lead]).astype(jnp.bfloat16)
            tiles[k, lead:] = (h2[...].astype(jnp.float32) + wide[lead:]).astype(jnp.bfloat16)
        else:
            tiles[k] = (block[...].astype(jnp.float32) + wide).astype(jnp.bfloat16)
        copy = pltpu.make_async_copy(
            tiles.at[k], copy_ref.at[:, pl.ds(pl.multiple_of(at * 256, 256), 256)], sems.at[k]
        )
        copy.start()
        copies.append(copy)

    mine = pl.ds(y * 4, 4)
    step = dot(rows_of(near_ref[mine, z], far_ref[mine, z]), basis, 1, 1) * scale
    step_ref[...] = step
    new_ref[...] = weight_ref[...] + step
    for source in range(4):
        rows = pl.ds(source * 16, 16)
        letter = y * 4 + source
        piece = near_ref[letter, 8].astype(jnp.float32) + near_ref[letter, 9].astype(jnp.float32)
        first_new, second_new = moments(piece, first_ref[rows, :], second_ref[rows, :])
        first_out[rows, :] = first_new
        second_out[rows, :] = second_new
    for copy in copies:
        copy.wait()


def finish(place, basis, weight, first, second, near, far, blocks):
    values = basis.shape[0]
    like = lambda array: jax.ShapeDtypeStruct(array.shape, jnp.float32)
    return pl.pallas_call(
        finish_kernel,
        in_specs=[SMEM] + [HBM] * 4 + [VMEM] * (2 + len(blocks)),
        out_specs=[VMEM, VMEM, HBM, VMEM, VMEM],
        out_shape=[
            like(weight),
            like(weight),
            pltpu.HBM((values, 2048), jnp.bfloat16),
            like(first),
            like(second),
        ],
        scratch_shapes=[
            pltpu.VMEM(basis.shape, basis.dtype),
            pltpu.VMEM(weight.shape, weight.dtype),
            pltpu.VMEM(first.shape, first.dtype),
            pltpu.VMEM(second.shape, second.dtype),
            pltpu.VMEM((8, values, 256), jnp.bfloat16),
            pltpu.SemaphoreType.DMA((12,)),
        ],
        compiler_params=limit(16),
        name="finish",
    )(place, *in_hbm(basis, weight, first, second), near, far, *in_vmem(*blocks))


def exchange(array, axes):
    return lax.all_to_all(array, axes, 0, 0, tiled=True)


def chain(first_mix, second_mix, lambda_head, head_gain, out_cotangent, basis, weight, first_moment, second_moment):
    place = jnp.stack([lax.axis_index(name).astype(jnp.int32) for name in ("z", "y", "x", "tp")])
    turned = weight.T
    narrow = turned.astype(jnp.bfloat16)

    lead = turned.shape[1] // 2
    w0 = widen(place, [narrow] + [shift(narrow, "y", hops) for hops in (1, 2, 3)])
    f1, b1 = shift(w0, "z", 1), shift(w0, "z", -1)
    f2, b2 = shift(f1, "z", 1), shift(b1, "z", -1)
    f3, b3 = shift(f2, "z", 1), shift(b2, "z", -1)
    h1, h2 = shift(f3[:lead], "z", 1), shift(b3[lead:], "z", -1)

    own, sent = heads(place, lambda_head, first_mix, second_mix, head_gain, basis)
    parts = gradient(own, swap_cores(sent), out_cotangent)
    folded = fold(exchange(parts, ("y", "x")))
    extra, copies = update(place, exchange(folded, "z"), first_moment, second_moment)
    near = exchange(letters(exchange(copies, "z"), extra, 16), ("y", "x"))
    far = swap_cores(near)
    weight_new, step_out, weight_copy, first_new, second_new = finish(
        place, basis, turned, first_moment, second_moment, near, far, (w0, f1, f2, f3, b1, b2, b3, h1, h2)
    )
    return (weight_new.T, weight_copy, step_out.T, first_new, second_new)


def solution(mesh):
    finer = Mesh(
        mesh.devices.reshape(8, 4, mesh.shape["rep"], mesh.shape["tp"]),
        ("z", "y", "x", "tp"),
    )
    return jax.shard_map(
        chain,
        mesh=finer,
        in_specs=(
            P(FS_REP, "tp"),
            P(FS_REP, "tp"),
            P("tp"),
            P(),
            P(FS_REP, None),
            P("tp", None),
            P("tp", FS),
            P(FS, "tp"),
            P(FS, "tp"),
        ),
        out_specs=(P("tp", FS), P("tp", None), P("tp", FS), P(FS, "tp"), P(FS, "tp")),
        check_vma=False,
    )
```

```python
import jax
import jax.numpy as jnp
from jax import lax
from jax.experimental import pallas as pl
from jax.experimental.pallas import tpu as pltpu
from jax.sharding import Mesh
from jax.sharding import PartitionSpec as P

OUT_SCALE = 0.8
BETA_FIRST = 0.9
BETA_SECOND = 0.95
FS = ("z", "y")
FS_REP = ("z", "y", "x")
SMEM = pl.BlockSpec(memory_space=pltpu.SMEM)
VMEM = pl.BlockSpec(memory_space=pltpu.VMEM)
HBM = pl.BlockSpec(memory_space=pltpu.HBM)
MIB = 1024 * 1024


def in_hbm(*arrays):
    return [pltpu.with_memory_space_constraint(array, pltpu.HBM) for array in arrays]


def in_vmem(*arrays):
    return [pltpu.with_memory_space_constraint(array, pltpu.VMEM) for array in arrays]


def shift(array, axis, hops):
    count = lax.axis_size(axis)
    return lax.ppermute(array, axis, [(i, (i + hops) % count) for i in range(count)])


def swap_cores(array):
    return lax.ppermute(array, "tp", [(0, 1), (1, 0)])


def dot(left, right, left_dim, right_dim):
    return lax.dot_general(
        left, right, (((left_dim,), (right_dim,)), ((), ())), preferred_element_type=jnp.float32
    )


def limit(mib):
    return pltpu.CompilerParams(vmem_limit_bytes=mib * MIB)


def heads_kernel(
    place_ref, lam_hbm, first_hbm, second_hbm, gain_hbm, basis_hbm, weight_hbm,
    own_ref, sent_ref, narrow_ref, first_ref, second_ref, basis_ref, lam_ref, gain_ref, weight_ref, sems,
):
    tokens, values = first_ref.shape
    width = gain_ref.shape[1]
    tile = tokens // 3

    def fetch(source, target, slot):
        copy = pltpu.make_async_copy(source, target, sems.at[slot])
        copy.start()
        return copy

    fixed = [fetch(lam_hbm, lam_ref, 0), fetch(gain_hbm, gain_ref, 1)]
    moving = []
    for step in range(3):
        rows = pl.ds(step * tile, tile)
        moving.append(
            [
                fetch(first_hbm.at[rows], first_ref.at[rows], 4 + 2 * step),
                fetch(second_hbm.at[rows], second_ref.at[rows], 5 + 2 * step),
            ]
        )
        if step == 0:
            fixed.append(fetch(basis_hbm, basis_ref, 2))
    last = fetch(weight_hbm, weight_ref, 3)
    for copy in fixed[:2]:
        copy.wait()
    gain = gain_ref[...] * OUT_SCALE
    is_low = place_ref[3] == 0
    for step in range(3):
        rows = pl.ds(step * tile, tile)
        for copy in moving[step]:
            copy.wait()
        if step == 0:
            fixed[2].wait()
        total = None
        for head in range(values // width):
            cols = slice(head * width, (head + 1) * width)
            first = first_ref[rows, cols].astype(jnp.float32)
            second = second_ref[rows, cols].astype(jnp.float32)
            mixture = first - lam_ref[:, head : head + 1] * second
            inverse = lax.rsqrt(jnp.mean(mixture * mixture, axis=-1, keepdims=True) + 1e-06)
            normed = (mixture * inverse * gain).astype(jnp.bfloat16)
            term = jnp.dot(normed, basis_ref[cols, :], preferred_element_type=jnp.float32)
            total = term if total is None else total + term
        half = total.shape[1] // 2
        low, high = total[:, :half], total[:, half:]
        own_ref[rows, :] = jnp.where(is_low, low, high)
        sent_ref[rows, :] = jnp.where(is_low, high, low).astype(jnp.bfloat16)
    last.wait()
    narrow_ref[...] = weight_ref[...].astype(jnp.bfloat16)


def heads(place, lambda_head, first_mix, second_mix, head_gain, basis, weight):
    tokens, values = first_mix.shape
    half = basis.shape[1] // 2
    lam, gain = lambda_head[None, :], head_gain[None, :]
    return pl.pallas_call(
        heads_kernel,
        in_specs=[SMEM] + [HBM] * 6,
        out_specs=[VMEM] * 3,
        out_shape=[
            jax.ShapeDtypeStruct((tokens, half), jnp.float32),
            jax.ShapeDtypeStruct((tokens, half), jnp.bfloat16),
            jax.ShapeDtypeStruct(weight.shape, jnp.bfloat16),
        ],
        scratch_shapes=[
            pltpu.VMEM((tokens, values), jnp.bfloat16),
            pltpu.VMEM((tokens, values), jnp.bfloat16),
            pltpu.VMEM(basis.shape, jnp.bfloat16),
            pltpu.VMEM(lam.shape, jnp.float32),
            pltpu.VMEM(gain.shape, jnp.float32),
            pltpu.VMEM(weight.shape, jnp.float32),
            pltpu.SemaphoreType.DMA((10,)),
        ],
        compiler_params=limit(12),
        name="heads",
    )(place, *in_hbm(lam, first_mix, second_mix, gain, basis, weight))


def widen_kernel(place_ref, own_ref, one_ref, two_ref, three_ref, out_ref, slots):
    y = place_ref[1]
    slots[y] = own_ref[...].astype(jnp.float32)
    slots[(y + 3) % 4] = one_ref[...].astype(jnp.float32)
    slots[(y + 2) % 4] = two_ref[...].astype(jnp.float32)
    slots[(y + 1) % 4] = three_ref[...].astype(jnp.float32)
    rows = slots.shape[0] * slots.shape[1]
    out_ref[...] = slots[...].reshape(rows, slots.shape[2]).T.astype(jnp.bfloat16)


def widen(place, blocks):
    rows, cols = blocks[0].shape
    return pl.pallas_call(
        widen_kernel,
        in_specs=[SMEM] + [VMEM] * 4,
        out_specs=VMEM,
        out_shape=jax.ShapeDtypeStruct((cols, 4 * rows), jnp.bfloat16),
        scratch_shapes=[pltpu.VMEM((4, rows, cols), jnp.float32)],
        compiler_params=limit(8),
        name="widen",
    )(place, *blocks)


def gradient_kernel(own_ref, far_ref, cot_ref, out_hbm, parts, sems):
    reduced = (own_ref[...] + far_ref[...].astype(jnp.float32)).T.astype(jnp.bfloat16)
    wide = 512
    copies = []
    for at in range(cot_ref.shape[1] // wide):
        block = dot(reduced, cot_ref[:, at * wide : (at + 1) * wide], 1, 0).T.astype(jnp.bfloat16)
        for z in range(2):
            rows = block[z * 256 : (z + 1) * 256]
            parts[:, at * 2 + z] = rows.reshape(16, 16, rows.shape[1])
        pair = pl.ds(at * 2, 2)
        copy = pltpu.make_async_copy(parts.at[:, pair], out_hbm.at[:, pair], sems.at[at])
        copy.start()
        copies.append(copy)
    for copy in copies:
        copy.wait()


def gradient(own, far, cot):
    shape = (16, 8, 16, own.shape[1])
    return pl.pallas_call(
        gradient_kernel,
        in_specs=[VMEM] * 3,
        out_specs=HBM,
        out_shape=pltpu.HBM(shape, jnp.bfloat16),
        scratch_shapes=[pltpu.VMEM(shape, jnp.bfloat16), pltpu.SemaphoreType.DMA((4,))],
        compiler_params=limit(8),
        name="gradient",
    )(own, far, cot)


def send(pairs, sems):
    copies = []
    for slot, (source, target) in enumerate(pairs):
        copy = pltpu.make_async_copy(source, target, sems.at[slot])
        copy.start()
        copies.append(copy)
    for copy in copies:
        copy.wait()


def fold_kernel(place_ref, parts_ref, first_ref, second_ref, out_hbm, letter_ref, sems):
    rows = pl.ds(pl.multiple_of(place_ref[2] * 16, 16), 16)
    letter_ref[:8] = jnp.sum(parts_ref[...].astype(jnp.float32), axis=0).astype(jnp.bfloat16)
    letter_ref[8] = first_ref[rows, :].astype(jnp.bfloat16)
    letter_ref[9] = second_ref[rows, :].astype(jnp.bfloat16)
    send([(letter_ref, out_hbm.at[z]) for z in range(8)], sems)


def fold(place, parts, first, second):
    shape = (10, *parts.shape[2:])
    return pl.pallas_call(
        fold_kernel,
        in_specs=[SMEM] + [VMEM] * 3,
        out_specs=HBM,
        out_shape=pltpu.HBM((8, *shape), jnp.bfloat16),
        scratch_shapes=[pltpu.VMEM(shape, jnp.bfloat16), pltpu.SemaphoreType.DMA((8,))],
        compiler_params=limit(8),
        name="fold",
    )(place, parts, first, second)


def moments(projected, first, second):
    first_new = BETA_FIRST * first + (1.0 - BETA_FIRST) * projected
    second_new = BETA_SECOND * second + (1.0 - BETA_SECOND) * projected * projected
    return first_new, second_new


def update_kernel(place_ref, letters_ref, out_hbm, letter_ref, projected_ref, sems):
    projected_ref[...] = jnp.sum(letters_ref[:, :8].astype(jnp.float32), axis=0)
    first, second = letters_ref[:, 8].astype(jnp.float32), letters_ref[:, 9].astype(jnp.float32)
    first_new, second_new = moments(projected_ref[...], first, second)
    letter_ref[:8] = (first_new / (jnp.sqrt(second_new) + 1e-08)).astype(jnp.bfloat16)
    mine = projected_ref[place_ref[0]]
    high = mine.astype(jnp.bfloat16)
    letter_ref[8] = high
    letter_ref[9] = (mine - high.astype(jnp.float32)).astype(jnp.bfloat16)
    send([(letter_ref, out_hbm.at[peer]) for peer in range(16)], sems)


def update(place, letters):
    shape = letters.shape[1:]
    return pl.pallas_call(
        update_kernel,
        in_specs=[SMEM, VMEM],
        out_specs=HBM,
        out_shape=pltpu.HBM((16, *shape), jnp.bfloat16),
        scratch_shapes=[
            pltpu.VMEM(shape, jnp.bfloat16),
            pltpu.VMEM((8, *shape[1:]), jnp.float32),
            pltpu.SemaphoreType.DMA((16,)),
        ],
        compiler_params=limit(8),
        name="update",
    )(place, letters)


def finish_kernel(
    place_ref, basis_hbm, weight_hbm, first_hbm, second_hbm, near_ref, far_ref,
    w0, f1, f2, f3, b1, b2, b3, h1, h2,
    new_ref, step_ref, copy_ref, first_out, second_out,
    basis_ref, weight_ref, first_ref, second_ref, tiles, sems,
):
    fetched = []
    for slot, (source, target) in enumerate(
        ((basis_hbm, basis_ref), (weight_hbm, weight_ref), (first_hbm, first_ref), (second_hbm, second_ref))
    ):
        copy = pltpu.make_async_copy(source, target, sems.at[8 + slot])
        copy.start()
        fetched.append(copy)
    z, y = place_ref[0], place_ref[1]
    is_low = place_ref[3] == 0
    near, far = near_ref[:, :8].astype(jnp.float32), far_ref[:, :8].astype(jnp.float32)
    energy = jnp.sum(near * near + far * far)
    count = 2 * near.shape[0] * near.shape[1] * near.shape[2] * near.shape[3]
    spread = jnp.sqrt(jnp.full((1, 128), energy / count, jnp.float32))
    scale = (-1.0 / (spread + 1e-06))[:, :1]
    for copy in fetched:
        copy.wait()
    basis = basis_ref[...]

    def rows_of(close, distant):
        close, distant = (array.reshape(-1, array.shape[-1]) for array in (close, distant))
        return jnp.concatenate(
            [jnp.where(is_low, close, distant), jnp.where(is_low, distant, close)], axis=1
        )

    copies = []
    for k, block in enumerate((w0, f1, f2, f3, b3, b2, b1, None)):
        at = (z + 8 - (k if k < 4 else k + 1 if block is not None else 4)) % 8
        wide = dot(basis, rows_of(near_ref[:, at], far_ref[:, at]), 1, 1) * scale
        if block is None:
            lead = wide.shape[0] // 2
            tiles[k, :lead] = (h1[...].astype(jnp.float32) + wide[:lead]).astype(jnp.bfloat16)
            tiles[k, lead:] = (h2[...].astype(jnp.float32) + wide[lead:]).astype(jnp.bfloat16)
        else:
            tiles[k] = (block[...].astype(jnp.float32) + wide).astype(jnp.bfloat16)
        copy = pltpu.make_async_copy(
            tiles.at[k], copy_ref.at[:, pl.ds(pl.multiple_of(at * 256, 256), 256)], sems.at[k]
        )
        copy.start()
        copies.append(copy)

    mine = pl.ds(y * 4, 4)
    step = dot(rows_of(near_ref[mine, z], far_ref[mine, z]), basis, 1, 1) * scale
    step_ref[...] = step
    new_ref[...] = weight_ref[...] + step
    for source in range(4):
        rows = pl.ds(source * 16, 16)
        letter = y * 4 + source
        piece = near_ref[letter, 8].astype(jnp.float32) + near_ref[letter, 9].astype(jnp.float32)
        first_new, second_new = moments(piece, first_ref[rows, :], second_ref[rows, :])
        first_out[rows, :] = first_new
        second_out[rows, :] = second_new
    for copy in copies:
        copy.wait()


def finish(place, basis, weight, first, second, near, far, blocks):
    values = basis.shape[0]
    like = lambda array: jax.ShapeDtypeStruct(array.shape, jnp.float32)
    return pl.pallas_call(
        finish_kernel,
        in_specs=[SMEM] + [HBM] * 4 + [VMEM] * (2 + len(blocks)),
        out_specs=[VMEM, VMEM, HBM, VMEM, VMEM],
        out_shape=[
            like(weight),
            like(weight),
            pltpu.HBM((values, 2048), jnp.bfloat16),
            like(first),
            like(second),
        ],
        scratch_shapes=[
            pltpu.VMEM(basis.shape, basis.dtype),
            pltpu.VMEM(weight.shape, weight.dtype),
            pltpu.VMEM(first.shape, first.dtype),
            pltpu.VMEM(second.shape, second.dtype),
            pltpu.VMEM((8, values, 256), jnp.bfloat16),
            pltpu.SemaphoreType.DMA((12,)),
        ],
        compiler_params=limit(16),
        name="finish",
    )(place, *in_hbm(basis, weight, first, second), near, far, *in_vmem(*blocks))


def exchange(array, axes):
    return lax.all_to_all(array, axes, 0, 0, tiled=True)


def chain(first_mix, second_mix, lambda_head, head_gain, out_cotangent, basis, weight, first_moment, second_moment):
    place = jnp.stack([lax.axis_index(name).astype(jnp.int32) for name in ("z", "y", "x", "tp")])
    turned = weight.T
    own, sent, narrow = heads(place, lambda_head, first_mix, second_mix, head_gain, basis, turned)

    lead = turned.shape[1] // 2
    w0 = widen(place, [narrow] + [shift(narrow, "y", hops) for hops in (1, 2, 3)])
    f1, b1 = shift(w0, "z", 1), shift(w0, "z", -1)
    f2, b2 = shift(f1, "z", 1), shift(b1, "z", -1)
    f3, b3 = shift(f2, "z", 1), shift(b2, "z", -1)
    h1, h2 = shift(f3[:lead], "z", 1), shift(b3[lead:], "z", -1)

    parts = gradient(own, swap_cores(sent), out_cotangent)
    sums = fold(place, exchange(parts, ("y", "x")), first_moment, second_moment)
    near = exchange(update(place, exchange(sums, "z")), ("y", "x"))
    far = swap_cores(near)
    weight_new, step_out, weight_copy, first_new, second_new = finish(
        place, basis, turned, first_moment, second_moment, near, far, (w0, f1, f2, f3, b1, b2, b3, h1, h2)
    )
    return (weight_new.T, weight_copy, step_out.T, first_new, second_new)


def solution(mesh):
    finer = Mesh(
        mesh.devices.reshape(8, 4, mesh.shape["rep"], mesh.shape["tp"]),
        ("z", "y", "x", "tp"),
    )
    return jax.shard_map(
        chain,
        mesh=finer,
        in_specs=(
            P(FS_REP, "tp"),
            P(FS_REP, "tp"),
            P("tp"),
            P(),
            P(FS_REP, None),
            P("tp", None),
            P("tp", FS),
            P(FS, "tp"),
            P(FS, "tp"),
        ),
        out_specs=(P("tp", FS), P("tp", None), P("tp", FS), P(FS, "tp"), P(FS, "tp")),
        check_vma=False,
    )
```

```python
import jax
import jax.numpy as jnp
from jax import lax
from jax.experimental import pallas as pl
from jax.experimental.pallas import tpu as pltpu
from jax.sharding import Mesh
from jax.sharding import PartitionSpec as P

OUT_SCALE = 0.8
BETA_FIRST = 0.9
BETA_SECOND = 0.95
FS = ("z", "y")
FS_REP = ("z", "y", "x")
SMEM = pl.BlockSpec(memory_space=pltpu.SMEM)
VMEM = pl.BlockSpec(memory_space=pltpu.VMEM)
HBM = pl.BlockSpec(memory_space=pltpu.HBM)
MIB = 1024 * 1024


def in_hbm(*arrays):
    return [pltpu.with_memory_space_constraint(array, pltpu.HBM) for array in arrays]


def in_vmem(*arrays):
    return [pltpu.with_memory_space_constraint(array, pltpu.VMEM) for array in arrays]


def shift(array, axis, hops):
    count = lax.axis_size(axis)
    return lax.ppermute(array, axis, [(i, (i + hops) % count) for i in range(count)])


def swap_cores(array):
    return lax.ppermute(array, "tp", [(0, 1), (1, 0)])


def dot(left, right, left_dim, right_dim):
    return lax.dot_general(
        left, right, (((left_dim,), (right_dim,)), ((), ())), preferred_element_type=jnp.float32
    )


def limit(mib):
    return pltpu.CompilerParams(vmem_limit_bytes=mib * MIB)


def heads_kernel(
    place_ref, lam_hbm, first_hbm, second_hbm, gain_hbm, basis_hbm, weight_hbm,
    own_ref, sent_ref, narrow_ref, first_ref, second_ref, basis_ref, lam_ref, gain_ref, weight_ref, sems,
):
    tokens, values = first_ref.shape
    width = gain_ref.shape[1]
    tile = tokens // 3

    def fetch(source, target, slot):
        copy = pltpu.make_async_copy(source, target, sems.at[slot])
        copy.start()
        return copy

    fixed = [fetch(lam_hbm, lam_ref, 0), fetch(gain_hbm, gain_ref, 1)]
    moving = []
    for step in range(3):
        rows = pl.ds(step * tile, tile)
        moving.append(
            [
                fetch(first_hbm.at[rows], first_ref.at[rows], 4 + 2 * step),
                fetch(second_hbm.at[rows], second_ref.at[rows], 5 + 2 * step),
            ]
        )
        if step == 0:
            fixed.append(fetch(basis_hbm, basis_ref, 2))
    last = fetch(weight_hbm, weight_ref, 3)
    for copy in fixed[:2]:
        copy.wait()
    gain = gain_ref[...] * OUT_SCALE
    is_low = place_ref[3] == 0
    for step in range(3):
        rows = pl.ds(step * tile, tile)
        for copy in moving[step]:
            copy.wait()
        if step == 0:
            fixed[2].wait()
        total = None
        for head in range(values // width):
            cols = slice(head * width, (head + 1) * width)
            first = first_ref[rows, cols].astype(jnp.float32)
            second = second_ref[rows, cols].astype(jnp.float32)
            mixture = first - lam_ref[:, head : head + 1] * second
            inverse = lax.rsqrt(jnp.mean(mixture * mixture, axis=-1, keepdims=True) + 1e-06)
            normed = (mixture * inverse * gain).astype(jnp.bfloat16)
            term = jnp.dot(normed, basis_ref[cols, :], preferred_element_type=jnp.float32)
            total = term if total is None else total + term
        half = total.shape[1] // 2
        low, high = total[:, :half], total[:, half:]
        own_ref[rows, :] = jnp.where(is_low, low, high)
        sent_ref[rows, :] = jnp.where(is_low, high, low).astype(jnp.bfloat16)
    last.wait()
    narrow_ref[...] = weight_ref[...].astype(jnp.bfloat16)


def heads(place, lambda_head, first_mix, second_mix, head_gain, basis, weight):
    tokens, values = first_mix.shape
    half = basis.shape[1] // 2
    lam, gain = lambda_head[None, :], head_gain[None, :]
    return pl.pallas_call(
        heads_kernel,
        in_specs=[SMEM] + [HBM] * 6,
        out_specs=[VMEM] * 3,
        out_shape=[
            jax.ShapeDtypeStruct((tokens, half), jnp.float32),
            jax.ShapeDtypeStruct((tokens, half), jnp.bfloat16),
            jax.ShapeDtypeStruct(weight.shape, jnp.bfloat16),
        ],
        scratch_shapes=[
            pltpu.VMEM((tokens, values), jnp.bfloat16),
            pltpu.VMEM((tokens, values), jnp.bfloat16),
            pltpu.VMEM(basis.shape, jnp.bfloat16),
            pltpu.VMEM(lam.shape, jnp.float32),
            pltpu.VMEM(gain.shape, jnp.float32),
            pltpu.VMEM(weight.shape, jnp.float32),
            pltpu.SemaphoreType.DMA((10,)),
        ],
        compiler_params=limit(12),
        name="heads",
    )(place, *in_hbm(lam, first_mix, second_mix, gain, basis, weight))


def widen_kernel(place_ref, own_ref, one_ref, two_ref, three_ref, out_ref, slots):
    y = place_ref[1]
    slots[y] = own_ref[...].astype(jnp.float32)
    slots[(y + 3) % 4] = one_ref[...].astype(jnp.float32)
    slots[(y + 2) % 4] = two_ref[...].astype(jnp.float32)
    slots[(y + 1) % 4] = three_ref[...].astype(jnp.float32)
    rows = slots.shape[0] * slots.shape[1]
    out_ref[...] = slots[...].reshape(rows, slots.shape[2]).T.astype(jnp.bfloat16)


def widen(place, blocks):
    rows, cols = blocks[0].shape
    return pl.pallas_call(
        widen_kernel,
        in_specs=[SMEM] + [VMEM] * 4,
        out_specs=VMEM,
        out_shape=jax.ShapeDtypeStruct((cols, 4 * rows), jnp.bfloat16),
        scratch_shapes=[pltpu.VMEM((4, rows, cols), jnp.float32)],
        compiler_params=limit(8),
        name="widen",
    )(place, *blocks)


def gradient_kernel(own_ref, far_ref, cot_ref, out_hbm, parts, sems):
    reduced = (own_ref[...] + far_ref[...].astype(jnp.float32)).T.astype(jnp.bfloat16)
    wide = 512
    copies = []
    for at in range(cot_ref.shape[1] // wide):
        block = dot(reduced, cot_ref[:, at * wide : (at + 1) * wide], 1, 0).T.astype(jnp.bfloat16)
        for z in range(2):
            rows = block[z * 256 : (z + 1) * 256]
            parts[:, at * 2 + z] = rows.reshape(16, 16, rows.shape[1])
        pair = pl.ds(at * 2, 2)
        copy = pltpu.make_async_copy(parts.at[:, pair], out_hbm.at[:, pair], sems.at[at])
        copy.start()
        copies.append(copy)
    for copy in copies:
        copy.wait()


def gradient(own, far, cot):
    shape = (16, 8, 16, own.shape[1])
    return pl.pallas_call(
        gradient_kernel,
        in_specs=[VMEM] * 3,
        out_specs=HBM,
        out_shape=pltpu.HBM(shape, jnp.bfloat16),
        scratch_shapes=[pltpu.VMEM(shape, jnp.bfloat16), pltpu.SemaphoreType.DMA((4,))],
        compiler_params=limit(8),
        name="gradient",
    )(own, far, cot)


def send(pairs, sems):
    copies = []
    for slot, (source, target) in enumerate(pairs):
        copy = pltpu.make_async_copy(source, target, sems.at[slot])
        copy.start()
        copies.append(copy)
    for copy in copies:
        copy.wait()


def fold_kernel(place_ref, parts_ref, first_ref, second_ref, out_hbm, letter_ref, sems):
    rows = pl.ds(pl.multiple_of(place_ref[2] * 16, 16), 16)
    letter_ref[:8] = jnp.sum(parts_ref[...].astype(jnp.float32), axis=0).astype(jnp.bfloat16)
    letter_ref[8] = first_ref[rows, :].astype(jnp.bfloat16)
    letter_ref[9] = second_ref[rows, :].astype(jnp.bfloat16)
    send([(letter_ref, out_hbm.at[z]) for z in range(8)], sems)


def fold(place, parts, first, second):
    shape = (10, *parts.shape[2:])
    return pl.pallas_call(
        fold_kernel,
        in_specs=[SMEM] + [VMEM] * 3,
        out_specs=HBM,
        out_shape=pltpu.HBM((8, *shape), jnp.bfloat16),
        scratch_shapes=[pltpu.VMEM(shape, jnp.bfloat16), pltpu.SemaphoreType.DMA((8,))],
        compiler_params=limit(8),
        name="fold",
    )(place, parts, first, second)


def moments(projected, first, second):
    first_new = BETA_FIRST * first + (1.0 - BETA_FIRST) * projected
    second_new = BETA_SECOND * second + (1.0 - BETA_SECOND) * projected * projected
    return first_new, second_new


def update_kernel(place_ref, letters_ref, out_hbm, letter_ref, projected_ref, sems):
    projected_ref[...] = jnp.sum(letters_ref[:, :8].astype(jnp.float32), axis=0)
    first, second = letters_ref[:, 8].astype(jnp.float32), letters_ref[:, 9].astype(jnp.float32)
    first_new, second_new = moments(projected_ref[...], first, second)
    letter_ref[:8] = (first_new / (jnp.sqrt(second_new) + 1e-08)).astype(jnp.bfloat16)
    mine = projected_ref[place_ref[0]]
    high = mine.astype(jnp.bfloat16)
    letter_ref[8] = high
    letter_ref[9] = (mine - high.astype(jnp.float32)).astype(jnp.bfloat16)
    send([(letter_ref, out_hbm.at[peer]) for peer in range(16)], sems)


def update(place, letters):
    shape = letters.shape[1:]
    return pl.pallas_call(
        update_kernel,
        in_specs=[SMEM, VMEM],
        out_specs=HBM,
        out_shape=pltpu.HBM((16, *shape), jnp.bfloat16),
        scratch_shapes=[
            pltpu.VMEM(shape, jnp.bfloat16),
            pltpu.VMEM((8, *shape[1:]), jnp.float32),
            pltpu.SemaphoreType.DMA((16,)),
        ],
        compiler_params=limit(8),
        name="update",
    )(place, letters)


def columns(block):
    return pl.ds(pl.multiple_of(block % 8 * 256, 256), 256)


def finish_kernel(
    place_ref, basis_hbm, weight_hbm, first_hbm, second_hbm, near_ref, far_ref, w0, f1, f2, w4, b2, b1,
    new_ref, step_ref, copy_ref, first_out, second_out, later_ref,
    basis_ref, weight_ref, first_ref, second_ref, tiles, sems,
):
    fetched = []
    for slot, (source, target) in enumerate(
        ((basis_hbm, basis_ref), (weight_hbm, weight_ref), (first_hbm, first_ref), (second_hbm, second_ref))
    ):
        copy = pltpu.make_async_copy(source, target, sems.at[6 + slot])
        copy.start()
        fetched.append(copy)
    z, y = place_ref[0], place_ref[1]
    is_low = place_ref[3] == 0
    near, far = near_ref[:, :8].astype(jnp.float32), far_ref[:, :8].astype(jnp.float32)
    energy = jnp.sum(near * near + far * far)
    count = 2 * near.shape[0] * near.shape[1] * near.shape[2] * near.shape[3]
    spread = jnp.sqrt(jnp.full((1, 128), energy / count, jnp.float32))
    scale = (-1.0 / (spread + 1e-06))[:, :1]
    for copy in fetched:
        copy.wait()
    basis = basis_ref[...]

    def rows_of(close, distant):
        close, distant = (array.reshape(-1, array.shape[-1]) for array in (close, distant))
        return jnp.concatenate(
            [jnp.where(is_low, close, distant), jnp.where(is_low, distant, close)], axis=1
        )

    def step_of(block):
        at = block % 8
        return dot(basis, rows_of(near_ref[:, at], far_ref[:, at]), 1, 1) * scale

    copies = []
    for slot, (block, hops) in enumerate(((w0, 0), (f1, 7), (b1, 1), (f2, 6), (b2, 2), (w4, 4))):
        tiles[slot] = (block[...].astype(jnp.float32) + step_of(z + hops)).astype(jnp.bfloat16)
        copy = pltpu.make_async_copy(tiles.at[slot], copy_ref.at[:, columns(z + hops)], sems.at[slot])
        copy.start()
        copies.append(copy)
    for slot, hops in enumerate((5, 3)):
        later_ref[slot] = step_of(z + hops)

    mine = pl.ds(y * 4, 4)
    step = dot(rows_of(near_ref[mine, z], far_ref[mine, z]), basis, 1, 1) * scale
    step_ref[...] = step
    new_ref[...] = weight_ref[...] + step
    for source in range(4):
        rows = pl.ds(source * 16, 16)
        letter = y * 4 + source
        piece = near_ref[letter, 8].astype(jnp.float32) + near_ref[letter, 9].astype(jnp.float32)
        first_new, second_new = moments(piece, first_ref[rows, :], second_ref[rows, :])
        first_out[rows, :] = first_new
        second_out[rows, :] = second_new
    for copy in copies:
        copy.wait()


def finish(place, basis, weight, first, second, near, far, blocks):
    values = basis.shape[0]
    like = lambda array: jax.ShapeDtypeStruct(array.shape, jnp.float32)
    return pl.pallas_call(
        finish_kernel,
        in_specs=[SMEM] + [HBM] * 4 + [VMEM] * (2 + len(blocks)),
        out_specs=[VMEM, VMEM, HBM, VMEM, VMEM, VMEM],
        out_shape=[
            like(weight),
            like(weight),
            pltpu.HBM((values, 2048), jnp.bfloat16),
            like(first),
            like(second),
            pltpu.VMEM((2, values, 256), jnp.float32),
        ],
        scratch_shapes=[
            pltpu.VMEM(basis.shape, basis.dtype),
            pltpu.VMEM(weight.shape, weight.dtype),
            pltpu.VMEM(first.shape, first.dtype),
            pltpu.VMEM(second.shape, second.dtype),
            pltpu.VMEM((6, values, 256), jnp.bfloat16),
            pltpu.SemaphoreType.DMA((10,)),
        ],
        compiler_params=limit(16),
        name="finish",
    )(place, *in_hbm(basis, weight, first, second), near, far, *in_vmem(*blocks))


def last_kernel(place_ref, later_ref, f3, b3, copy_in, copy_ref, tiles, sems):
    z = place_ref[0]
    copies = []
    for slot, (block, hops) in enumerate(((f3, 5), (b3, 3))):
        tiles[slot] = (block[...].astype(jnp.float32) + later_ref[slot]).astype(jnp.bfloat16)
        copy = pltpu.make_async_copy(tiles.at[slot], copy_ref.at[:, columns(z + hops)], sems.at[slot])
        copy.start()
        copies.append(copy)
    for copy in copies:
        copy.wait()


def last(place, later, f3, b3, copy):
    return pl.pallas_call(
        last_kernel,
        in_specs=[SMEM, VMEM, VMEM, VMEM, HBM],
        out_specs=HBM,
        out_shape=pltpu.HBM(copy.shape, copy.dtype),
        input_output_aliases={4: 0},
        scratch_shapes=[pltpu.VMEM((2, copy.shape[0], 256), copy.dtype), pltpu.SemaphoreType.DMA((2,))],
        compiler_params=limit(8),
        name="last",
    )(place, *in_vmem(later, f3, b3), *in_hbm(copy))


def exchange(array, axes):
    return lax.all_to_all(array, axes, 0, 0, tiled=True)


def chain(first_mix, second_mix, lambda_head, head_gain, out_cotangent, basis, weight, first_moment, second_moment):
    place = jnp.stack([lax.axis_index(name).astype(jnp.int32) for name in ("z", "y", "x", "tp")])
    turned = weight.T
    own, sent, narrow = heads(place, lambda_head, first_mix, second_mix, head_gain, basis, turned)

    w0 = widen(place, [narrow] + [shift(narrow, "y", hops) for hops in (1, 2, 3)])
    opposite = shift(narrow, "z", 4)
    w4 = widen(place, [opposite] + [shift(opposite, "y", hops) for hops in (1, 2, 3)])
    f1, b1 = shift(w0, "z", 1), shift(w0, "z", -1)
    f2, b2 = shift(f1, "z", 1), shift(b1, "z", -1)
    f3, b3 = shift(f2, "z", 1), shift(b2, "z", -1)

    parts = gradient(own, swap_cores(sent), out_cotangent)
    sums = fold(place, exchange(parts, ("y", "x")), first_moment, second_moment)
    near = exchange(update(place, exchange(sums, "z")), ("y", "x"))
    far = swap_cores(near)
    weight_new, step_out, most, first_new, second_new, later = finish(
        place, basis, turned, first_moment, second_moment, near, far, (w0, f1, f2, w4, b2, b1)
    )
    weight_copy = last(place, later, f3, b3, most)
    return (weight_new.T, weight_copy, step_out.T, first_new, second_new)


def solution(mesh):
    finer = Mesh(
        mesh.devices.reshape(8, 4, mesh.shape["rep"], mesh.shape["tp"]),
        ("z", "y", "x", "tp"),
    )
    return jax.shard_map(
        chain,
        mesh=finer,
        in_specs=(
            P(FS_REP, "tp"),
            P(FS_REP, "tp"),
            P("tp"),
            P(),
            P(FS_REP, None),
            P("tp", None),
            P("tp", FS),
            P(FS, "tp"),
            P(FS, "tp"),
        ),
        out_specs=(P("tp", FS), P("tp", None), P("tp", FS), P(FS, "tp"), P(FS, "tp")),
        check_vma=False,
    )
```

```python
import jax
import jax.numpy as jnp
from jax import lax
from jax.experimental import pallas as pl
from jax.experimental.pallas import tpu as pltpu
from jax.sharding import Mesh
from jax.sharding import PartitionSpec as P

OUT_SCALE = 0.8
BETA_FIRST = 0.9
BETA_SECOND = 0.95
FS = ("z", "y")
FS_REP = ("z", "y", "x")
SMEM = pl.BlockSpec(memory_space=pltpu.SMEM)
VMEM = pl.BlockSpec(memory_space=pltpu.VMEM)
HBM = pl.BlockSpec(memory_space=pltpu.HBM)
MIB = 1024 * 1024


def in_hbm(*arrays):
    return [pltpu.with_memory_space_constraint(array, pltpu.HBM) for array in arrays]


def in_vmem(*arrays):
    return [pltpu.with_memory_space_constraint(array, pltpu.VMEM) for array in arrays]


def shift(array, axis, hops):
    count = lax.axis_size(axis)
    return lax.ppermute(array, axis, [(i, (i + hops) % count) for i in range(count)])


def swap_cores(array):
    return lax.ppermute(array, "tp", [(0, 1), (1, 0)])


def dot(left, right, left_dim, right_dim):
    return lax.dot_general(
        left, right, (((left_dim,), (right_dim,)), ((), ())), preferred_element_type=jnp.float32
    )


def limit(mib):
    return pltpu.CompilerParams(vmem_limit_bytes=mib * MIB)


def heads_kernel(
    place_ref, lam_hbm, first_hbm, second_hbm, gain_hbm, basis_hbm, weight_hbm,
    own_ref, sent_ref, narrow_ref, first_ref, second_ref, basis_ref, lam_ref, gain_ref, weight_ref, sems,
):
    tokens, values = first_ref.shape
    width = gain_ref.shape[1]
    tile = tokens // 3

    def fetch(source, target, slot):
        copy = pltpu.make_async_copy(source, target, sems.at[slot])
        copy.start()
        return copy

    fixed = [fetch(lam_hbm, lam_ref, 0), fetch(gain_hbm, gain_ref, 1)]
    moving = []
    for step in range(3):
        rows = pl.ds(step * tile, tile)
        moving.append(
            [
                fetch(first_hbm.at[rows], first_ref.at[rows], 4 + 2 * step),
                fetch(second_hbm.at[rows], second_ref.at[rows], 5 + 2 * step),
            ]
        )
        if step == 0:
            fixed.append(fetch(basis_hbm, basis_ref, 2))
    last = fetch(weight_hbm, weight_ref, 3)
    for copy in fixed[:2]:
        copy.wait()
    gain = gain_ref[...] * OUT_SCALE
    is_low = place_ref[3] == 0
    for step in range(3):
        rows = pl.ds(step * tile, tile)
        for copy in moving[step]:
            copy.wait()
        if step == 0:
            fixed[2].wait()
        total = None
        for head in range(values // width):
            cols = slice(head * width, (head + 1) * width)
            first = first_ref[rows, cols].astype(jnp.float32)
            second = second_ref[rows, cols].astype(jnp.float32)
            mixture = first - lam_ref[:, head : head + 1] * second
            inverse = lax.rsqrt(jnp.mean(mixture * mixture, axis=-1, keepdims=True) + 1e-06)
            normed = (mixture * inverse * gain).astype(jnp.bfloat16)
            term = jnp.dot(normed, basis_ref[cols, :], preferred_element_type=jnp.float32)
            total = term if total is None else total + term
        half = total.shape[1] // 2
        low, high = total[:, :half], total[:, half:]
        own_ref[rows, :] = jnp.where(is_low, low, high)
        sent_ref[rows, :] = jnp.where(is_low, high, low).astype(jnp.bfloat16)
    last.wait()
    narrow_ref[...] = weight_ref[...].astype(jnp.bfloat16)


def heads(place, lambda_head, first_mix, second_mix, head_gain, basis, weight):
    tokens, values = first_mix.shape
    half = basis.shape[1] // 2
    lam, gain = lambda_head[None, :], head_gain[None, :]
    return pl.pallas_call(
        heads_kernel,
        in_specs=[SMEM] + [HBM] * 6,
        out_specs=[VMEM] * 3,
        out_shape=[
            jax.ShapeDtypeStruct((tokens, half), jnp.float32),
            jax.ShapeDtypeStruct((tokens, half), jnp.bfloat16),
            pltpu.VMEM(weight.shape, jnp.bfloat16),
        ],
        scratch_shapes=[
            pltpu.VMEM((tokens, values), jnp.bfloat16),
            pltpu.VMEM((tokens, values), jnp.bfloat16),
            pltpu.VMEM(basis.shape, jnp.bfloat16),
            pltpu.VMEM(lam.shape, jnp.float32),
            pltpu.VMEM(gain.shape, jnp.float32),
            pltpu.VMEM(weight.shape, jnp.float32),
            pltpu.SemaphoreType.DMA((10,)),
        ],
        compiler_params=limit(12),
        name="heads",
    )(place, *in_hbm(lam, first_mix, second_mix, gain, basis, weight))


def widen_kernel(place_ref, own_ref, one_hbm, two_hbm, three_hbm, out_ref, slots, sems):
    y = place_ref[1]
    copies = []
    for hops, source in ((1, one_hbm), (2, two_hbm), (3, three_hbm)):
        copy = pltpu.make_async_copy(source, slots.at[(y + 4 - hops) % 4], sems.at[hops])
        copy.start()
        copies.append(copy)
    slots[y] = own_ref[...]
    for copy in copies:
        copy.wait()
    rows = slots.shape[0] * slots.shape[1]
    out_ref[...] = slots[...].reshape(rows, slots.shape[2]).astype(jnp.float32).T.astype(jnp.bfloat16)


def widen(place, blocks):
    rows, cols = blocks[0].shape
    return pl.pallas_call(
        widen_kernel,
        in_specs=[SMEM, VMEM] + [HBM] * 3,
        out_specs=VMEM,
        out_shape=jax.ShapeDtypeStruct((cols, 4 * rows), jnp.bfloat16),
        scratch_shapes=[pltpu.VMEM((4, rows, cols), jnp.bfloat16), pltpu.SemaphoreType.DMA((4,))],
        compiler_params=limit(6),
        name="widen",
    )(place, blocks[0], *in_hbm(*blocks[1:]))


def gradient_kernel(own_ref, far_ref, cot_ref, out_hbm, parts, sems):
    reduced = (own_ref[...] + far_ref[...].astype(jnp.float32)).T.astype(jnp.bfloat16)
    wide = 512
    copies = []
    for at in range(cot_ref.shape[1] // wide):
        block = dot(reduced, cot_ref[:, at * wide : (at + 1) * wide], 1, 0).T.astype(jnp.bfloat16)
        for z in range(2):
            rows = block[z * 256 : (z + 1) * 256]
            parts[:, at * 2 + z] = rows.reshape(16, 16, rows.shape[1])
        pair = pl.ds(at * 2, 2)
        copy = pltpu.make_async_copy(parts.at[:, pair], out_hbm.at[:, pair], sems.at[at])
        copy.start()
        copies.append(copy)
    for copy in copies:
        copy.wait()


def gradient(own, far, cot):
    shape = (16, 8, 16, own.shape[1])
    return pl.pallas_call(
        gradient_kernel,
        in_specs=[VMEM] * 3,
        out_specs=HBM,
        out_shape=pltpu.HBM(shape, jnp.bfloat16),
        scratch_shapes=[pltpu.VMEM(shape, jnp.bfloat16), pltpu.SemaphoreType.DMA((4,))],
        compiler_params=limit(8),
        name="gradient",
    )(own, far, cot)


def send(pairs, sems):
    copies = []
    for slot, (source, target) in enumerate(pairs):
        copy = pltpu.make_async_copy(source, target, sems.at[slot])
        copy.start()
        copies.append(copy)
    for copy in copies:
        copy.wait()


def fold_kernel(place_ref, parts_ref, first_ref, second_ref, out_hbm, letter_ref, sems):
    rows = pl.ds(pl.multiple_of(place_ref[2] * 16, 16), 16)
    letter_ref[:8] = jnp.sum(parts_ref[...].astype(jnp.float32), axis=0).astype(jnp.bfloat16)
    letter_ref[8] = first_ref[rows, :].astype(jnp.bfloat16)
    letter_ref[9] = second_ref[rows, :].astype(jnp.bfloat16)
    send([(letter_ref, out_hbm.at[z]) for z in range(8)], sems)


def fold(place, parts, first, second):
    shape = (10, *parts.shape[2:])
    return pl.pallas_call(
        fold_kernel,
        in_specs=[SMEM] + [VMEM] * 3,
        out_specs=HBM,
        out_shape=pltpu.HBM((8, *shape), jnp.bfloat16),
        scratch_shapes=[pltpu.VMEM(shape, jnp.bfloat16), pltpu.SemaphoreType.DMA((8,))],
        compiler_params=limit(8),
        name="fold",
    )(place, parts, first, second)


def moments(projected, first, second):
    first_new = BETA_FIRST * first + (1.0 - BETA_FIRST) * projected
    second_new = BETA_SECOND * second + (1.0 - BETA_SECOND) * projected * projected
    return first_new, second_new


def update_kernel(place_ref, letters_ref, out_hbm, letter_ref, projected_ref, sems):
    projected_ref[...] = jnp.sum(letters_ref[:, :8].astype(jnp.float32), axis=0)
    first, second = letters_ref[:, 8].astype(jnp.float32), letters_ref[:, 9].astype(jnp.float32)
    first_new, second_new = moments(projected_ref[...], first, second)
    letter_ref[:8] = (first_new / (jnp.sqrt(second_new) + 1e-08)).astype(jnp.bfloat16)
    mine = projected_ref[place_ref[0]]
    high = mine.astype(jnp.bfloat16)
    letter_ref[8] = high
    letter_ref[9] = (mine - high.astype(jnp.float32)).astype(jnp.bfloat16)
    send([(letter_ref, out_hbm.at[peer]) for peer in range(16)], sems)


def update(place, letters):
    shape = letters.shape[1:]
    return pl.pallas_call(
        update_kernel,
        in_specs=[SMEM, VMEM],
        out_specs=HBM,
        out_shape=pltpu.HBM((16, *shape), jnp.bfloat16),
        scratch_shapes=[
            pltpu.VMEM(shape, jnp.bfloat16),
            pltpu.VMEM((8, *shape[1:]), jnp.float32),
            pltpu.SemaphoreType.DMA((16,)),
        ],
        compiler_params=limit(8),
        name="update",
    )(place, letters)


def columns(block):
    return pl.ds(pl.multiple_of(block % 8 * 256, 256), 256)


def finish_kernel(
    place_ref, basis_hbm, weight_hbm, first_hbm, second_hbm, near_ref, far_ref, w0, w4, b1, f1_hbm, f2_hbm, b2_hbm,
    new_ref, step_ref, copy_ref, first_out, second_out, later_ref,
    basis_ref, weight_ref, first_ref, second_ref, blocks, tiles, sems,
):
    fetched = []
    for slot, (source, target) in enumerate(
        (
            (basis_hbm, basis_ref),
            (f1_hbm, blocks.at[0]),
            (f2_hbm, blocks.at[1]),
            (b2_hbm, blocks.at[2]),
            (weight_hbm, weight_ref),
            (first_hbm, first_ref),
            (second_hbm, second_ref),
        )
    ):
        copy = pltpu.make_async_copy(source, target, sems.at[6 + slot])
        copy.start()
        fetched.append(copy)
    z, y = place_ref[0], place_ref[1]
    is_low = place_ref[3] == 0
    near, far = near_ref[:, :8].astype(jnp.float32), far_ref[:, :8].astype(jnp.float32)
    energy = jnp.sum(near * near + far * far)
    count = 2 * near.shape[0] * near.shape[1] * near.shape[2] * near.shape[3]
    spread = jnp.sqrt(jnp.full((1, 128), energy / count, jnp.float32))
    scale = (-1.0 / (spread + 1e-06))[:, :1]
    fetched[0].wait()
    basis = basis_ref[...]

    def rows_of(close, distant):
        close, distant = (array.reshape(-1, array.shape[-1]) for array in (close, distant))
        return jnp.concatenate(
            [jnp.where(is_low, close, distant), jnp.where(is_low, distant, close)], axis=1
        )

    def step_of(block):
        at = block % 8
        return dot(basis, rows_of(near_ref[:, at], far_ref[:, at]), 1, 1) * scale

    copies = []
    near_blocks = ((w0, 0), (w4, 4), (b1, 1), (blocks.at[0], 7), (blocks.at[1], 6), (blocks.at[2], 2))
    for slot, (block, hops) in enumerate(near_blocks):
        if slot >= 3:
            fetched[slot - 2].wait()
        tiles[slot] = (block[...].astype(jnp.float32) + step_of(z + hops)).astype(jnp.bfloat16)
        copy = pltpu.make_async_copy(tiles.at[slot], copy_ref.at[:, columns(z + hops)], sems.at[slot])
        copy.start()
        copies.append(copy)
    for slot, hops in enumerate((5, 3)):
        later_ref[slot] = step_of(z + hops)

    for copy in fetched[4:]:
        copy.wait()
    mine = pl.ds(y * 4, 4)
    step = dot(rows_of(near_ref[mine, z], far_ref[mine, z]), basis, 1, 1) * scale
    step_ref[...] = step
    new_ref[...] = weight_ref[...] + step
    for source in range(4):
        rows = pl.ds(source * 16, 16)
        letter = y * 4 + source
        piece = near_ref[letter, 8].astype(jnp.float32) + near_ref[letter, 9].astype(jnp.float32)
        first_new, second_new = moments(piece, first_ref[rows, :], second_ref[rows, :])
        first_out[rows, :] = first_new
        second_out[rows, :] = second_new
    for copy in copies:
        copy.wait()


def finish(place, basis, weight, first, second, near, far, blocks):
    values = basis.shape[0]
    like = lambda array: jax.ShapeDtypeStruct(array.shape, jnp.float32)
    return pl.pallas_call(
        finish_kernel,
        in_specs=[SMEM] + [HBM] * 4 + [VMEM] * 5 + [HBM] * 3,
        out_specs=[VMEM, VMEM, HBM, VMEM, VMEM, VMEM],
        out_shape=[
            like(weight),
            like(weight),
            pltpu.HBM((values, 2048), jnp.bfloat16),
            like(first),
            like(second),
            pltpu.VMEM((2, values, 256), jnp.float32),
        ],
        scratch_shapes=[
            pltpu.VMEM(basis.shape, basis.dtype),
            pltpu.VMEM(weight.shape, weight.dtype),
            pltpu.VMEM(first.shape, first.dtype),
            pltpu.VMEM(second.shape, second.dtype),
            pltpu.VMEM((3, values, 256), jnp.bfloat16),
            pltpu.VMEM((6, values, 256), jnp.bfloat16),
            pltpu.SemaphoreType.DMA((13,)),
        ],
        compiler_params=limit(16),
        name="finish",
    )(place, *in_hbm(basis, weight, first, second), near, far, *blocks[:3], *in_hbm(*blocks[3:]))


def last_kernel(place_ref, later_ref, f3, b3, copy_in, copy_ref, tiles, sems):
    z = place_ref[0]
    copies = []
    for slot, (block, hops) in enumerate(((f3, 5), (b3, 3))):
        tiles[slot] = (block[...].astype(jnp.float32) + later_ref[slot]).astype(jnp.bfloat16)
        copy = pltpu.make_async_copy(tiles.at[slot], copy_ref.at[:, columns(z + hops)], sems.at[slot])
        copy.start()
        copies.append(copy)
    for copy in copies:
        copy.wait()


def last(place, later, f3, b3, copy):
    return pl.pallas_call(
        last_kernel,
        in_specs=[SMEM, VMEM, VMEM, VMEM, HBM],
        out_specs=HBM,
        out_shape=pltpu.HBM(copy.shape, copy.dtype),
        input_output_aliases={4: 0},
        scratch_shapes=[pltpu.VMEM((2, copy.shape[0], 256), copy.dtype), pltpu.SemaphoreType.DMA((2,))],
        compiler_params=limit(8),
        name="last",
    )(place, *in_vmem(later), f3, b3, *in_hbm(copy))


def exchange(array, axes):
    return lax.all_to_all(array, axes, 0, 0, tiled=True)


def chain(first_mix, second_mix, lambda_head, head_gain, out_cotangent, basis, weight, first_moment, second_moment):
    place = jnp.stack([lax.axis_index(name).astype(jnp.int32) for name in ("z", "y", "x", "tp")])
    turned = weight.T
    own, sent, narrow = heads(place, lambda_head, first_mix, second_mix, head_gain, basis, turned)

    w0 = widen(place, [narrow] + [shift(narrow, "y", hops) for hops in (1, 2, 3)])
    opposite = shift(narrow, "z", 4)
    w4 = widen(place, [opposite] + [shift(opposite, "y", hops) for hops in (1, 2, 3)])
    f1, b1 = shift(w0, "z", 1), shift(w0, "z", -1)
    f2, b2 = shift(f1, "z", 1), shift(b1, "z", -1)
    f3, b3 = shift(f2, "z", 1), shift(b2, "z", -1)

    parts = gradient(own, swap_cores(sent), out_cotangent)
    sums = fold(place, exchange(parts, ("y", "x")), first_moment, second_moment)
    near = exchange(update(place, exchange(sums, "z")), ("y", "x"))
    far = swap_cores(near)
    weight_new, step_out, most, first_new, second_new, later = finish(
        place, basis, turned, first_moment, second_moment, near, far, (w0, w4, b1, f1, f2, b2)
    )
    weight_copy = last(place, later, f3, b3, most)
    return (weight_new.T, weight_copy, step_out.T, first_new, second_new)


def solution(mesh):
    finer = Mesh(
        mesh.devices.reshape(8, 4, mesh.shape["rep"], mesh.shape["tp"]),
        ("z", "y", "x", "tp"),
    )
    return jax.shard_map(
        chain,
        mesh=finer,
        in_specs=(
            P(FS_REP, "tp"),
            P(FS_REP, "tp"),
            P("tp"),
            P(),
            P(FS_REP, None),
            P("tp", None),
            P("tp", FS),
            P(FS, "tp"),
            P(FS, "tp"),
        ),
        out_specs=(P("tp", FS), P("tp", None), P("tp", FS), P(FS, "tp"), P(FS, "tp")),
        check_vma=False,
    )
```

```python
import jax
import jax.numpy as jnp
from jax import lax
from jax.experimental import pallas as pl
from jax.experimental.pallas import tpu as pltpu
from jax.sharding import Mesh
from jax.sharding import PartitionSpec as P

OUT_SCALE = 0.8
BETA_FIRST = 0.9
BETA_SECOND = 0.95
Z = ("zh", "zl")
FS = (*Z, "y")
FS_REP = (*FS, "x")
NEAR = ("zl", "y", "x")
SMEM = pl.BlockSpec(memory_space=pltpu.SMEM)
VMEM = pl.BlockSpec(memory_space=pltpu.VMEM)
HBM = pl.BlockSpec(memory_space=pltpu.HBM)
MIB = 1024 * 1024


def in_hbm(*arrays):
    return [pltpu.with_memory_space_constraint(array, pltpu.HBM) for array in arrays]


def in_vmem(*arrays):
    return [pltpu.with_memory_space_constraint(array, pltpu.VMEM) for array in arrays]


def shift(array, axis, hops):
    count = lax.axis_size(axis)
    return lax.ppermute(array, axis, [(i, (i + hops) % count) for i in range(count)])


def swap_cores(array):
    return lax.ppermute(array, "tp", [(0, 1), (1, 0)])


def dot(left, right, left_dim, right_dim):
    return lax.dot_general(
        left, right, (((left_dim,), (right_dim,)), ((), ())), preferred_element_type=jnp.float32
    )


def limit(mib):
    return pltpu.CompilerParams(vmem_limit_bytes=mib * MIB)


def heads_kernel(
    place_ref, lam_hbm, first_hbm, second_hbm, gain_hbm, basis_hbm, weight_hbm,
    own_ref, sent_ref, narrow_ref, first_ref, second_ref, basis_ref, lam_ref, gain_ref, weight_ref, sems,
):
    tokens, values = first_ref.shape
    width = gain_ref.shape[1]
    tile = tokens // 3

    def fetch(source, target, slot):
        copy = pltpu.make_async_copy(source, target, sems.at[slot])
        copy.start()
        return copy

    fixed = [fetch(lam_hbm, lam_ref, 0), fetch(gain_hbm, gain_ref, 1)]
    moving = []
    for step in range(3):
        rows = pl.ds(step * tile, tile)
        moving.append(
            [
                fetch(first_hbm.at[rows], first_ref.at[rows], 4 + 2 * step),
                fetch(second_hbm.at[rows], second_ref.at[rows], 5 + 2 * step),
            ]
        )
        if step == 0:
            fixed.append(fetch(basis_hbm, basis_ref, 2))
    last = fetch(weight_hbm, weight_ref, 3)
    for copy in fixed[:2]:
        copy.wait()
    gain = gain_ref[...] * OUT_SCALE
    is_low = place_ref[3] == 0
    for step in range(3):
        rows = pl.ds(step * tile, tile)
        for copy in moving[step]:
            copy.wait()
        if step == 0:
            fixed[2].wait()
        total = None
        for head in range(values // width):
            cols = slice(head * width, (head + 1) * width)
            first = first_ref[rows, cols].astype(jnp.float32)
            second = second_ref[rows, cols].astype(jnp.float32)
            mixture = first - lam_ref[:, head : head + 1] * second
            inverse = lax.rsqrt(jnp.mean(mixture * mixture, axis=-1, keepdims=True) + 1e-06)
            normed = (mixture * inverse * gain).astype(jnp.bfloat16)
            term = jnp.dot(normed, basis_ref[cols, :], preferred_element_type=jnp.float32)
            total = term if total is None else total + term
        half = total.shape[1] // 2
        low, high = total[:, :half], total[:, half:]
        own_ref[rows, :] = jnp.where(is_low, low, high)
        sent_ref[rows, :] = jnp.where(is_low, high, low).astype(jnp.bfloat16)
    last.wait()
    narrow_ref[...] = weight_ref[...].astype(jnp.bfloat16)


def heads(place, lambda_head, first_mix, second_mix, head_gain, basis, weight):
    tokens, values = first_mix.shape
    half = basis.shape[1] // 2
    lam, gain = lambda_head[None, :], head_gain[None, :]
    return pl.pallas_call(
        heads_kernel,
        in_specs=[SMEM] + [HBM] * 6,
        out_specs=[VMEM] * 3,
        out_shape=[
            jax.ShapeDtypeStruct((tokens, half), jnp.float32),
            jax.ShapeDtypeStruct((tokens, half), jnp.bfloat16),
            pltpu.VMEM(weight.shape, jnp.bfloat16),
        ],
        scratch_shapes=[
            pltpu.VMEM((tokens, values), jnp.bfloat16),
            pltpu.VMEM((tokens, values), jnp.bfloat16),
            pltpu.VMEM(basis.shape, jnp.bfloat16),
            pltpu.VMEM(lam.shape, jnp.float32),
            pltpu.VMEM(gain.shape, jnp.float32),
            pltpu.VMEM(weight.shape, jnp.float32),
            pltpu.SemaphoreType.DMA((10,)),
        ],
        compiler_params=limit(12),
        name="heads",
    )(place, *in_hbm(lam, first_mix, second_mix, gain, basis, weight))


def widen_kernel(place_ref, own_ref, one_ref, two_ref, three_ref, out_ref, slots):
    y = place_ref[1]
    slots[y] = own_ref[...].astype(jnp.float32)
    slots[(y + 3) % 4] = one_ref[...].astype(jnp.float32)
    slots[(y + 2) % 4] = two_ref[...].astype(jnp.float32)
    slots[(y + 1) % 4] = three_ref[...].astype(jnp.float32)
    rows = slots.shape[0] * slots.shape[1]
    out_ref[...] = slots[...].reshape(rows, slots.shape[2]).T.astype(jnp.bfloat16)


def widen(place, blocks):
    rows, cols = blocks[0].shape
    return pl.pallas_call(
        widen_kernel,
        in_specs=[SMEM] + [VMEM] * 4,
        out_specs=VMEM,
        out_shape=jax.ShapeDtypeStruct((cols, 4 * rows), jnp.bfloat16),
        scratch_shapes=[pltpu.VMEM((4, rows, cols), jnp.float32)],
        compiler_params=limit(8),
        name="widen",
    )(place, *blocks)


def gradient_kernel(own_ref, far_ref, cot_ref, out_hbm, parts, sems):
    reduced = (own_ref[...] + far_ref[...].astype(jnp.float32)).T.astype(jnp.bfloat16)
    wide = 512
    copies = []
    for at in range(cot_ref.shape[1] // wide):
        block = dot(reduced, cot_ref[:, at * wide : (at + 1) * wide], 1, 0).T.astype(jnp.bfloat16)
        for z in range(2):
            rows = block[z * 256 : (z + 1) * 256]
            parts[z * 16 : (z + 1) * 16, at] = rows.reshape(16, 16, rows.shape[1])
        copy = pltpu.make_async_copy(parts.at[:, at], out_hbm.at[:, at], sems.at[at])
        copy.start()
        copies.append(copy)
    for copy in copies:
        copy.wait()


def gradient(own, far, cot):
    shape = (32, 4, 16, own.shape[1])
    return pl.pallas_call(
        gradient_kernel,
        in_specs=[VMEM] * 3,
        out_specs=HBM,
        out_shape=pltpu.HBM(shape, jnp.bfloat16),
        scratch_shapes=[pltpu.VMEM(shape, jnp.bfloat16), pltpu.SemaphoreType.DMA((4,))],
        compiler_params=limit(8),
        name="gradient",
    )(own, far, cot)


def send(pairs, sems):
    copies = []
    for slot, (source, target) in enumerate(pairs):
        copy = pltpu.make_async_copy(source, target, sems.at[slot])
        copy.start()
        copies.append(copy)
    for copy in copies:
        copy.wait()


def fold_kernel(place_ref, parts_ref, first_ref, second_ref, out_hbm, letter_ref, sems):
    rows = pl.ds(pl.multiple_of(place_ref[2] * 16, 16), 16)
    letter_ref[:4] = jnp.sum(parts_ref[...].astype(jnp.float32), axis=0).astype(jnp.bfloat16)
    letter_ref[4] = first_ref[rows, :].astype(jnp.bfloat16)
    letter_ref[5] = second_ref[rows, :].astype(jnp.bfloat16)
    send([(letter_ref, out_hbm.at[peer]) for peer in range(4)], sems)


def fold(place, parts, first, second):
    shape = (6, *parts.shape[2:])
    return pl.pallas_call(
        fold_kernel,
        in_specs=[SMEM] + [VMEM] * 3,
        out_specs=HBM,
        out_shape=pltpu.HBM((4, *shape), jnp.bfloat16),
        scratch_shapes=[pltpu.VMEM(shape, jnp.bfloat16), pltpu.SemaphoreType.DMA((4,))],
        compiler_params=limit(8),
        name="fold",
    )(place, parts, first, second)


def moments(projected, first, second):
    first_new = BETA_FIRST * first + (1.0 - BETA_FIRST) * projected
    second_new = BETA_SECOND * second + (1.0 - BETA_SECOND) * projected * projected
    return first_new, second_new


def update_kernel(place_ref, letters_ref, out_hbm, letter_ref, projected_ref, sems):
    projected_ref[...] = jnp.sum(letters_ref[:, :4].astype(jnp.float32), axis=0)
    first, second = letters_ref[:, 4].astype(jnp.float32), letters_ref[:, 5].astype(jnp.float32)
    first_new, second_new = moments(projected_ref[...], first, second)
    letter_ref[:4] = (first_new / (jnp.sqrt(second_new) + 1e-08)).astype(jnp.bfloat16)
    mine = projected_ref[place_ref[0] // 2]
    high = mine.astype(jnp.bfloat16)
    letter_ref[4] = high
    letter_ref[5] = (mine - high.astype(jnp.float32)).astype(jnp.bfloat16)
    send([(letter_ref, out_hbm.at[peer]) for peer in range(32)], sems)


def update(place, letters):
    shape = letters.shape[1:]
    return pl.pallas_call(
        update_kernel,
        in_specs=[SMEM, VMEM],
        out_specs=HBM,
        out_shape=pltpu.HBM((32, *shape), jnp.bfloat16),
        scratch_shapes=[
            pltpu.VMEM(shape, jnp.bfloat16),
            pltpu.VMEM((4, *shape[1:]), jnp.float32),
            pltpu.SemaphoreType.DMA((32,)),
        ],
        compiler_params=limit(8),
        name="update",
    )(place, letters)


def columns(block):
    return pl.ds(pl.multiple_of(block % 8 * 256, 256), 256)


def finish_kernel(
    place_ref, basis_hbm, weight_hbm, first_hbm, second_hbm, near_ref, far_ref,
    w0_hbm, b1_hbm, f1_hbm, w4_hbm, f2_hbm, b2_hbm,
    new_ref, step_ref, copy_ref, first_out, second_out, rows_out, scale_out, basis_ref,
    weight_ref, first_ref, second_ref, blocks, tiles, sems,
):
    fetched = []
    for slot, (source, target) in enumerate(
        (
            (basis_hbm, basis_ref),
            (w0_hbm, blocks.at[0]),
            (b1_hbm, blocks.at[1]),
            (f1_hbm, blocks.at[2]),
            (w4_hbm, blocks.at[3]),
            (f2_hbm, blocks.at[4]),
            (b2_hbm, blocks.at[5]),
            (weight_hbm, weight_ref),
            (first_hbm, first_ref),
            (second_hbm, second_ref),
        )
    ):
        copy = pltpu.make_async_copy(source, target, sems.at[6 + slot])
        copy.start()
        fetched.append(copy)
    z, y = place_ref[0], place_ref[1]
    is_low = place_ref[3] == 0
    near, far = near_ref[:, :4].astype(jnp.float32), far_ref[:, :4].astype(jnp.float32)
    energy = jnp.sum(near * near + far * far)
    count = 2 * near.shape[0] * near.shape[1] * near.shape[2] * near.shape[3]
    spread = jnp.sqrt(jnp.full((1, 128), energy / count, jnp.float32))
    scales = -1.0 / (spread + 1e-06)
    scale_out[...] = scales
    scale = scales[:, :1]

    def rows_of(close, distant):
        close, distant = (array.reshape(-1, array.shape[-1]) for array in (close, distant))
        return jnp.concatenate(
            [jnp.where(is_low, close, distant), jnp.where(is_low, distant, close)], axis=1
        )

    def block_rows(block):
        peers, at = pl.ds(pl.multiple_of(block % 2 * 16, 16), 16), block % 8 // 2
        return rows_of(near_ref[peers, at], far_ref[peers, at])

    fetched[0].wait()
    basis = basis_ref[...]
    copies = []
    for slot, hops in enumerate((0, 1, 7, 4, 6, 2)):
        step = dot(basis, block_rows(z + hops), 1, 1) * scale
        fetched[slot + 1].wait()
        tiles[slot] = (blocks[slot].astype(jnp.float32) + step).astype(jnp.bfloat16)
        copy = pltpu.make_async_copy(tiles.at[slot], copy_ref.at[:, columns(z + hops)], sems.at[slot])
        copy.start()
        copies.append(copy)
    for slot, hops in enumerate((5, 3)):
        rows_out[slot] = block_rows(z + hops)

    for copy in fetched[7:]:
        copy.wait()
    first_letter = z % 2 * 16 + y * 4
    mine = pl.ds(first_letter, 4)
    step = dot(rows_of(near_ref[mine, z // 2], far_ref[mine, z // 2]), basis, 1, 1) * scale
    step_ref[...] = step
    new_ref[...] = weight_ref[...] + step
    for source in range(4):
        rows = pl.ds(source * 16, 16)
        letter = first_letter + source
        piece = near_ref[letter, 4].astype(jnp.float32) + near_ref[letter, 5].astype(jnp.float32)
        first_new, second_new = moments(piece, first_ref[rows, :], second_ref[rows, :])
        first_out[rows, :] = first_new
        second_out[rows, :] = second_new
    for copy in copies:
        copy.wait()


def finish(place, basis, weight, first, second, near, far, blocks):
    values, rank = basis.shape
    like = lambda array: jax.ShapeDtypeStruct(array.shape, jnp.float32)
    return pl.pallas_call(
        finish_kernel,
        in_specs=[SMEM] + [HBM] * 4 + [VMEM] * 2 + [HBM] * 6,
        out_specs=[VMEM, VMEM, HBM] + [VMEM] * 5,
        out_shape=[
            like(weight),
            like(weight),
            pltpu.HBM((values, 2048), jnp.bfloat16),
            like(first),
            like(second),
            pltpu.VMEM((2, 256, rank), jnp.bfloat16),
            pltpu.VMEM((1, 128), jnp.float32),
            pltpu.VMEM(basis.shape, basis.dtype),
        ],
        scratch_shapes=[
            pltpu.VMEM(weight.shape, weight.dtype),
            pltpu.VMEM(first.shape, first.dtype),
            pltpu.VMEM(second.shape, second.dtype),
            pltpu.VMEM((6, values, 256), jnp.bfloat16),
            pltpu.VMEM((6, values, 256), jnp.bfloat16),
            pltpu.SemaphoreType.DMA((16,)),
        ],
        compiler_params=limit(20),
        name="finish",
    )(place, *in_hbm(basis, weight, first, second), near, far, *in_hbm(*blocks))


def last_kernel(place_ref, rows_ref, scale_ref, basis_ref, f3, b3, copy_in, copy_ref, tiles, sems):
    z = place_ref[0]
    copies = []
    for slot, (block, hops) in enumerate(((f3, 5), (b3, 3))):
        step = dot(basis_ref[...], rows_ref[slot], 1, 1) * scale_ref[:, :1]
        tiles[slot] = (block[...].astype(jnp.float32) + step).astype(jnp.bfloat16)
        copy = pltpu.make_async_copy(tiles.at[slot], copy_ref.at[:, columns(z + hops)], sems.at[slot])
        copy.start()
        copies.append(copy)
    for copy in copies:
        copy.wait()


def last(place, later, f3, b3, copy):
    return pl.pallas_call(
        last_kernel,
        in_specs=[SMEM] + [VMEM] * 5 + [HBM],
        out_specs=HBM,
        out_shape=pltpu.HBM(copy.shape, copy.dtype),
        input_output_aliases={6: 0},
        scratch_shapes=[pltpu.VMEM((2, copy.shape[0], 256), copy.dtype), pltpu.SemaphoreType.DMA((2,))],
        compiler_params=limit(8),
        name="last",
    )(place, *in_vmem(*later), f3, b3, *in_hbm(copy))


def exchange(array, axes):
    return lax.all_to_all(array, axes, 0, 0, tiled=True)


def chain(first_mix, second_mix, lambda_head, head_gain, out_cotangent, basis, weight, first_moment, second_moment):
    place = jnp.stack([lax.axis_index(name).astype(jnp.int32) for name in (Z, "y", "x", "tp")])
    turned = weight.T
    own, sent, narrow = heads(place, lambda_head, first_mix, second_mix, head_gain, basis, turned)

    w0 = widen(place, [narrow] + [shift(narrow, "y", hops) for hops in (1, 2, 3)])
    opposite = shift(narrow, Z, 4)
    w4 = widen(place, [opposite] + [shift(opposite, "y", hops) for hops in (1, 2, 3)])
    f1, b1 = shift(w0, Z, 1), shift(w0, Z, -1)
    f2, b2 = shift(f1, Z, 1), shift(b1, Z, -1)
    f3, b3 = shift(f2, Z, 1), shift(b2, Z, -1)

    parts = gradient(own, swap_cores(sent), out_cotangent)
    sums = fold(place, exchange(parts, NEAR), first_moment, second_moment)
    near = exchange(update(place, exchange(sums, "zh")), NEAR)
    far = swap_cores(near)
    weight_new, step_out, most, first_new, second_new, *later = finish(
        place, basis, turned, first_moment, second_moment, near, far, (w0, b1, f1, w4, f2, b2)
    )
    weight_copy = last(place, later, f3, b3, most)
    return (weight_new.T, weight_copy, step_out.T, first_new, second_new)


def solution(mesh):
    finer = Mesh(
        mesh.devices.reshape(4, 2, 4, mesh.shape["rep"], mesh.shape["tp"]),
        (*FS_REP, "tp"),
    )
    return jax.shard_map(
        chain,
        mesh=finer,
        in_specs=(
            P(FS_REP, "tp"),
            P(FS_REP, "tp"),
            P("tp"),
            P(),
            P(FS_REP, None),
            P("tp", None),
            P("tp", FS),
            P(FS, "tp"),
            P(FS, "tp"),
        ),
        out_specs=(P("tp", FS), P("tp", None), P("tp", FS), P(FS, "tp"), P(FS, "tp")),
        check_vma=False,
    )
```

```python
import jax
import jax.numpy as jnp
from jax import lax
from jax.experimental import pallas as pl
from jax.experimental.pallas import tpu as pltpu
from jax.sharding import Mesh
from jax.sharding import PartitionSpec as P

OUT_SCALE = 0.8
BETA_FIRST = 0.9
BETA_SECOND = 0.95
FS = ("z", "y")
FS_REP = ("z", "y", "x")
SMEM = pl.BlockSpec(memory_space=pltpu.SMEM)
VMEM = pl.BlockSpec(memory_space=pltpu.VMEM)
HBM = pl.BlockSpec(memory_space=pltpu.HBM)
MIB = 1024 * 1024


def in_hbm(*arrays):
    return [pltpu.with_memory_space_constraint(array, pltpu.HBM) for array in arrays]


def in_vmem(*arrays):
    return [pltpu.with_memory_space_constraint(array, pltpu.VMEM) for array in arrays]


def shift(array, axis, hops):
    count = lax.axis_size(axis)
    return lax.ppermute(array, axis, [(i, (i + hops) % count) for i in range(count)])


def swap_cores(array):
    return lax.ppermute(array, "tp", [(0, 1), (1, 0)])


def dot(left, right, left_dim, right_dim):
    return lax.dot_general(
        left, right, (((left_dim,), (right_dim,)), ((), ())), preferred_element_type=jnp.float32
    )


def limit(mib):
    return pltpu.CompilerParams(vmem_limit_bytes=mib * MIB)


def heads_kernel(
    place_ref, lam_hbm, first_hbm, second_hbm, gain_hbm, basis_hbm, weight_hbm,
    own_ref, sent_ref, narrow_ref, first_ref, second_ref, basis_ref, lam_ref, gain_ref, weight_ref, sems,
):
    tokens, values = first_ref.shape
    width = gain_ref.shape[1]
    tile = tokens // 3

    def fetch(source, target, slot):
        copy = pltpu.make_async_copy(source, target, sems.at[slot])
        copy.start()
        return copy

    fixed = [fetch(lam_hbm, lam_ref, 0), fetch(gain_hbm, gain_ref, 1)]
    moving = []
    for step in range(3):
        rows = pl.ds(step * tile, tile)
        moving.append(
            [
                fetch(first_hbm.at[rows], first_ref.at[rows], 4 + 2 * step),
                fetch(second_hbm.at[rows], second_ref.at[rows], 5 + 2 * step),
            ]
        )
        if step == 0:
            fixed.append(fetch(basis_hbm, basis_ref, 2))
    last = fetch(weight_hbm, weight_ref, 3)
    for copy in fixed[:2]:
        copy.wait()
    gain = gain_ref[...] * OUT_SCALE
    is_low = place_ref[3] == 0
    for step in range(3):
        rows = pl.ds(step * tile, tile)
        for copy in moving[step]:
            copy.wait()
        if step == 0:
            fixed[2].wait()
        total = None
        for head in range(values // width):
            cols = slice(head * width, (head + 1) * width)
            first = first_ref[rows, cols].astype(jnp.float32)
            second = second_ref[rows, cols].astype(jnp.float32)
            mixture = first - lam_ref[:, head : head + 1] * second
            inverse = lax.rsqrt(jnp.mean(mixture * mixture, axis=-1, keepdims=True) + 1e-06)
            normed = (mixture * inverse * gain).astype(jnp.bfloat16)
            term = jnp.dot(normed, basis_ref[cols, :], preferred_element_type=jnp.float32)
            total = term if total is None else total + term
        half = total.shape[1] // 2
        low, high = total[:, :half], total[:, half:]
        own_ref[rows, :] = jnp.where(is_low, low, high)
        sent_ref[rows, :] = jnp.where(is_low, high, low).astype(jnp.bfloat16)
    last.wait()
    narrow_ref[...] = weight_ref[...].astype(jnp.bfloat16)


def heads(place, lambda_head, first_mix, second_mix, head_gain, basis, weight):
    tokens, values = first_mix.shape
    half = basis.shape[1] // 2
    lam, gain = lambda_head[None, :], head_gain[None, :]
    return pl.pallas_call(
        heads_kernel,
        in_specs=[SMEM] + [HBM] * 6,
        out_specs=[VMEM] * 3,
        out_shape=[
            jax.ShapeDtypeStruct((tokens, half), jnp.float32),
            jax.ShapeDtypeStruct((tokens, half), jnp.bfloat16),
            pltpu.VMEM(weight.shape, jnp.bfloat16),
        ],
        scratch_shapes=[
            pltpu.VMEM((tokens, values), jnp.bfloat16),
            pltpu.VMEM((tokens, values), jnp.bfloat16),
            pltpu.VMEM(basis.shape, jnp.bfloat16),
            pltpu.VMEM(lam.shape, jnp.float32),
            pltpu.VMEM(gain.shape, jnp.float32),
            pltpu.VMEM(weight.shape, jnp.float32),
            pltpu.SemaphoreType.DMA((10,)),
        ],
        compiler_params=limit(12),
        name="heads",
    )(place, *in_hbm(lam, first_mix, second_mix, gain, basis, weight))


def widen_kernel(place_ref, own_ref, one_ref, two_ref, three_ref, out_ref, slots):
    y = place_ref[1]
    slots[y] = own_ref[...].astype(jnp.float32)
    slots[(y + 3) % 4] = one_ref[...].astype(jnp.float32)
    slots[(y + 2) % 4] = two_ref[...].astype(jnp.float32)
    slots[(y + 1) % 4] = three_ref[...].astype(jnp.float32)
    rows = slots.shape[0] * slots.shape[1]
    out_ref[...] = slots[...].reshape(rows, slots.shape[2]).T.astype(jnp.bfloat16)


def widen(place, blocks):
    rows, cols = blocks[0].shape
    return pl.pallas_call(
        widen_kernel,
        in_specs=[SMEM] + [VMEM] * 4,
        out_specs=VMEM,
        out_shape=jax.ShapeDtypeStruct((cols, 4 * rows), jnp.bfloat16),
        scratch_shapes=[pltpu.VMEM((4, rows, cols), jnp.float32)],
        compiler_params=limit(8),
        name="widen",
    )(place, *blocks)


def gradient_kernel(own_ref, far_ref, cot_ref, out_hbm, parts, sems):
    reduced = (own_ref[...] + far_ref[...].astype(jnp.float32)).T.astype(jnp.bfloat16)
    wide = 512
    copies = []
    for at in range(cot_ref.shape[1] // wide):
        block = dot(reduced, cot_ref[:, at * wide : (at + 1) * wide], 1, 0).T.astype(jnp.bfloat16)
        for z in range(2):
            rows = block[z * 256 : (z + 1) * 256]
            parts[:, at * 2 + z] = rows.reshape(16, 16, rows.shape[1])
        pair = pl.ds(at * 2, 2)
        copy = pltpu.make_async_copy(parts.at[:, pair], out_hbm.at[:, pair], sems.at[at])
        copy.start()
        copies.append(copy)
    for copy in copies:
        copy.wait()


def gradient(own, far, cot):
    shape = (16, 8, 16, own.shape[1])
    return pl.pallas_call(
        gradient_kernel,
        in_specs=[VMEM] * 3,
        out_specs=HBM,
        out_shape=pltpu.HBM(shape, jnp.bfloat16),
        scratch_shapes=[pltpu.VMEM(shape, jnp.bfloat16), pltpu.SemaphoreType.DMA((4,))],
        compiler_params=limit(8),
        name="gradient",
    )(own, far, cot)


def send(pairs, sems):
    copies = []
    for slot, (source, target) in enumerate(pairs):
        copy = pltpu.make_async_copy(source, target, sems.at[slot])
        copy.start()
        copies.append(copy)
    for copy in copies:
        copy.wait()


def fold_kernel(place_ref, parts_ref, first_ref, second_ref, out_hbm, letter_ref, sems):
    rows = pl.ds(pl.multiple_of(place_ref[2] * 16, 16), 16)
    letter_ref[:8] = jnp.sum(parts_ref[...].astype(jnp.float32), axis=0).astype(jnp.bfloat16)
    letter_ref[8] = first_ref[rows, :].astype(jnp.bfloat16)
    letter_ref[9] = second_ref[rows, :].astype(jnp.bfloat16)
    send([(letter_ref, out_hbm.at[z]) for z in range(8)], sems)


def fold(place, parts, first, second):
    shape = (10, *parts.shape[2:])
    return pl.pallas_call(
        fold_kernel,
        in_specs=[SMEM] + [VMEM] * 3,
        out_specs=HBM,
        out_shape=pltpu.HBM((8, *shape), jnp.bfloat16),
        scratch_shapes=[pltpu.VMEM(shape, jnp.bfloat16), pltpu.SemaphoreType.DMA((8,))],
        compiler_params=limit(8),
        name="fold",
    )(place, parts, first, second)


def moments(projected, first, second):
    first_new = BETA_FIRST * first + (1.0 - BETA_FIRST) * projected
    second_new = BETA_SECOND * second + (1.0 - BETA_SECOND) * projected * projected
    return first_new, second_new


def update_kernel(place_ref, letters_ref, out_hbm, letter_ref, projected_ref, sems):
    projected_ref[...] = jnp.sum(letters_ref[:, :8].astype(jnp.float32), axis=0)
    first, second = letters_ref[:, 8].astype(jnp.float32), letters_ref[:, 9].astype(jnp.float32)
    first_new, second_new = moments(projected_ref[...], first, second)
    letter_ref[:8] = (first_new / (jnp.sqrt(second_new) + 1e-08)).astype(jnp.bfloat16)
    mine = projected_ref[place_ref[0]]
    high = mine.astype(jnp.bfloat16)
    letter_ref[8] = high
    letter_ref[9] = (mine - high.astype(jnp.float32)).astype(jnp.bfloat16)
    send([(letter_ref, out_hbm.at[peer]) for peer in range(16)], sems)


def update(place, letters):
    shape = letters.shape[1:]
    return pl.pallas_call(
        update_kernel,
        in_specs=[SMEM, VMEM],
        out_specs=HBM,
        out_shape=pltpu.HBM((16, *shape), jnp.bfloat16),
        scratch_shapes=[
            pltpu.VMEM(shape, jnp.bfloat16),
            pltpu.VMEM((8, *shape[1:]), jnp.float32),
            pltpu.SemaphoreType.DMA((16,)),
        ],
        compiler_params=limit(8),
        name="update",
    )(place, letters)


def columns(block):
    return pl.ds(pl.multiple_of(block % 8 * 256, 256), 256)


def finish_kernel(
    place_ref, basis_hbm, weight_hbm, first_hbm, second_hbm, near_ref, far_ref, w4, w0_hbm, b1_hbm, f1_hbm, f2_hbm, b2_hbm,
    new_ref, step_ref, copy_ref, first_out, second_out, later_ref, scale_out, basis_ref,
    weight_ref, first_ref, second_ref, blocks, tiles, sems,
):
    fetched = []
    for slot, (source, target) in enumerate(
        (
            (basis_hbm, basis_ref),
            (w0_hbm, blocks.at[0]),
            (b1_hbm, blocks.at[1]),
            (f1_hbm, blocks.at[2]),
            (f2_hbm, blocks.at[3]),
            (b2_hbm, blocks.at[4]),
            (weight_hbm, weight_ref),
            (first_hbm, first_ref),
            (second_hbm, second_ref),
        )
    ):
        copy = pltpu.make_async_copy(source, target, sems.at[6 + slot])
        copy.start()
        fetched.append(copy)
    z, y = place_ref[0], place_ref[1]
    is_low = place_ref[3] == 0
    near, far = near_ref[:, :8].astype(jnp.float32), far_ref[:, :8].astype(jnp.float32)
    energy = jnp.sum(near * near + far * far)
    count = 2 * near.shape[0] * near.shape[1] * near.shape[2] * near.shape[3]
    spread = jnp.sqrt(jnp.full((1, 128), energy / count, jnp.float32))
    scale_out[...] = -1.0 / (spread + 1e-06)
    scale = scale_out[:, :1]
    fetched[0].wait()
    basis = basis_ref[...]

    def rows_of(close, distant):
        close, distant = (array.reshape(-1, array.shape[-1]) for array in (close, distant))
        return jnp.concatenate(
            [jnp.where(is_low, close, distant), jnp.where(is_low, distant, close)], axis=1
        )

    def rows_at(block):
        at = block % 8
        return rows_of(near_ref[:, at], far_ref[:, at])

    def step_of(block):
        return dot(basis, rows_at(block), 1, 1) * scale

    copies = []
    for slot, hops in enumerate((4, 0, 1, 7, 6, 2)):
        step = step_of(z + hops)
        if slot:
            fetched[slot].wait()
        block = blocks[slot - 1] if slot else w4[...]
        tiles[slot] = (block.astype(jnp.float32) + step).astype(jnp.bfloat16)
        copy = pltpu.make_async_copy(tiles.at[slot], copy_ref.at[:, columns(z + hops)], sems.at[slot])
        copy.start()
        copies.append(copy)
    for slot, hops in enumerate((5, 3)):
        later_ref[slot] = rows_at(z + hops)

    for copy in fetched[6:]:
        copy.wait()
    mine = pl.ds(y * 4, 4)
    step = dot(rows_of(near_ref[mine, z], far_ref[mine, z]), basis, 1, 1) * scale
    step_ref[...] = step
    new_ref[...] = weight_ref[...] + step
    for source in range(4):
        rows = pl.ds(source * 16, 16)
        letter = y * 4 + source
        piece = near_ref[letter, 8].astype(jnp.float32) + near_ref[letter, 9].astype(jnp.float32)
        first_new, second_new = moments(piece, first_ref[rows, :], second_ref[rows, :])
        first_out[rows, :] = first_new
        second_out[rows, :] = second_new
    for copy in copies:
        copy.wait()


def finish(place, basis, weight, first, second, near, far, blocks):
    values = basis.shape[0]
    like = lambda array: jax.ShapeDtypeStruct(array.shape, jnp.float32)
    return pl.pallas_call(
        finish_kernel,
        in_specs=[SMEM] + [HBM] * 4 + [VMEM] * 3 + [HBM] * 5,
        out_specs=[VMEM, VMEM, HBM] + [VMEM] * 5,
        out_shape=[
            like(weight),
            like(weight),
            pltpu.HBM((values, 2048), jnp.bfloat16),
            like(first),
            like(second),
            pltpu.VMEM((2, 256, 256), jnp.bfloat16),
            pltpu.VMEM((1, 128), jnp.float32),
            pltpu.VMEM(basis.shape, basis.dtype),
        ],
        scratch_shapes=[
            pltpu.VMEM(weight.shape, weight.dtype),
            pltpu.VMEM(first.shape, first.dtype),
            pltpu.VMEM(second.shape, second.dtype),
            pltpu.VMEM((5, values, 256), jnp.bfloat16),
            pltpu.VMEM((6, values, 256), jnp.bfloat16),
            pltpu.SemaphoreType.DMA((15,)),
        ],
        compiler_params=limit(16),
        name="finish",
    )(place, *in_hbm(basis, weight, first, second), near, far, blocks[0], *in_hbm(*blocks[1:]))


def last_kernel(place_ref, rows_ref, scale_ref, basis_ref, f3, b3, copy_in, copy_ref, tiles, sems):
    z = place_ref[0]
    copies = []
    for slot, (block, hops) in enumerate(((f3, 5), (b3, 3))):
        step = dot(basis_ref[...], rows_ref[slot], 1, 1) * scale_ref[:, :1]
        tiles[slot] = (block[...].astype(jnp.float32) + step).astype(jnp.bfloat16)
        copy = pltpu.make_async_copy(tiles.at[slot], copy_ref.at[:, columns(z + hops)], sems.at[slot])
        copy.start()
        copies.append(copy)
    for copy in copies:
        copy.wait()


def last(place, later, f3, b3, copy):
    return pl.pallas_call(
        last_kernel,
        in_specs=[SMEM] + [VMEM] * 5 + [HBM],
        out_specs=HBM,
        out_shape=pltpu.HBM(copy.shape, copy.dtype),
        input_output_aliases={6: 0},
        scratch_shapes=[pltpu.VMEM((2, copy.shape[0], 256), copy.dtype), pltpu.SemaphoreType.DMA((2,))],
        compiler_params=limit(8),
        name="last",
    )(place, *in_vmem(*later), f3, b3, *in_hbm(copy))


def exchange(array, axes):
    return lax.all_to_all(array, axes, 0, 0, tiled=True)


def chain(first_mix, second_mix, lambda_head, head_gain, out_cotangent, basis, weight, first_moment, second_moment):
    place = jnp.stack([lax.axis_index(name).astype(jnp.int32) for name in ("z", "y", "x", "tp")])
    turned = weight.T
    own, sent, narrow = heads(place, lambda_head, first_mix, second_mix, head_gain, basis, turned)

    w0 = widen(place, [narrow] + [shift(narrow, "y", hops) for hops in (1, 2, 3)])
    opposite = shift(narrow, "z", 4)
    w4 = widen(place, [opposite] + [shift(opposite, "y", hops) for hops in (1, 2, 3)])
    f1, b1 = shift(w0, "z", 1), shift(w0, "z", -1)
    f2, b2 = shift(f1, "z", 1), shift(b1, "z", -1)
    f3, b3 = shift(f2, "z", 1), shift(b2, "z", -1)

    parts = gradient(own, swap_cores(sent), out_cotangent)
    sums = fold(place, exchange(parts, ("y", "x")), first_moment, second_moment)
    near = exchange(update(place, exchange(sums, "z")), ("y", "x"))
    far = swap_cores(near)
    weight_new, step_out, most, first_new, second_new, *later = finish(
        place, basis, turned, first_moment, second_moment, near, far, (w4, w0, b1, f1, f2, b2)
    )
    weight_copy = last(place, later, f3, b3, most)
    return (weight_new.T, weight_copy, step_out.T, first_new, second_new)


def solution(mesh):
    finer = Mesh(
        mesh.devices.reshape(8, 4, mesh.shape["rep"], mesh.shape["tp"]),
        ("z", "y", "x", "tp"),
    )
    return jax.shard_map(
        chain,
        mesh=finer,
        in_specs=(
            P(FS_REP, "tp"),
            P(FS_REP, "tp"),
            P("tp"),
            P(),
            P(FS_REP, None),
            P("tp", None),
            P("tp", FS),
            P(FS, "tp"),
            P(FS, "tp"),
        ),
        out_specs=(P("tp", FS), P("tp", None), P("tp", FS), P(FS, "tp"), P(FS, "tp")),
        check_vma=False,
    )
```

```python
import jax
import jax.numpy as jnp
from jax import lax
from jax.experimental import pallas as pl
from jax.experimental.pallas import tpu as pltpu
from jax.sharding import Mesh
from jax.sharding import PartitionSpec as P

OUT_SCALE = 0.8
BETA_FIRST = 0.9
BETA_SECOND = 0.95
FS = ("z", "y")
FS_REP = ("z", "y", "x")
SMEM = pl.BlockSpec(memory_space=pltpu.SMEM)
VMEM = pl.BlockSpec(memory_space=pltpu.VMEM)
HBM = pl.BlockSpec(memory_space=pltpu.HBM)
MIB = 1024 * 1024


def in_hbm(*arrays):
    return [pltpu.with_memory_space_constraint(array, pltpu.HBM) for array in arrays]


def in_vmem(*arrays):
    return [pltpu.with_memory_space_constraint(array, pltpu.VMEM) for array in arrays]


def shift(array, axis, hops):
    count = lax.axis_size(axis)
    return lax.ppermute(array, axis, [(i, (i + hops) % count) for i in range(count)])


def swap_cores(array):
    return lax.ppermute(array, "tp", [(0, 1), (1, 0)])


def dot(left, right, left_dim, right_dim):
    return lax.dot_general(
        left, right, (((left_dim,), (right_dim,)), ((), ())), preferred_element_type=jnp.float32
    )


def limit(mib):
    return pltpu.CompilerParams(vmem_limit_bytes=mib * MIB)


def heads_kernel(
    place_ref, lam_hbm, first_hbm, second_hbm, gain_hbm, basis_hbm, weight_hbm,
    own_ref, sent_ref, narrow_ref, first_ref, second_ref, basis_ref, lam_ref, gain_ref, weight_ref, sems,
):
    tokens, values = first_ref.shape
    width = gain_ref.shape[1]
    tile = tokens // 3

    def fetch(source, target, slot):
        copy = pltpu.make_async_copy(source, target, sems.at[slot])
        copy.start()
        return copy

    fixed = [fetch(lam_hbm, lam_ref, 0), fetch(gain_hbm, gain_ref, 1)]
    moving = []
    for step in range(3):
        rows = pl.ds(step * tile, tile)
        moving.append(
            [
                fetch(first_hbm.at[rows], first_ref.at[rows], 4 + 2 * step),
                fetch(second_hbm.at[rows], second_ref.at[rows], 5 + 2 * step),
            ]
        )
        if step == 0:
            fixed.append(fetch(basis_hbm, basis_ref, 2))
    last = fetch(weight_hbm, weight_ref, 3)
    for copy in fixed[:2]:
        copy.wait()
    gain = gain_ref[...] * OUT_SCALE
    is_low = place_ref[3] == 0
    for step in range(3):
        rows = pl.ds(step * tile, tile)
        for copy in moving[step]:
            copy.wait()
        if step == 0:
            fixed[2].wait()
        total = None
        for head in range(values // width):
            cols = slice(head * width, (head + 1) * width)
            first = first_ref[rows, cols].astype(jnp.float32)
            second = second_ref[rows, cols].astype(jnp.float32)
            mixture = first - lam_ref[:, head : head + 1] * second
            inverse = lax.rsqrt(jnp.mean(mixture * mixture, axis=-1, keepdims=True) + 1e-06)
            normed = (mixture * inverse * gain).astype(jnp.bfloat16)
            term = jnp.dot(normed, basis_ref[cols, :], preferred_element_type=jnp.float32)
            total = term if total is None else total + term
        half = total.shape[1] // 2
        low, high = total[:, :half], total[:, half:]
        own_ref[rows, :] = jnp.where(is_low, low, high)
        sent_ref[rows, :] = jnp.where(is_low, high, low).astype(jnp.bfloat16)
    last.wait()
    narrow_ref[...] = weight_ref[...].astype(jnp.bfloat16)


def heads(place, lambda_head, first_mix, second_mix, head_gain, basis, weight):
    tokens, values = first_mix.shape
    half = basis.shape[1] // 2
    lam, gain = lambda_head[None, :], head_gain[None, :]
    return pl.pallas_call(
        heads_kernel,
        in_specs=[SMEM] + [HBM] * 6,
        out_specs=[VMEM] * 3,
        out_shape=[
            jax.ShapeDtypeStruct((tokens, half), jnp.float32),
            jax.ShapeDtypeStruct((tokens, half), jnp.bfloat16),
            pltpu.VMEM(weight.shape, jnp.bfloat16),
        ],
        scratch_shapes=[
            pltpu.VMEM((tokens, values), jnp.bfloat16),
            pltpu.VMEM((tokens, values), jnp.bfloat16),
            pltpu.VMEM(basis.shape, jnp.bfloat16),
            pltpu.VMEM(lam.shape, jnp.float32),
            pltpu.VMEM(gain.shape, jnp.float32),
            pltpu.VMEM(weight.shape, jnp.float32),
            pltpu.SemaphoreType.DMA((10,)),
        ],
        compiler_params=limit(12),
        name="heads",
    )(place, *in_hbm(lam, first_mix, second_mix, gain, basis, weight))


def widen_kernel(place_ref, own_ref, one_ref, two_ref, three_ref, out_ref, slots):
    y = place_ref[1]
    slots[y] = own_ref[...].astype(jnp.float32)
    slots[(y + 3) % 4] = one_ref[...].astype(jnp.float32)
    slots[(y + 2) % 4] = two_ref[...].astype(jnp.float32)
    slots[(y + 1) % 4] = three_ref[...].astype(jnp.float32)
    rows = slots.shape[0] * slots.shape[1]
    out_ref[...] = slots[...].reshape(rows, slots.shape[2]).T.astype(jnp.bfloat16)


def widen(place, blocks):
    rows, cols = blocks[0].shape
    return pl.pallas_call(
        widen_kernel,
        in_specs=[SMEM] + [VMEM] * 4,
        out_specs=VMEM,
        out_shape=jax.ShapeDtypeStruct((cols, 4 * rows), jnp.bfloat16),
        scratch_shapes=[pltpu.VMEM((4, rows, cols), jnp.float32)],
        compiler_params=limit(8),
        name="widen",
    )(place, *blocks)


def gradient_kernel(own_ref, far_ref, cot_ref, out_hbm, parts, sems):
    reduced = (own_ref[...] + far_ref[...].astype(jnp.float32)).T.astype(jnp.bfloat16)
    wide = 512
    copies = []
    for at in range(cot_ref.shape[1] // wide):
        block = dot(reduced, cot_ref[:, at * wide : (at + 1) * wide], 1, 0).T.astype(jnp.bfloat16)
        for z in range(2):
            rows = block[z * 256 : (z + 1) * 256]
            parts[:, at * 2 + z] = rows.reshape(16, 16, rows.shape[1])
        pair = pl.ds(at * 2, 2)
        copy = pltpu.make_async_copy(parts.at[:, pair], out_hbm.at[:, pair], sems.at[at])
        copy.start()
        copies.append(copy)
    for copy in copies:
        copy.wait()


def gradient(own, far, cot):
    shape = (16, 8, 16, own.shape[1])
    return pl.pallas_call(
        gradient_kernel,
        in_specs=[VMEM] * 3,
        out_specs=HBM,
        out_shape=pltpu.HBM(shape, jnp.bfloat16),
        scratch_shapes=[pltpu.VMEM(shape, jnp.bfloat16), pltpu.SemaphoreType.DMA((4,))],
        compiler_params=limit(8),
        name="gradient",
    )(own, far, cot)


def send(pairs, sems):
    copies = []
    for slot, (source, target) in enumerate(pairs):
        copy = pltpu.make_async_copy(source, target, sems.at[slot])
        copy.start()
        copies.append(copy)
    for copy in copies:
        copy.wait()


def fold_kernel(place_ref, parts_ref, first_ref, second_ref, out_hbm, letter_ref, sems):
    rows = pl.ds(pl.multiple_of(place_ref[2] * 16, 16), 16)
    letter_ref[:8] = jnp.sum(parts_ref[...].astype(jnp.float32), axis=0).astype(jnp.bfloat16)
    letter_ref[8] = first_ref[rows, :].astype(jnp.bfloat16)
    letter_ref[9] = second_ref[rows, :].astype(jnp.bfloat16)
    send([(letter_ref, out_hbm.at[z]) for z in range(8)], sems)


def fold(place, parts, first, second):
    shape = (10, *parts.shape[2:])
    return pl.pallas_call(
        fold_kernel,
        in_specs=[SMEM] + [VMEM] * 3,
        out_specs=HBM,
        out_shape=pltpu.HBM((8, *shape), jnp.bfloat16),
        scratch_shapes=[pltpu.VMEM(shape, jnp.bfloat16), pltpu.SemaphoreType.DMA((8,))],
        compiler_params=limit(8),
        name="fold",
    )(place, parts, first, second)


def moments(projected, first, second):
    first_new = BETA_FIRST * first + (1.0 - BETA_FIRST) * projected
    second_new = BETA_SECOND * second + (1.0 - BETA_SECOND) * projected * projected
    return first_new, second_new


def update_kernel(place_ref, letters_ref, out_hbm, letter_ref, projected_ref, sems):
    projected_ref[...] = jnp.sum(letters_ref[:, :8].astype(jnp.float32), axis=0)
    first, second = letters_ref[:, 8].astype(jnp.float32), letters_ref[:, 9].astype(jnp.float32)
    first_new, second_new = moments(projected_ref[...], first, second)
    letter_ref[:8] = (first_new / (jnp.sqrt(second_new) + 1e-08)).astype(jnp.bfloat16)
    mine = projected_ref[place_ref[0]]
    high = mine.astype(jnp.bfloat16)
    letter_ref[8] = high
    letter_ref[9] = (mine - high.astype(jnp.float32)).astype(jnp.bfloat16)
    send([(letter_ref, out_hbm.at[peer]) for peer in range(16)], sems)


def update(place, letters):
    shape = letters.shape[1:]
    return pl.pallas_call(
        update_kernel,
        in_specs=[SMEM, VMEM],
        out_specs=HBM,
        out_shape=pltpu.HBM((16, *shape), jnp.bfloat16),
        scratch_shapes=[
            pltpu.VMEM(shape, jnp.bfloat16),
            pltpu.VMEM((8, *shape[1:]), jnp.float32),
            pltpu.SemaphoreType.DMA((16,)),
        ],
        compiler_params=limit(8),
        name="update",
    )(place, letters)


def columns(block):
    return pl.ds(pl.multiple_of(block % 8 * 256, 256), 256)


def finish_kernel(
    place_ref, basis_hbm, weight_hbm, first_hbm, second_hbm, near_ref, far_ref, w0, w4, b1, f1_hbm, f2_hbm, b2_hbm,
    new_ref, step_ref, copy_ref, first_out, second_out, later_ref, scale_out, basis_ref,
    weight_ref, first_ref, second_ref, blocks, tiles, sems,
):
    fetched = []
    for slot, (source, target) in enumerate(
        (
            (basis_hbm, basis_ref),
            (f1_hbm, blocks.at[0]),
            (f2_hbm, blocks.at[1]),
            (b2_hbm, blocks.at[2]),
            (weight_hbm, weight_ref),
            (first_hbm, first_ref),
            (second_hbm, second_ref),
        )
    ):
        copy = pltpu.make_async_copy(source, target, sems.at[6 + slot])
        copy.start()
        fetched.append(copy)
    z, y = place_ref[0], place_ref[1]
    is_low = place_ref[3] == 0
    near, far = near_ref[:, :8].astype(jnp.float32), far_ref[:, :8].astype(jnp.float32)
    energy = jnp.sum(near * near + far * far)
    count = 2 * near.shape[0] * near.shape[1] * near.shape[2] * near.shape[3]
    spread = jnp.sqrt(jnp.full((1, 128), energy / count, jnp.float32))
    scale_out[...] = -1.0 / (spread + 1e-06)
    scale = scale_out[:, :1]
    fetched[0].wait()
    basis = basis_ref[...]

    def rows_of(close, distant):
        close, distant = (array.reshape(-1, array.shape[-1]) for array in (close, distant))
        return jnp.concatenate(
            [jnp.where(is_low, close, distant), jnp.where(is_low, distant, close)], axis=1
        )

    def rows_at(block):
        at = block % 8
        return rows_of(near_ref[:, at], far_ref[:, at])

    def step_of(block):
        return dot(basis, rows_at(block), 1, 1) * scale

    copies = []
    near_blocks = ((w0, 0), (w4, 4), (b1, 1), (blocks.at[0], 7), (blocks.at[1], 6), (blocks.at[2], 2))
    for slot, (block, hops) in enumerate(near_blocks):
        if slot >= 3:
            fetched[slot - 2].wait()
        tiles[slot] = (block[...].astype(jnp.float32) + step_of(z + hops)).astype(jnp.bfloat16)
        copy = pltpu.make_async_copy(tiles.at[slot], copy_ref.at[:, columns(z + hops)], sems.at[slot])
        copy.start()
        copies.append(copy)
    for slot, hops in enumerate((5, 3)):
        later_ref[slot] = rows_at(z + hops)

    for copy in fetched[4:]:
        copy.wait()
    mine = pl.ds(y * 4, 4)
    step = dot(rows_of(near_ref[mine, z], far_ref[mine, z]), basis, 1, 1) * scale
    step_ref[...] = step
    new_ref[...] = weight_ref[...] + step
    for source in range(4):
        rows = pl.ds(source * 16, 16)
        letter = y * 4 + source
        piece = near_ref[letter, 8].astype(jnp.float32) + near_ref[letter, 9].astype(jnp.float32)
        first_new, second_new = moments(piece, first_ref[rows, :], second_ref[rows, :])
        first_out[rows, :] = first_new
        second_out[rows, :] = second_new
    for copy in copies:
        copy.wait()


def finish(place, basis, weight, first, second, near, far, blocks):
    values = basis.shape[0]
    like = lambda array: jax.ShapeDtypeStruct(array.shape, jnp.float32)
    return pl.pallas_call(
        finish_kernel,
        in_specs=[SMEM] + [HBM] * 4 + [VMEM] * 5 + [HBM] * 3,
        out_specs=[VMEM, VMEM, HBM] + [VMEM] * 5,
        out_shape=[
            like(weight),
            like(weight),
            pltpu.HBM((values, 2048), jnp.bfloat16),
            like(first),
            like(second),
            pltpu.VMEM((2, 256, 256), jnp.bfloat16),
            pltpu.VMEM((1, 128), jnp.float32),
            pltpu.VMEM(basis.shape, basis.dtype),
        ],
        scratch_shapes=[
            pltpu.VMEM(weight.shape, weight.dtype),
            pltpu.VMEM(first.shape, first.dtype),
            pltpu.VMEM(second.shape, second.dtype),
            pltpu.VMEM((3, values, 256), jnp.bfloat16),
            pltpu.VMEM((6, values, 256), jnp.bfloat16),
            pltpu.SemaphoreType.DMA((13,)),
        ],
        compiler_params=limit(16),
        name="finish",
    )(place, *in_hbm(basis, weight, first, second), near, far, *blocks[:3], *in_hbm(*blocks[3:]))


def last_kernel(place_ref, rows_ref, scale_ref, basis_ref, f3, b3, copy_in, copy_ref, tiles, sems):
    z = place_ref[0]
    copies = []
    for slot, (block, hops) in enumerate(((f3, 5), (b3, 3))):
        step = dot(basis_ref[...], rows_ref[slot], 1, 1) * scale_ref[:, :1]
        tiles[slot] = (block[...].astype(jnp.float32) + step).astype(jnp.bfloat16)
        copy = pltpu.make_async_copy(tiles.at[slot], copy_ref.at[:, columns(z + hops)], sems.at[slot])
        copy.start()
        copies.append(copy)
    for copy in copies:
        copy.wait()


def last(place, later, f3, b3, copy):
    return pl.pallas_call(
        last_kernel,
        in_specs=[SMEM] + [VMEM] * 5 + [HBM],
        out_specs=HBM,
        out_shape=pltpu.HBM(copy.shape, copy.dtype),
        input_output_aliases={6: 0},
        scratch_shapes=[pltpu.VMEM((2, copy.shape[0], 256), copy.dtype), pltpu.SemaphoreType.DMA((2,))],
        compiler_params=limit(8),
        name="last",
    )(place, *in_vmem(*later), f3, b3, *in_hbm(copy))


def exchange(array, axes):
    return lax.all_to_all(array, axes, 0, 0, tiled=True)


def chain(first_mix, second_mix, lambda_head, head_gain, out_cotangent, basis, weight, first_moment, second_moment):
    place = jnp.stack([lax.axis_index(name).astype(jnp.int32) for name in ("z", "y", "x", "tp")])
    turned = weight.T
    own, sent, narrow = heads(place, lambda_head, first_mix, second_mix, head_gain, basis, turned)

    w0 = widen(place, [narrow] + [shift(narrow, "y", hops) for hops in (1, 2, 3)])
    opposite = shift(narrow, "z", 4)
    w4 = widen(place, [opposite] + [shift(opposite, "y", hops) for hops in (1, 2, 3)])
    f1, b1 = shift(w0, "z", 1), shift(w0, "z", -1)
    f2, b2 = shift(f1, "z", 1), shift(b1, "z", -1)
    f3, b3 = shift(f2, "z", 1), shift(b2, "z", -1)

    parts = gradient(own, swap_cores(sent), out_cotangent)
    sums = fold(place, exchange(parts, ("y", "x")), first_moment, second_moment)
    near = exchange(update(place, exchange(sums, "z")), ("y", "x"))
    far = swap_cores(near)
    weight_new, step_out, most, first_new, second_new, *later = finish(
        place, basis, turned, first_moment, second_moment, near, far, (w0, w4, b1, f1, f2, b2)
    )
    weight_copy = last(place, later, f3, b3, most)
    return (weight_new.T, weight_copy, step_out.T, first_new, second_new)


def solution(mesh):
    finer = Mesh(
        mesh.devices.reshape(8, 4, mesh.shape["rep"], mesh.shape["tp"]),
        ("z", "y", "x", "tp"),
    )
    return jax.shard_map(
        chain,
        mesh=finer,
        in_specs=(
            P(FS_REP, "tp"),
            P(FS_REP, "tp"),
            P("tp"),
            P(),
            P(FS_REP, None),
            P("tp", None),
            P("tp", FS),
            P(FS, "tp"),
            P(FS, "tp"),
        ),
        out_specs=(P("tp", FS), P("tp", None), P("tp", FS), P(FS, "tp"), P(FS, "tp")),
        check_vma=False,
    )
```

```python
import jax
import jax.numpy as jnp
from jax import lax
from jax.experimental import pallas as pl
from jax.experimental.pallas import tpu as pltpu
from jax.sharding import Mesh
from jax.sharding import PartitionSpec as P

OUT_SCALE = 0.8
BETA_FIRST = 0.9
BETA_SECOND = 0.95
FS = ("z", "y")
FS_REP = ("z", "y", "x")
SMEM = pl.BlockSpec(memory_space=pltpu.SMEM)
VMEM = pl.BlockSpec(memory_space=pltpu.VMEM)
HBM = pl.BlockSpec(memory_space=pltpu.HBM)
MIB = 1024 * 1024


def in_hbm(*arrays):
    return [pltpu.with_memory_space_constraint(array, pltpu.HBM) for array in arrays]


def in_vmem(*arrays):
    return [pltpu.with_memory_space_constraint(array, pltpu.VMEM) for array in arrays]


def shift(array, axis, hops):
    count = lax.axis_size(axis)
    return lax.ppermute(array, axis, [(i, (i + hops) % count) for i in range(count)])


def swap_cores(array):
    return lax.ppermute(array, "tp", [(0, 1), (1, 0)])


def dot(left, right, left_dim, right_dim):
    return lax.dot_general(
        left, right, (((left_dim,), (right_dim,)), ((), ())), preferred_element_type=jnp.float32
    )


def limit(mib):
    return pltpu.CompilerParams(vmem_limit_bytes=mib * MIB)


def heads_kernel(
    place_ref, lam_hbm, first_hbm, second_hbm, gain_hbm, basis_hbm, weight_hbm,
    own_ref, sent_ref, narrow_ref, first_ref, second_ref, basis_ref, lam_ref, gain_ref, weight_ref, sems,
):
    tokens, values = first_ref.shape
    width = gain_ref.shape[1]
    steps = 6
    tile = tokens // steps

    def fetch(source, target, slot):
        copy = pltpu.make_async_copy(source, target, sems.at[slot])
        copy.start()
        return copy

    fixed = [fetch(lam_hbm, lam_ref, 0), fetch(gain_hbm, gain_ref, 1)]
    moving = []
    for step in range(steps):
        rows = pl.ds(step * tile, tile)
        moving.append(
            [
                fetch(first_hbm.at[rows], first_ref.at[rows], 4 + 2 * step),
                fetch(second_hbm.at[rows], second_ref.at[rows], 5 + 2 * step),
            ]
        )
        if step == 0:
            fixed.append(fetch(basis_hbm, basis_ref, 2))
    last = fetch(weight_hbm, weight_ref, 3)
    for copy in fixed[:2]:
        copy.wait()
    gain = gain_ref[...] * OUT_SCALE
    is_low = place_ref[3] == 0
    for step in range(steps):
        rows = pl.ds(step * tile, tile)
        for copy in moving[step]:
            copy.wait()
        if step == 0:
            fixed[2].wait()
        total = None
        for head in range(values // width):
            cols = slice(head * width, (head + 1) * width)
            first = first_ref[rows, cols].astype(jnp.float32)
            second = second_ref[rows, cols].astype(jnp.float32)
            mixture = first - lam_ref[:, head : head + 1] * second
            inverse = lax.rsqrt(jnp.mean(mixture * mixture, axis=-1, keepdims=True) + 1e-06)
            normed = (mixture * inverse * gain).astype(jnp.bfloat16)
            term = jnp.dot(normed, basis_ref[cols, :], preferred_element_type=jnp.float32)
            total = term if total is None else total + term
        half = total.shape[1] // 2
        low, high = total[:, :half], total[:, half:]
        own_ref[rows, :] = jnp.where(is_low, low, high)
        sent_ref[rows, :] = jnp.where(is_low, high, low).astype(jnp.bfloat16)
    last.wait()
    narrow_ref[...] = weight_ref[...].astype(jnp.bfloat16)


def heads(place, lambda_head, first_mix, second_mix, head_gain, basis, weight):
    tokens, values = first_mix.shape
    half = basis.shape[1] // 2
    lam, gain = lambda_head[None, :], head_gain[None, :]
    return pl.pallas_call(
        heads_kernel,
        in_specs=[SMEM] + [HBM] * 6,
        out_specs=[VMEM] * 3,
        out_shape=[
            jax.ShapeDtypeStruct((tokens, half), jnp.float32),
            jax.ShapeDtypeStruct((tokens, half), jnp.bfloat16),
            pltpu.VMEM(weight.shape, jnp.bfloat16),
        ],
        scratch_shapes=[
            pltpu.VMEM((tokens, values), jnp.bfloat16),
            pltpu.VMEM((tokens, values), jnp.bfloat16),
            pltpu.VMEM(basis.shape, jnp.bfloat16),
            pltpu.VMEM(lam.shape, jnp.float32),
            pltpu.VMEM(gain.shape, jnp.float32),
            pltpu.VMEM(weight.shape, jnp.float32),
            pltpu.SemaphoreType.DMA((16,)),
        ],
        compiler_params=limit(12),
        name="heads",
    )(place, *in_hbm(lam, first_mix, second_mix, gain, basis, weight))


def widen_kernel(place_ref, own_ref, one_ref, two_ref, three_ref, out_ref, slots):
    y = place_ref[1]
    slots[y] = own_ref[...].astype(jnp.float32)
    slots[(y + 3) % 4] = one_ref[...].astype(jnp.float32)
    slots[(y + 2) % 4] = two_ref[...].astype(jnp.float32)
    slots[(y + 1) % 4] = three_ref[...].astype(jnp.float32)
    rows = slots.shape[0] * slots.shape[1]
    out_ref[...] = slots[...].reshape(rows, slots.shape[2]).T.astype(jnp.bfloat16)


def widen(place, blocks):
    rows, cols = blocks[0].shape
    return pl.pallas_call(
        widen_kernel,
        in_specs=[SMEM] + [VMEM] * 4,
        out_specs=VMEM,
        out_shape=jax.ShapeDtypeStruct((cols, 4 * rows), jnp.bfloat16),
        scratch_shapes=[pltpu.VMEM((4, rows, cols), jnp.float32)],
        compiler_params=limit(8),
        name="widen",
    )(place, *blocks)


def gradient_kernel(own_ref, far_ref, cot_ref, out_hbm, parts, sems):
    reduced = (own_ref[...] + far_ref[...].astype(jnp.float32)).T.astype(jnp.bfloat16)
    wide = 512
    copies = []
    for at in range(cot_ref.shape[1] // wide):
        block = dot(reduced, cot_ref[:, at * wide : (at + 1) * wide], 1, 0).T.astype(jnp.bfloat16)
        for z in range(2):
            rows = block[z * 256 : (z + 1) * 256]
            parts[:, at * 2 + z] = rows.reshape(16, 16, rows.shape[1])
        pair = pl.ds(at * 2, 2)
        copy = pltpu.make_async_copy(parts.at[:, pair], out_hbm.at[:, pair], sems.at[at])
        copy.start()
        copies.append(copy)
    for copy in copies:
        copy.wait()


def gradient(own, far, cot):
    shape = (16, 8, 16, own.shape[1])
    return pl.pallas_call(
        gradient_kernel,
        in_specs=[VMEM] * 3,
        out_specs=HBM,
        out_shape=pltpu.HBM(shape, jnp.bfloat16),
        scratch_shapes=[pltpu.VMEM(shape, jnp.bfloat16), pltpu.SemaphoreType.DMA((4,))],
        compiler_params=limit(8),
        name="gradient",
    )(own, far, cot)


def send(pairs, sems):
    copies = []
    for slot, (source, target) in enumerate(pairs):
        copy = pltpu.make_async_copy(source, target, sems.at[slot])
        copy.start()
        copies.append(copy)
    for copy in copies:
        copy.wait()


def fold_kernel(place_ref, parts_ref, first_ref, second_ref, out_hbm, letter_ref, sems):
    rows = pl.ds(pl.multiple_of(place_ref[2] * 16, 16), 16)
    letter_ref[:8] = jnp.sum(parts_ref[...].astype(jnp.float32), axis=0).astype(jnp.bfloat16)
    letter_ref[8] = first_ref[rows, :].astype(jnp.bfloat16)
    letter_ref[9] = second_ref[rows, :].astype(jnp.bfloat16)
    send([(letter_ref, out_hbm.at[z]) for z in range(8)], sems)


def fold(place, parts, first, second):
    shape = (10, *parts.shape[2:])
    return pl.pallas_call(
        fold_kernel,
        in_specs=[SMEM] + [VMEM] * 3,
        out_specs=HBM,
        out_shape=pltpu.HBM((8, *shape), jnp.bfloat16),
        scratch_shapes=[pltpu.VMEM(shape, jnp.bfloat16), pltpu.SemaphoreType.DMA((8,))],
        compiler_params=limit(8),
        name="fold",
    )(place, parts, first, second)


def moments(projected, first, second):
    first_new = BETA_FIRST * first + (1.0 - BETA_FIRST) * projected
    second_new = BETA_SECOND * second + (1.0 - BETA_SECOND) * projected * projected
    return first_new, second_new


def update_kernel(place_ref, letters_ref, out_hbm, letter_ref, projected_ref, sems):
    projected_ref[...] = jnp.sum(letters_ref[:, :8].astype(jnp.float32), axis=0)
    first, second = letters_ref[:, 8].astype(jnp.float32), letters_ref[:, 9].astype(jnp.float32)
    first_new, second_new = moments(projected_ref[...], first, second)
    letter_ref[:8] = (first_new / (jnp.sqrt(second_new) + 1e-08)).astype(jnp.bfloat16)
    mine = projected_ref[place_ref[0]]
    high = mine.astype(jnp.bfloat16)
    letter_ref[8] = high
    letter_ref[9] = (mine - high.astype(jnp.float32)).astype(jnp.bfloat16)
    send([(letter_ref, out_hbm.at[peer]) for peer in range(16)], sems)


def update(place, letters):
    shape = letters.shape[1:]
    return pl.pallas_call(
        update_kernel,
        in_specs=[SMEM, VMEM],
        out_specs=HBM,
        out_shape=pltpu.HBM((16, *shape), jnp.bfloat16),
        scratch_shapes=[
            pltpu.VMEM(shape, jnp.bfloat16),
            pltpu.VMEM((8, *shape[1:]), jnp.float32),
            pltpu.SemaphoreType.DMA((16,)),
        ],
        compiler_params=limit(8),
        name="update",
    )(place, letters)


def columns(block):
    return pl.ds(pl.multiple_of(block % 8 * 256, 256), 256)


def finish_kernel(
    place_ref, basis_hbm, weight_hbm, first_hbm, second_hbm, near_ref, far_ref, w0, w4, b1, f1_hbm, f2_hbm, b2_hbm,
    new_ref, step_ref, copy_ref, first_out, second_out, later_ref, scale_out, basis_ref,
    weight_ref, first_ref, second_ref, blocks, tiles, sems,
):
    fetched = []
    for slot, (source, target) in enumerate(
        (
            (basis_hbm, basis_ref),
            (f1_hbm, blocks.at[0]),
            (f2_hbm, blocks.at[1]),
            (b2_hbm, blocks.at[2]),
            (weight_hbm, weight_ref),
            (first_hbm, first_ref),
            (second_hbm, second_ref),
        )
    ):
        copy = pltpu.make_async_copy(source, target, sems.at[6 + slot])
        copy.start()
        fetched.append(copy)
    z, y = place_ref[0], place_ref[1]
    is_low = place_ref[3] == 0
    near, far = near_ref[:, :8].astype(jnp.float32), far_ref[:, :8].astype(jnp.float32)
    energy = jnp.sum(near * near + far * far)
    count = 2 * near.shape[0] * near.shape[1] * near.shape[2] * near.shape[3]
    spread = jnp.sqrt(jnp.full((1, 128), energy / count, jnp.float32))
    scale_out[...] = -1.0 / (spread + 1e-06)
    scale = scale_out[:, :1]
    fetched[0].wait()
    basis = basis_ref[...]

    def rows_of(close, distant):
        close, distant = (array.reshape(-1, array.shape[-1]) for array in (close, distant))
        return jnp.concatenate(
            [jnp.where(is_low, close, distant), jnp.where(is_low, distant, close)], axis=1
        )

    def rows_at(block):
        at = block % 8
        return rows_of(near_ref[:, at], far_ref[:, at])

    def step_of(block):
        return dot(basis, rows_at(block), 1, 1) * scale

    copies = []
    near_blocks = ((w0, 0), (w4, 4), (b1, 1), (blocks.at[0], 7), (blocks.at[1], 6), (blocks.at[2], 2))
    for slot, (block, hops) in enumerate(near_blocks):
        if slot >= 3:
            fetched[slot - 2].wait()
        tiles[slot] = (block[...].astype(jnp.float32) + step_of(z + hops)).astype(jnp.bfloat16)
        copy = pltpu.make_async_copy(tiles.at[slot], copy_ref.at[:, columns(z + hops)], sems.at[slot])
        copy.start()
        copies.append(copy)
    for slot, hops in enumerate((5, 3)):
        later_ref[slot] = rows_at(z + hops)

    for copy in fetched[4:]:
        copy.wait()
    mine = pl.ds(y * 4, 4)
    step = dot(rows_of(near_ref[mine, z], far_ref[mine, z]), basis, 1, 1) * scale
    step_ref[...] = step
    new_ref[...] = weight_ref[...] + step
    for source in range(4):
        rows = pl.ds(source * 16, 16)
        letter = y * 4 + source
        piece = near_ref[letter, 8].astype(jnp.float32) + near_ref[letter, 9].astype(jnp.float32)
        first_new, second_new = moments(piece, first_ref[rows, :], second_ref[rows, :])
        first_out[rows, :] = first_new
        second_out[rows, :] = second_new
    for copy in copies:
        copy.wait()


def finish(place, basis, weight, first, second, near, far, blocks):
    values = basis.shape[0]
    like = lambda array: jax.ShapeDtypeStruct(array.shape, jnp.float32)
    return pl.pallas_call(
        finish_kernel,
        in_specs=[SMEM] + [HBM] * 4 + [VMEM] * 5 + [HBM] * 3,
        out_specs=[VMEM, VMEM, HBM] + [VMEM] * 5,
        out_shape=[
            like(weight),
            like(weight),
            pltpu.HBM((values, 2048), jnp.bfloat16),
            like(first),
            like(second),
            pltpu.VMEM((2, 256, 256), jnp.bfloat16),
            pltpu.VMEM((1, 128), jnp.float32),
            pltpu.VMEM(basis.shape, basis.dtype),
        ],
        scratch_shapes=[
            pltpu.VMEM(weight.shape, weight.dtype),
            pltpu.VMEM(first.shape, first.dtype),
            pltpu.VMEM(second.shape, second.dtype),
            pltpu.VMEM((3, values, 256), jnp.bfloat16),
            pltpu.VMEM((6, values, 256), jnp.bfloat16),
            pltpu.SemaphoreType.DMA((13,)),
        ],
        compiler_params=limit(16),
        name="finish",
    )(place, *in_hbm(basis, weight, first, second), near, far, *blocks[:3], *in_hbm(*blocks[3:]))


def last_kernel(place_ref, rows_ref, scale_ref, basis_ref, f3, b3, copy_in, copy_ref, tiles, sems):
    z = place_ref[0]
    copies = []
    for slot, (block, hops) in enumerate(((f3, 5), (b3, 3))):
        step = dot(basis_ref[...], rows_ref[slot], 1, 1) * scale_ref[:, :1]
        tiles[slot] = (block[...].astype(jnp.float32) + step).astype(jnp.bfloat16)
        copy = pltpu.make_async_copy(tiles.at[slot], copy_ref.at[:, columns(z + hops)], sems.at[slot])
        copy.start()
        copies.append(copy)
    for copy in copies:
        copy.wait()


def last(place, later, f3, b3, copy):
    return pl.pallas_call(
        last_kernel,
        in_specs=[SMEM] + [VMEM] * 5 + [HBM],
        out_specs=HBM,
        out_shape=pltpu.HBM(copy.shape, copy.dtype),
        input_output_aliases={6: 0},
        scratch_shapes=[pltpu.VMEM((2, copy.shape[0], 256), copy.dtype), pltpu.SemaphoreType.DMA((2,))],
        compiler_params=limit(8),
        name="last",
    )(place, *in_vmem(*later), f3, b3, *in_hbm(copy))


def exchange(array, axes):
    return lax.all_to_all(array, axes, 0, 0, tiled=True)


def chain(first_mix, second_mix, lambda_head, head_gain, out_cotangent, basis, weight, first_moment, second_moment):
    place = jnp.stack([lax.axis_index(name).astype(jnp.int32) for name in ("z", "y", "x", "tp")])
    turned = weight.T
    own, sent, narrow = heads(place, lambda_head, first_mix, second_mix, head_gain, basis, turned)

    w0 = widen(place, [narrow] + [shift(narrow, "y", hops) for hops in (1, 2, 3)])
    opposite = shift(narrow, "z", 4)
    w4 = widen(place, [opposite] + [shift(opposite, "y", hops) for hops in (1, 2, 3)])
    f1, b1 = shift(w0, "z", 1), shift(w0, "z", -1)
    f2, b2 = shift(f1, "z", 1), shift(b1, "z", -1)
    f3, b3 = shift(f2, "z", 1), shift(b2, "z", -1)

    parts = gradient(own, swap_cores(sent), out_cotangent)
    sums = fold(place, exchange(parts, ("y", "x")), first_moment, second_moment)
    near = exchange(update(place, exchange(sums, "z")), ("y", "x"))
    far = swap_cores(near)
    weight_new, step_out, most, first_new, second_new, *later = finish(
        place, basis, turned, first_moment, second_moment, near, far, (w0, w4, b1, f1, f2, b2)
    )
    weight_copy = last(place, later, f3, b3, most)
    return (weight_new.T, weight_copy, step_out.T, first_new, second_new)


def solution(mesh):
    finer = Mesh(
        mesh.devices.reshape(8, 4, mesh.shape["rep"], mesh.shape["tp"]),
        ("z", "y", "x", "tp"),
    )
    return jax.shard_map(
        chain,
        mesh=finer,
        in_specs=(
            P(FS_REP, "tp"),
            P(FS_REP, "tp"),
            P("tp"),
            P(),
            P(FS_REP, None),
            P("tp", None),
            P("tp", FS),
            P(FS, "tp"),
            P(FS, "tp"),
        ),
        out_specs=(P("tp", FS), P("tp", None), P("tp", FS), P(FS, "tp"), P(FS, "tp")),
        check_vma=False,
    )
```

```python
import jax
import jax.numpy as jnp
from jax import lax
from jax.experimental import pallas as pl
from jax.experimental.pallas import tpu as pltpu
from jax.sharding import Mesh
from jax.sharding import PartitionSpec as P

OUT_SCALE = 0.8
BETA_FIRST = 0.9
BETA_SECOND = 0.95
FS = ("z", "y")
FS_REP = ("z", "y", "x")
SMEM = pl.BlockSpec(memory_space=pltpu.SMEM)
VMEM = pl.BlockSpec(memory_space=pltpu.VMEM)
HBM = pl.BlockSpec(memory_space=pltpu.HBM)
MIB = 1024 * 1024


def in_hbm(*arrays):
    return [pltpu.with_memory_space_constraint(array, pltpu.HBM) for array in arrays]


def in_vmem(*arrays):
    return [pltpu.with_memory_space_constraint(array, pltpu.VMEM) for array in arrays]


def shift(array, axis, hops):
    count = lax.axis_size(axis)
    return lax.ppermute(array, axis, [(i, (i + hops) % count) for i in range(count)])


def swap_cores(array):
    return lax.ppermute(array, "tp", [(0, 1), (1, 0)])


def dot(left, right, left_dim, right_dim):
    return lax.dot_general(
        left, right, (((left_dim,), (right_dim,)), ((), ())), preferred_element_type=jnp.float32
    )


def limit(mib):
    return pltpu.CompilerParams(vmem_limit_bytes=mib * MIB)


def heads_kernel(
    place_ref, lam_hbm, first_hbm, second_hbm, gain_hbm, basis_hbm, weight_hbm,
    own_ref, sent_ref, narrow_ref, first_ref, second_ref, basis_ref, lam_ref, gain_ref, weight_ref, sems,
):
    tokens, values = first_ref.shape
    width = gain_ref.shape[1]
    steps = 3
    tile = tokens // steps

    def fetch(source, target, slot):
        copy = pltpu.make_async_copy(source, target, sems.at[slot])
        copy.start()
        return copy

    fixed = [fetch(lam_hbm, lam_ref, 0), fetch(gain_hbm, gain_ref, 1)]
    moving = []
    for step in range(steps):
        rows = pl.ds(step * tile, tile)
        moving.append(
            [
                fetch(first_hbm.at[rows], first_ref.at[rows], 4 + 2 * step),
                fetch(second_hbm.at[rows], second_ref.at[rows], 5 + 2 * step),
            ]
        )
        if step == 0:
            fixed.append(fetch(basis_hbm, basis_ref, 2))
    last = fetch(weight_hbm, weight_ref, 3)
    for copy in fixed[:2]:
        copy.wait()
    gain = gain_ref[...] * OUT_SCALE
    is_low = place_ref[3] == 0
    for step in range(steps):
        rows = pl.ds(step * tile, tile)
        for copy in moving[step]:
            copy.wait()
        if step == 0:
            fixed[2].wait()
        total = None
        for head in range(values // width):
            cols = slice(head * width, (head + 1) * width)
            first = first_ref[rows, cols].astype(jnp.float32)
            second = second_ref[rows, cols].astype(jnp.float32)
            mixture = first - lam_ref[:, head : head + 1] * second
            inverse = lax.rsqrt(jnp.mean(mixture * mixture, axis=-1, keepdims=True) + 1e-06)
            normed = (mixture * inverse * gain).astype(jnp.bfloat16)
            term = jnp.dot(normed, basis_ref[cols, :], preferred_element_type=jnp.float32)
            total = term if total is None else total + term
        half = total.shape[1] // 2
        low, high = total[:, :half], total[:, half:]
        own_ref[rows, :] = jnp.where(is_low, low, high)
        sent_ref[rows, :] = jnp.where(is_low, high, low).astype(jnp.bfloat16)
    last.wait()
    narrow_ref[...] = weight_ref[...].astype(jnp.bfloat16)


def heads(place, lambda_head, first_mix, second_mix, head_gain, basis, weight):
    tokens, values = first_mix.shape
    half = basis.shape[1] // 2
    lam, gain = lambda_head[None, :], head_gain[None, :]
    return pl.pallas_call(
        heads_kernel,
        in_specs=[SMEM] + [HBM] * 6,
        out_specs=[VMEM] * 3,
        out_shape=[
            jax.ShapeDtypeStruct((tokens, half), jnp.float32),
            jax.ShapeDtypeStruct((tokens, half), jnp.bfloat16),
            pltpu.VMEM(weight.shape, jnp.bfloat16),
        ],
        scratch_shapes=[
            pltpu.VMEM((tokens, values), jnp.bfloat16),
            pltpu.VMEM((tokens, values), jnp.bfloat16),
            pltpu.VMEM(basis.shape, jnp.bfloat16),
            pltpu.VMEM(lam.shape, jnp.float32),
            pltpu.VMEM(gain.shape, jnp.float32),
            pltpu.VMEM(weight.shape, jnp.float32),
            pltpu.SemaphoreType.DMA((16,)),
        ],
        compiler_params=limit(12),
        name="heads",
    )(place, *in_hbm(lam, first_mix, second_mix, gain, basis, weight))


def widen_kernel(place_ref, own_ref, one_ref, two_ref, three_ref, out_ref, slots):
    y = place_ref[1]
    slots[y] = own_ref[...].astype(jnp.float32)
    slots[(y + 3) % 4] = one_ref[...].astype(jnp.float32)
    slots[(y + 2) % 4] = two_ref[...].astype(jnp.float32)
    slots[(y + 1) % 4] = three_ref[...].astype(jnp.float32)
    rows = slots.shape[0] * slots.shape[1]
    out_ref[...] = slots[...].reshape(rows, slots.shape[2]).T.astype(jnp.bfloat16)


def widen(place, blocks):
    rows, cols = blocks[0].shape
    return pl.pallas_call(
        widen_kernel,
        in_specs=[SMEM] + [VMEM] * 4,
        out_specs=VMEM,
        out_shape=jax.ShapeDtypeStruct((cols, 4 * rows), jnp.bfloat16),
        scratch_shapes=[pltpu.VMEM((4, rows, cols), jnp.float32)],
        compiler_params=limit(8),
        name="widen",
    )(place, *blocks)


def gradient_kernel(own_ref, far_ref, cot_ref, out_hbm, parts, sems):
    reduced = (own_ref[...] + far_ref[...].astype(jnp.float32)).T.astype(jnp.bfloat16)
    wide = 512
    copies = []
    for at in range(cot_ref.shape[1] // wide):
        block = dot(reduced, cot_ref[:, at * wide : (at + 1) * wide], 1, 0).T.astype(jnp.bfloat16)
        for z in range(2):
            rows = block[z * 256 : (z + 1) * 256]
            parts[:, at * 2 + z] = rows.reshape(16, 16, rows.shape[1])
        pair = pl.ds(at * 2, 2)
        copy = pltpu.make_async_copy(parts.at[:, pair], out_hbm.at[:, pair], sems.at[at])
        copy.start()
        copies.append(copy)
    for copy in copies:
        copy.wait()


def gradient(own, far, cot):
    shape = (16, 8, 16, own.shape[1])
    return pl.pallas_call(
        gradient_kernel,
        in_specs=[VMEM] * 3,
        out_specs=HBM,
        out_shape=pltpu.HBM(shape, jnp.bfloat16),
        scratch_shapes=[pltpu.VMEM(shape, jnp.bfloat16), pltpu.SemaphoreType.DMA((4,))],
        compiler_params=limit(8),
        name="gradient",
    )(own, far, cot)


def send(pairs, sems):
    copies = []
    for slot, (source, target) in enumerate(pairs):
        copy = pltpu.make_async_copy(source, target, sems.at[slot])
        copy.start()
        copies.append(copy)
    for copy in copies:
        copy.wait()


def fold_kernel(place_ref, parts_ref, first_ref, second_ref, out_hbm, letter_ref, sems):
    rows = pl.ds(pl.multiple_of(place_ref[2] * 16, 16), 16)
    letter_ref[:8] = jnp.sum(parts_ref[...].astype(jnp.float32), axis=0).astype(jnp.bfloat16)
    letter_ref[8] = first_ref[rows, :].astype(jnp.bfloat16)
    letter_ref[9] = second_ref[rows, :].astype(jnp.bfloat16)
    send([(letter_ref, out_hbm.at[z]) for z in range(8)], sems)


def fold(place, parts, first, second):
    shape = (10, *parts.shape[2:])
    return pl.pallas_call(
        fold_kernel,
        in_specs=[SMEM] + [VMEM] * 3,
        out_specs=HBM,
        out_shape=pltpu.HBM((8, *shape), jnp.bfloat16),
        scratch_shapes=[pltpu.VMEM(shape, jnp.bfloat16), pltpu.SemaphoreType.DMA((8,))],
        compiler_params=limit(8),
        name="fold",
    )(place, parts, first, second)


def moments(projected, first, second):
    first_new = BETA_FIRST * first + (1.0 - BETA_FIRST) * projected
    second_new = BETA_SECOND * second + (1.0 - BETA_SECOND) * projected * projected
    return first_new, second_new


def update_kernel(place_ref, letters_ref, out_hbm, letter_ref, projected_ref, sems):
    projected_ref[...] = jnp.sum(letters_ref[:, :8].astype(jnp.float32), axis=0)
    first, second = letters_ref[:, 8].astype(jnp.float32), letters_ref[:, 9].astype(jnp.float32)
    first_new, second_new = moments(projected_ref[...], first, second)
    letter_ref[:8] = (first_new / (jnp.sqrt(second_new) + 1e-08)).astype(jnp.bfloat16)
    mine = projected_ref[place_ref[0]]
    high = mine.astype(jnp.bfloat16)
    letter_ref[8] = high
    letter_ref[9] = (mine - high.astype(jnp.float32)).astype(jnp.bfloat16)
    send([(letter_ref, out_hbm.at[peer]) for peer in range(16)], sems)


def update(place, letters):
    shape = letters.shape[1:]
    return pl.pallas_call(
        update_kernel,
        in_specs=[SMEM, VMEM],
        out_specs=HBM,
        out_shape=pltpu.HBM((16, *shape), jnp.bfloat16),
        scratch_shapes=[
            pltpu.VMEM(shape, jnp.bfloat16),
            pltpu.VMEM((8, *shape[1:]), jnp.float32),
            pltpu.SemaphoreType.DMA((16,)),
        ],
        compiler_params=limit(8),
        name="update",
    )(place, letters)


def columns(block):
    return pl.ds(pl.multiple_of(block % 8 * 256, 256), 256)


def finish_kernel(
    place_ref, basis_hbm, weight_hbm, first_hbm, second_hbm, near_ref, far_ref, w0, w4, b1, f1_hbm, f2_hbm, b2_hbm,
    new_ref, step_ref, copy_ref, first_out, second_out, later_ref, scale_out, basis_ref,
    weight_ref, first_ref, second_ref, blocks, tiles, sems,
):
    fetched = []
    for slot, (source, target) in enumerate(
        (
            (basis_hbm, basis_ref),
            (f1_hbm, blocks.at[0]),
            (f2_hbm, blocks.at[1]),
            (b2_hbm, blocks.at[2]),
            (weight_hbm, weight_ref),
            (first_hbm, first_ref),
            (second_hbm, second_ref),
        )
    ):
        copy = pltpu.make_async_copy(source, target, sems.at[6 + slot])
        copy.start()
        fetched.append(copy)
    z, y = place_ref[0], place_ref[1]
    is_low = place_ref[3] == 0
    near, far = near_ref[:, :8].astype(jnp.float32), far_ref[:, :8].astype(jnp.float32)
    energy = jnp.sum(near * near + far * far)
    count = 2 * near.shape[0] * near.shape[1] * near.shape[2] * near.shape[3]
    spread = jnp.sqrt(jnp.full((1, 128), energy / count, jnp.float32))
    scale_out[...] = -1.0 / (spread + 1e-06)
    scale = scale_out[:, :1]
    fetched[0].wait()
    basis = basis_ref[...]

    def rows_of(close, distant):
        close, distant = (array.reshape(-1, array.shape[-1]) for array in (close, distant))
        return jnp.concatenate(
            [jnp.where(is_low, close, distant), jnp.where(is_low, distant, close)], axis=1
        )

    def rows_at(block):
        at = block % 8
        return rows_of(near_ref[:, at], far_ref[:, at])

    def step_of(block):
        return dot(basis, rows_at(block), 1, 1) * scale

    copies = []
    near_blocks = ((w0, 0), (w4, 4), (b1, 1), (blocks.at[0], 7), (blocks.at[1], 6), (blocks.at[2], 2))
    for slot, (block, hops) in enumerate(near_blocks):
        if slot >= 3:
            fetched[slot - 2].wait()
        tiles[slot] = (block[...].astype(jnp.float32) + step_of(z + hops)).astype(jnp.bfloat16)
        copy = pltpu.make_async_copy(tiles.at[slot], copy_ref.at[:, columns(z + hops)], sems.at[slot])
        copy.start()
        copies.append(copy)
    for slot, hops in enumerate((5, 3)):
        later_ref[slot] = rows_at(z + hops)

    for copy in fetched[4:]:
        copy.wait()
    mine = pl.ds(y * 4, 4)
    step = dot(rows_of(near_ref[mine, z], far_ref[mine, z]), basis, 1, 1) * scale
    step_ref[...] = step
    new_ref[...] = weight_ref[...] + step
    for source in range(4):
        rows = pl.ds(source * 16, 16)
        letter = y * 4 + source
        piece = near_ref[letter, 8].astype(jnp.float32) + near_ref[letter, 9].astype(jnp.float32)
        first_new, second_new = moments(piece, first_ref[rows, :], second_ref[rows, :])
        first_out[rows, :] = first_new
        second_out[rows, :] = second_new
    for copy in copies:
        copy.wait()


def finish(place, basis, weight, first, second, near, far, blocks):
    values = basis.shape[0]
    like = lambda array: jax.ShapeDtypeStruct(array.shape, jnp.float32)
    return pl.pallas_call(
        finish_kernel,
        in_specs=[SMEM] + [HBM] * 4 + [VMEM] * 5 + [HBM] * 3,
        out_specs=[VMEM, VMEM, HBM] + [VMEM] * 5,
        out_shape=[
            like(weight),
            like(weight),
            pltpu.HBM((values, 2048), jnp.bfloat16),
            like(first),
            like(second),
            pltpu.VMEM((2, 256, 256), jnp.bfloat16),
            pltpu.VMEM((1, 128), jnp.float32),
            pltpu.VMEM(basis.shape, basis.dtype),
        ],
        scratch_shapes=[
            pltpu.VMEM(weight.shape, weight.dtype),
            pltpu.VMEM(first.shape, first.dtype),
            pltpu.VMEM(second.shape, second.dtype),
            pltpu.VMEM((3, values, 256), jnp.bfloat16),
            pltpu.VMEM((6, values, 256), jnp.bfloat16),
            pltpu.SemaphoreType.DMA((13,)),
        ],
        compiler_params=limit(16),
        name="finish",
    )(place, *in_hbm(basis, weight, first, second), near, far, *blocks[:3], *in_hbm(*blocks[3:]))


def last_kernel(place_ref, rows_ref, scale_ref, basis_ref, f3, b3, copy_in, copy_ref, tiles, sems):
    z = place_ref[0]
    part = basis_ref.shape[0] // 2
    copies = []
    for slot, (block, hops) in enumerate(((f3, 5), (b3, 3))):
        for half in range(2):
            rows = pl.ds(half * part, part)
            step = dot(basis_ref[rows, :], rows_ref[slot], 1, 1) * scale_ref[:, :1]
            tiles[slot, rows] = (block[rows, :].astype(jnp.float32) + step).astype(jnp.bfloat16)
            copy = pltpu.make_async_copy(
                tiles.at[slot, rows], copy_ref.at[rows, columns(z + hops)], sems.at[2 * slot + half]
            )
            copy.start()
            copies.append(copy)
    for copy in copies:
        copy.wait()


def last(place, later, f3, b3, copy):
    return pl.pallas_call(
        last_kernel,
        in_specs=[SMEM] + [VMEM] * 5 + [HBM],
        out_specs=HBM,
        out_shape=pltpu.HBM(copy.shape, copy.dtype),
        input_output_aliases={6: 0},
        scratch_shapes=[pltpu.VMEM((2, copy.shape[0], 256), copy.dtype), pltpu.SemaphoreType.DMA((4,))],
        compiler_params=limit(8),
        name="last",
    )(place, *in_vmem(*later), f3, b3, *in_hbm(copy))


def exchange(array, axes):
    return lax.all_to_all(array, axes, 0, 0, tiled=True)


def chain(first_mix, second_mix, lambda_head, head_gain, out_cotangent, basis, weight, first_moment, second_moment):
    place = jnp.stack([lax.axis_index(name).astype(jnp.int32) for name in ("z", "y", "x", "tp")])
    turned = weight.T
    own, sent, narrow = heads(place, lambda_head, first_mix, second_mix, head_gain, basis, turned)

    w0 = widen(place, [narrow] + [shift(narrow, "y", hops) for hops in (1, 2, 3)])
    opposite = shift(narrow, "z", 4)
    w4 = widen(place, [opposite] + [shift(opposite, "y", hops) for hops in (1, 2, 3)])
    f1, b1 = shift(w0, "z", 1), shift(w0, "z", -1)
    f2, b2 = shift(f1, "z", 1), shift(b1, "z", -1)
    f3, b3 = shift(f2, "z", 1), shift(b2, "z", -1)

    parts = gradient(own, swap_cores(sent), out_cotangent)
    sums = fold(place, exchange(parts, ("y", "x")), first_moment, second_moment)
    near = exchange(update(place, exchange(sums, "z")), ("y", "x"))
    far = swap_cores(near)
    weight_new, step_out, most, first_new, second_new, *later = finish(
        place, basis, turned, first_moment, second_moment, near, far, (w0, w4, b1, f1, f2, b2)
    )
    weight_copy = last(place, later, f3, b3, most)
    return (weight_new.T, weight_copy, step_out.T, first_new, second_new)


def solution(mesh):
    finer = Mesh(
        mesh.devices.reshape(8, 4, mesh.shape["rep"], mesh.shape["tp"]),
        ("z", "y", "x", "tp"),
    )
    return jax.shard_map(
        chain,
        mesh=finer,
        in_specs=(
            P(FS_REP, "tp"),
            P(FS_REP, "tp"),
            P("tp"),
            P(),
            P(FS_REP, None),
            P("tp", None),
            P("tp", FS),
            P(FS, "tp"),
            P(FS, "tp"),
        ),
        out_specs=(P("tp", FS), P("tp", None), P("tp", FS), P(FS, "tp"), P(FS, "tp")),
        check_vma=False,
    )
```

```python
import jax
import jax.numpy as jnp
from jax import lax
from jax.experimental import pallas as pl
from jax.experimental.pallas import tpu as pltpu
from jax.sharding import Mesh
from jax.sharding import PartitionSpec as P

OUT_SCALE = 0.8
BETA_FIRST = 0.9
BETA_SECOND = 0.95
FS = ("z", "y")
FS_REP = ("z", "y", "x")
SMEM = pl.BlockSpec(memory_space=pltpu.SMEM)
VMEM = pl.BlockSpec(memory_space=pltpu.VMEM)
HBM = pl.BlockSpec(memory_space=pltpu.HBM)
MIB = 1024 * 1024


def in_hbm(*arrays):
    return [pltpu.with_memory_space_constraint(array, pltpu.HBM) for array in arrays]


def in_vmem(*arrays):
    return [pltpu.with_memory_space_constraint(array, pltpu.VMEM) for array in arrays]


def shift(array, axis, hops):
    count = lax.axis_size(axis)
    return lax.ppermute(array, axis, [(i, (i + hops) % count) for i in range(count)])


def swap_cores(array):
    return lax.ppermute(array, "tp", [(0, 1), (1, 0)])


def dot(left, right, left_dim, right_dim):
    return lax.dot_general(
        left, right, (((left_dim,), (right_dim,)), ((), ())), preferred_element_type=jnp.float32
    )


def limit(mib):
    return pltpu.CompilerParams(vmem_limit_bytes=mib * MIB)


def heads_kernel(
    place_ref, lam_hbm, first_hbm, second_hbm, gain_hbm, basis_hbm, weight_hbm,
    own_ref, sent_ref, narrow_ref, first_ref, second_ref, basis_ref, lam_ref, gain_ref, weight_ref, sems,
):
    tokens, values = first_ref.shape
    width = gain_ref.shape[1]
    steps = 3
    tile = tokens // steps

    def fetch(source, target, slot):
        copy = pltpu.make_async_copy(source, target, sems.at[slot])
        copy.start()
        return copy

    fixed = [fetch(lam_hbm, lam_ref, 0), fetch(gain_hbm, gain_ref, 1)]
    moving = []
    for step in range(steps):
        rows = pl.ds(step * tile, tile)
        moving.append(
            [
                fetch(first_hbm.at[rows], first_ref.at[rows], 4 + 2 * step),
                fetch(second_hbm.at[rows], second_ref.at[rows], 5 + 2 * step),
            ]
        )
        if step == 0:
            fixed.append(fetch(basis_hbm, basis_ref, 2))
    last = fetch(weight_hbm, weight_ref, 3)
    for copy in fixed[:2]:
        copy.wait()
    gain = gain_ref[...] * OUT_SCALE
    is_low = place_ref[3] == 0
    for step in range(steps):
        rows = pl.ds(step * tile, tile)
        for copy in moving[step]:
            copy.wait()
        if step == 0:
            fixed[2].wait()
        total = None
        for head in range(values // width):
            cols = slice(head * width, (head + 1) * width)
            first = first_ref[rows, cols].astype(jnp.float32)
            second = second_ref[rows, cols].astype(jnp.float32)
            mixture = first - lam_ref[:, head : head + 1] * second
            inverse = lax.rsqrt(jnp.mean(mixture * mixture, axis=-1, keepdims=True) + 1e-06)
            normed = (mixture * inverse * gain).astype(jnp.bfloat16)
            term = jnp.dot(normed, basis_ref[cols, :], preferred_element_type=jnp.float32)
            total = term if total is None else total + term
        half = total.shape[1] // 2
        low, high = total[:, :half], total[:, half:]
        own_ref[rows, :] = jnp.where(is_low, low, high)
        sent_ref[rows, :] = jnp.where(is_low, high, low).astype(jnp.bfloat16)
    last.wait()
    narrow_ref[...] = weight_ref[...].astype(jnp.bfloat16)


def heads(place, lambda_head, first_mix, second_mix, head_gain, basis, weight):
    tokens, values = first_mix.shape
    half = basis.shape[1] // 2
    lam, gain = lambda_head[None, :], head_gain[None, :]
    return pl.pallas_call(
        heads_kernel,
        in_specs=[SMEM] + [HBM] * 6,
        out_specs=[VMEM] * 3,
        out_shape=[
            jax.ShapeDtypeStruct((tokens, half), jnp.float32),
            jax.ShapeDtypeStruct((tokens, half), jnp.bfloat16),
            pltpu.VMEM(weight.shape, jnp.bfloat16),
        ],
        scratch_shapes=[
            pltpu.VMEM((tokens, values), jnp.bfloat16),
            pltpu.VMEM((tokens, values), jnp.bfloat16),
            pltpu.VMEM(basis.shape, jnp.bfloat16),
            pltpu.VMEM(lam.shape, jnp.float32),
            pltpu.VMEM(gain.shape, jnp.float32),
            pltpu.VMEM(weight.shape, jnp.float32),
            pltpu.SemaphoreType.DMA((16,)),
        ],
        compiler_params=limit(12),
        name="heads",
    )(place, *in_hbm(lam, first_mix, second_mix, gain, basis, weight))


def widen_kernel(place_ref, own_ref, one_ref, two_ref, three_ref, out_ref, slots):
    y = place_ref[1]
    slots[y] = own_ref[...].astype(jnp.float32)
    slots[(y + 3) % 4] = one_ref[...].astype(jnp.float32)
    slots[(y + 2) % 4] = two_ref[...].astype(jnp.float32)
    slots[(y + 1) % 4] = three_ref[...].astype(jnp.float32)
    rows = slots.shape[0] * slots.shape[1]
    out_ref[...] = slots[...].reshape(rows, slots.shape[2]).T.astype(jnp.bfloat16)


def widen(place, blocks):
    rows, cols = blocks[0].shape
    return pl.pallas_call(
        widen_kernel,
        in_specs=[SMEM] + [VMEM] * 4,
        out_specs=VMEM,
        out_shape=jax.ShapeDtypeStruct((cols, 4 * rows), jnp.bfloat16),
        scratch_shapes=[pltpu.VMEM((4, rows, cols), jnp.float32)],
        compiler_params=limit(8),
        name="widen",
    )(place, *blocks)


def gradient_kernel(own_ref, far_ref, cot_ref, out_hbm, parts, sems):
    reduced = (own_ref[...] + far_ref[...].astype(jnp.float32)).T.astype(jnp.bfloat16)
    wide = 512
    copies = []
    for at in range(cot_ref.shape[1] // wide):
        block = dot(reduced, cot_ref[:, at * wide : (at + 1) * wide], 1, 0).T.astype(jnp.bfloat16)
        for z in range(2):
            rows = block[z * 256 : (z + 1) * 256]
            parts[:, at * 2 + z] = rows.reshape(16, 16, rows.shape[1])
        pair = pl.ds(at * 2, 2)
        copy = pltpu.make_async_copy(parts.at[:, pair], out_hbm.at[:, pair], sems.at[at])
        copy.start()
        copies.append(copy)
    for copy in copies:
        copy.wait()


def gradient(own, far, cot):
    shape = (16, 8, 16, own.shape[1])
    return pl.pallas_call(
        gradient_kernel,
        in_specs=[VMEM] * 3,
        out_specs=HBM,
        out_shape=pltpu.HBM(shape, jnp.bfloat16),
        scratch_shapes=[pltpu.VMEM(shape, jnp.bfloat16), pltpu.SemaphoreType.DMA((4,))],
        compiler_params=limit(8),
        name="gradient",
    )(own, far, cot)


def send(pairs, sems):
    copies = []
    for slot, (source, target) in enumerate(pairs):
        copy = pltpu.make_async_copy(source, target, sems.at[slot])
        copy.start()
        copies.append(copy)
    for copy in copies:
        copy.wait()


def fold_kernel(place_ref, parts_ref, first_ref, second_ref, out_hbm, letter_ref, sems):
    rows = pl.ds(pl.multiple_of(place_ref[2] * 16, 16), 16)
    letter_ref[:8] = jnp.sum(parts_ref[...].astype(jnp.float32), axis=0).astype(jnp.bfloat16)
    letter_ref[8] = first_ref[rows, :].astype(jnp.bfloat16)
    letter_ref[9] = second_ref[rows, :].astype(jnp.bfloat16)
    send([(letter_ref, out_hbm.at[z]) for z in range(8)], sems)


def fold(place, parts, first, second):
    shape = (10, *parts.shape[2:])
    return pl.pallas_call(
        fold_kernel,
        in_specs=[SMEM] + [VMEM] * 3,
        out_specs=HBM,
        out_shape=pltpu.HBM((8, *shape), jnp.bfloat16),
        scratch_shapes=[pltpu.VMEM(shape, jnp.bfloat16), pltpu.SemaphoreType.DMA((8,))],
        compiler_params=limit(8),
        name="fold",
    )(place, parts, first, second)


def moments(projected, first, second):
    first_new = BETA_FIRST * first + (1.0 - BETA_FIRST) * projected
    second_new = BETA_SECOND * second + (1.0 - BETA_SECOND) * projected * projected
    return first_new, second_new


def update_kernel(place_ref, letters_ref, out_hbm, letter_ref, projected_ref, sems):
    projected_ref[...] = jnp.sum(letters_ref[:, :8].astype(jnp.float32), axis=0)
    first, second = letters_ref[:, 8].astype(jnp.float32), letters_ref[:, 9].astype(jnp.float32)
    first_new, second_new = moments(projected_ref[...], first, second)
    letter_ref[:8] = (first_new / (jnp.sqrt(second_new) + 1e-08)).astype(jnp.bfloat16)
    mine = projected_ref[place_ref[0]]
    letter_ref[8] = mine.astype(jnp.bfloat16)
    send([(letter_ref, out_hbm.at[peer]) for peer in range(16)], sems)


def update(place, letters):
    shape = (9, *letters.shape[2:])
    return pl.pallas_call(
        update_kernel,
        in_specs=[SMEM, VMEM],
        out_specs=HBM,
        out_shape=pltpu.HBM((16, *shape), jnp.bfloat16),
        scratch_shapes=[
            pltpu.VMEM(shape, jnp.bfloat16),
            pltpu.VMEM((8, *shape[1:]), jnp.float32),
            pltpu.SemaphoreType.DMA((16,)),
        ],
        compiler_params=limit(8),
        name="update",
    )(place, letters)


def columns(block):
    return pl.ds(pl.multiple_of(block % 8 * 256, 256), 256)


def finish_kernel(
    place_ref, basis_hbm, weight_hbm, first_hbm, second_hbm, near_ref, far_ref, w0, w4, b1, f1_hbm, f2_hbm, b2_hbm,
    new_ref, step_ref, copy_ref, first_out, second_out, later_ref, scale_out, basis_ref,
    weight_ref, first_ref, second_ref, blocks, tiles, sems,
):
    fetched = []
    for slot, (source, target) in enumerate(
        (
            (basis_hbm, basis_ref),
            (f1_hbm, blocks.at[0]),
            (f2_hbm, blocks.at[1]),
            (b2_hbm, blocks.at[2]),
            (weight_hbm, weight_ref),
            (first_hbm, first_ref),
            (second_hbm, second_ref),
        )
    ):
        copy = pltpu.make_async_copy(source, target, sems.at[6 + slot])
        copy.start()
        fetched.append(copy)
    z, y = place_ref[0], place_ref[1]
    is_low = place_ref[3] == 0
    near, far = near_ref[:, :8].astype(jnp.float32), far_ref[:, :8].astype(jnp.float32)
    energy = jnp.sum(near * near + far * far)
    count = 2 * near.shape[0] * near.shape[1] * near.shape[2] * near.shape[3]
    spread = jnp.sqrt(jnp.full((1, 128), energy / count, jnp.float32))
    scale_out[...] = -1.0 / (spread + 1e-06)
    scale = scale_out[:, :1]
    fetched[0].wait()
    basis = basis_ref[...]

    def rows_of(close, distant):
        close, distant = (array.reshape(-1, array.shape[-1]) for array in (close, distant))
        return jnp.concatenate(
            [jnp.where(is_low, close, distant), jnp.where(is_low, distant, close)], axis=1
        )

    def rows_at(block):
        at = block % 8
        return rows_of(near_ref[:, at], far_ref[:, at])

    def step_of(block):
        return dot(basis, rows_at(block), 1, 1) * scale

    copies = []
    near_blocks = ((w0, 0), (w4, 4), (b1, 1), (blocks.at[0], 7), (blocks.at[1], 6), (blocks.at[2], 2))
    for slot, (block, hops) in enumerate(near_blocks):
        if slot >= 3:
            fetched[slot - 2].wait()
        tiles[slot] = (block[...].astype(jnp.float32) + step_of(z + hops)).astype(jnp.bfloat16)
        copy = pltpu.make_async_copy(tiles.at[slot], copy_ref.at[:, columns(z + hops)], sems.at[slot])
        copy.start()
        copies.append(copy)
    for slot, hops in enumerate((5, 3)):
        later_ref[slot] = rows_at(z + hops)

    for copy in fetched[4:]:
        copy.wait()
    mine = pl.ds(y * 4, 4)
    step = dot(rows_of(near_ref[mine, z], far_ref[mine, z]), basis, 1, 1) * scale
    step_ref[...] = step
    new_ref[...] = weight_ref[...] + step
    for source in range(4):
        rows = pl.ds(source * 16, 16)
        letter = y * 4 + source
        piece = near_ref[letter, 8].astype(jnp.float32)
        first_new, second_new = moments(piece, first_ref[rows, :], second_ref[rows, :])
        first_out[rows, :] = first_new
        second_out[rows, :] = second_new
    for copy in copies:
        copy.wait()


def finish(place, basis, weight, first, second, near, far, blocks):
    values = basis.shape[0]
    like = lambda array: jax.ShapeDtypeStruct(array.shape, jnp.float32)
    return pl.pallas_call(
        finish_kernel,
        in_specs=[SMEM] + [HBM] * 4 + [VMEM] * 5 + [HBM] * 3,
        out_specs=[VMEM, VMEM, HBM] + [VMEM] * 5,
        out_shape=[
            like(weight),
            like(weight),
            pltpu.HBM((values, 2048), jnp.bfloat16),
            like(first),
            like(second),
            pltpu.VMEM((2, 256, 256), jnp.bfloat16),
            pltpu.VMEM((1, 128), jnp.float32),
            pltpu.VMEM(basis.shape, basis.dtype),
        ],
        scratch_shapes=[
            pltpu.VMEM(weight.shape, weight.dtype),
            pltpu.VMEM(first.shape, first.dtype),
            pltpu.VMEM(second.shape, second.dtype),
            pltpu.VMEM((3, values, 256), jnp.bfloat16),
            pltpu.VMEM((6, values, 256), jnp.bfloat16),
            pltpu.SemaphoreType.DMA((13,)),
        ],
        compiler_params=limit(16),
        name="finish",
    )(place, *in_hbm(basis, weight, first, second), near, far, *blocks[:3], *in_hbm(*blocks[3:]))


def last_kernel(place_ref, rows_ref, scale_ref, basis_ref, f3, b3, copy_in, copy_ref, tiles, sems):
    z = place_ref[0]
    part = basis_ref.shape[0] // 2
    copies = []
    for slot, (block, hops) in enumerate(((f3, 5), (b3, 3))):
        for half in range(2):
            rows = pl.ds(half * part, part)
            step = dot(basis_ref[rows, :], rows_ref[slot], 1, 1) * scale_ref[:, :1]
            tiles[slot, rows] = (block[rows, :].astype(jnp.float32) + step).astype(jnp.bfloat16)
            copy = pltpu.make_async_copy(
                tiles.at[slot, rows], copy_ref.at[rows, columns(z + hops)], sems.at[2 * slot + half]
            )
            copy.start()
            copies.append(copy)
    for copy in copies:
        copy.wait()


def last(place, later, f3, b3, copy):
    return pl.pallas_call(
        last_kernel,
        in_specs=[SMEM] + [VMEM] * 5 + [HBM],
        out_specs=HBM,
        out_shape=pltpu.HBM(copy.shape, copy.dtype),
        input_output_aliases={6: 0},
        scratch_shapes=[pltpu.VMEM((2, copy.shape[0], 256), copy.dtype), pltpu.SemaphoreType.DMA((4,))],
        compiler_params=limit(8),
        name="last",
    )(place, *in_vmem(*later), f3, b3, *in_hbm(copy))


def exchange(array, axes):
    return lax.all_to_all(array, axes, 0, 0, tiled=True)


def chain(first_mix, second_mix, lambda_head, head_gain, out_cotangent, basis, weight, first_moment, second_moment):
    place = jnp.stack([lax.axis_index(name).astype(jnp.int32) for name in ("z", "y", "x", "tp")])
    turned = weight.T
    own, sent, narrow = heads(place, lambda_head, first_mix, second_mix, head_gain, basis, turned)

    w0 = widen(place, [narrow] + [shift(narrow, "y", hops) for hops in (1, 2, 3)])
    opposite = shift(narrow, "z", 4)
    w4 = widen(place, [opposite] + [shift(opposite, "y", hops) for hops in (1, 2, 3)])
    f1, b1 = shift(w0, "z", 1), shift(w0, "z", -1)
    f2, b2 = shift(f1, "z", 1), shift(b1, "z", -1)
    f3, b3 = shift(f2, "z", 1), shift(b2, "z", -1)

    parts = gradient(own, swap_cores(sent), out_cotangent)
    sums = fold(place, exchange(parts, ("y", "x")), first_moment, second_moment)
    near = exchange(update(place, exchange(sums, "z")), ("y", "x"))
    far = swap_cores(near)
    weight_new, step_out, most, first_new, second_new, *later = finish(
        place, basis, turned, first_moment, second_moment, near, far, (w0, w4, b1, f1, f2, b2)
    )
    weight_copy = last(place, later, f3, b3, most)
    return (weight_new.T, weight_copy, step_out.T, first_new, second_new)


def solution(mesh):
    finer = Mesh(
        mesh.devices.reshape(8, 4, mesh.shape["rep"], mesh.shape["tp"]),
        ("z", "y", "x", "tp"),
    )
    return jax.shard_map(
        chain,
        mesh=finer,
        in_specs=(
            P(FS_REP, "tp"),
            P(FS_REP, "tp"),
            P("tp"),
            P(),
            P(FS_REP, None),
            P("tp", None),
            P("tp", FS),
            P(FS, "tp"),
            P(FS, "tp"),
        ),
        out_specs=(P("tp", FS), P("tp", None), P("tp", FS), P(FS, "tp"), P(FS, "tp")),
        check_vma=False,
    )
```
